32 devices in a mesh: kv: 16 (over z, y, x), tp: 2 (over core).
Axes of the slice: x: 2, y: 2, z: 4, core: 2. Of those that a mesh axis runs over, the one named last changes fastest.
Arguments:
- tokens: bfloat16 [4096, 2048], P('kv'), may hold values from -72 to 72
- w_query: bfloat16 [2048, 1024], P(None, 'tp'), may hold values from -0.125 to 0.125
- w_key: bfloat16 [2048, 1024], P(None, 'tp'), may hold values from -0.125 to 0.125
- w_value: bfloat16 [2048, 1024], P(None, 'tp'), may hold values from -0.125 to 0.125
- w_out: bfloat16 [1024, 2048], P('tp'), may hold values from -0.1875 to 0.1875
- chosen: int32 [64, 16], replicated, may hold values from -1 to 63, as said below
Outputs:
- mixed: bfloat16 [4096, 2048], P(('kv', 'tp'))
- log_sums: float32 [16, 4096], P('tp', 'kv')
The draws below stay inside these ranges and needn't reach their ends.
Inputs may be any that keep to these rules, and one draw needn't show every extreme that they name: `chosen`: row b begins with b itself, then lists distinct key blocks at most b, then holds -1 in its remaining entries. Taken together, the rows of the query blocks of one index of kv list at most 2 distinct blocks of the positions of any other index of kv, and exactly 2 for some pairs of indices in every draw.
All inputs are finite; a program needn't handle non-finite values.
Results may differ from the reference program's by a relative error of at most 0.03.
Values may be sent and summed in bfloat16 or wider, within the bound.
A program may use at most 64 MiB of HBM per device.

```python
import jax
import jax.numpy as jnp
from jax import lax

D = 2048
HEADS = 16
HEAD_DIM = 64
BLK = 64
SEL = 16
CAP = 2
TOK_DEV = 256
ATT = 1024
TOKENS = 4096
NBLK = 64
N_TP = 2


def draw_tokens(key, part):
    values = jnp.clip(jax.random.normal(key, (TOKENS, D), jnp.float32), -6.0, 6.0)
    return values.astype(jnp.bfloat16)


def draw_chosen(key, part):
    per_dev = TOK_DEV // BLK
    devices = NBLK // per_dev
    pair_key = jax.random.fold_in(key, 11)
    hot_key = jax.random.fold_in(key, 12)
    rank_key = jax.random.fold_in(key, 13)
    order_bits = jax.random.randint(pair_key, (devices, devices, per_dev), 0, 1 << 20) * per_dev + jnp.arange(per_dev)
    ordering = jnp.argsort(order_bits, axis=-1)[..., :CAP]
    picked_blocks = jnp.arange(devices)[None, :, None] * per_dev + ordering
    hotness = jax.random.randint(hot_key, (devices,), 0, 4)
    blocks = jnp.arange(NBLK)
    query_block = blocks[:, None]
    target = blocks[None, :]
    query_dev = query_block // per_dev
    target_dev = target // per_dev
    pair_table = jnp.any(picked_blocks[:, blocks // per_dev, :] == blocks[None, :, None], axis=-1)
    in_pair = pair_table[blocks // per_dev] & (target_dev < query_dev)
    same_dev = (target_dev == query_dev) & (target <= query_block)
    near_dev = (target_dev == query_dev - 1) | (target_dev == query_dev - devices // 2)
    tier_level = jnp.where(target == query_block, 3, jnp.where(same_dev | in_pair & near_dev, 2, 1))
    jitter = jax.random.randint(rank_key, (NBLK, NBLK), 0, 1 << 12)
    rating = ((tier_level * 4 + hotness[target_dev]) * 4096 + jitter) * NBLK + target
    rating = jnp.where(same_dev | in_pair, rating, -1 - target)
    values, position = lax.top_k(rating, SEL)
    return jnp.where(values >= 0, position, -1).astype(jnp.int32)


def level_of(stream_key, extent, split, smallest, high):
    gain = 1.0
    for dim, blocks in split:
        steps = jax.random.uniform(jax.random.fold_in(jax.random.fold_in(stream_key, 6), dim), (blocks,), jnp.float32, smallest / len(split), high / len(split))
        gain = gain * jnp.repeat(jnp.exp(steps), extent[dim] // blocks).reshape((-1,) + (1,) * (len(extent) - 1 - dim))
    return gain


def normal_values(stream_key, shape, deviation, reach, cuts=(), held_as=jnp.bfloat16):
    result = deviation * jax.random.normal(stream_key, shape, jnp.float32)
    if cuts:
        result = result * level_of(stream_key, shape, cuts, -0.22, 0.18)
    return jnp.clip(result, -reach, reach).astype(held_as)


def setup_inputs(seed: int = 0) -> dict:
    keys = jax.random.split(jax.random.key(seed), 7)
    tokens = draw_tokens(jax.random.fold_in(keys[6], 71), 0)
    w_query = normal_values(keys[1], (D, ATT), D ** -0.5, 0.125, ((1, 2),))
    w_key = normal_values(keys[2], (D, ATT), D ** -0.5, 0.125, ((1, 2),))
    w_value = normal_values(keys[3], (D, ATT), D ** -0.5, 0.125, ((1, 2),))
    w_out = normal_values(keys[4], (ATT, D), ATT ** -0.5, 0.1875, ((0, 2),))
    chosen = draw_chosen(jax.random.fold_in(keys[6], 71), 0)
    return dict(tokens=tokens, w_query=w_query, w_key=w_key, w_value=w_value, w_out=w_out, chosen=chosen)


rotary_base = 500000.0
masked_score = -1e30


def rotate(values, positions, head_count, head_size):
    half_size = head_size // 2
    inverse = rotary_base ** (-jnp.arange(half_size, dtype=jnp.float32) / half_size)
    angles = positions.astype(jnp.float32)[:, None, None] * inverse[None, None, :]
    cos_part = jnp.cos(angles)
    sin_part = jnp.sin(angles)
    grouped = values.reshape(values.shape[0], head_count, head_size)
    first_half = grouped[..., :half_size]
    second_half = grouped[..., half_size:]
    turned = jnp.concatenate([first_half * cos_part - second_half * sin_part, second_half * cos_part + first_half * sin_part], axis=-1)
    return turned.reshape(values.shape)


def reference(tokens, w_query, w_key, w_value, w_out, chosen):
    positions = jnp.arange(TOKENS)
    query = rotate(jnp.dot(tokens, w_query, preferred_element_type=jnp.float32), positions, HEADS, HEAD_DIM).astype(jnp.bfloat16)
    keys_all = rotate(jnp.dot(tokens, w_key, preferred_element_type=jnp.float32), positions, HEADS, HEAD_DIM).astype(jnp.bfloat16)
    values_all = jnp.dot(tokens, w_value, preferred_element_type=jnp.float32).astype(jnp.bfloat16)
    key_blocks = keys_all.reshape(NBLK, BLK, HEADS, HEAD_DIM)
    value_blocks = values_all.reshape(NBLK, BLK, HEADS, HEAD_DIM)
    query_blocks = query.reshape(NBLK, BLK, HEADS, HEAD_DIM)
    scaling = HEAD_DIM ** -0.5

    def one_block(inputs):
        query_rows, listed = inputs
        usable = listed >= 0
        safe_rows = jnp.maximum(listed, 0)
        picked_keys = key_blocks[safe_rows].reshape(SEL * BLK, HEADS, HEAD_DIM)
        picked_values = value_blocks[safe_rows].reshape(SEL * BLK, HEADS, HEAD_DIM)
        scores = jnp.einsum('qhd,khd->hqk', query_rows.astype(jnp.float32), picked_keys.astype(jnp.float32)) * scaling
        key_mask = jnp.broadcast_to(usable[:, None], (SEL, BLK)).reshape(SEL * BLK)
        scores = jnp.where(key_mask[None, None, :], scores, masked_score)
        row_max = jnp.max(scores, axis=-1)
        weights = jnp.where(key_mask[None, None, :], jnp.exp(scores - row_max[..., None]), 0.0)
        totals = jnp.sum(weights, axis=-1)
        rounded = lax.optimization_barrier(weights.astype(jnp.bfloat16)).astype(jnp.float32)
        summed = jnp.einsum('hqk,khd->qhd', rounded, picked_values.astype(jnp.float32))
        mixed_rows = (summed / jnp.transpose(totals)[:, :, None]).reshape(BLK, HEADS * HEAD_DIM).astype(jnp.bfloat16)
        return mixed_rows, row_max + jnp.log(totals)

    mixed_all, log_blocks = lax.map(one_block, (query_blocks, chosen))
    attended = mixed_all.reshape(TOKENS, HEADS * HEAD_DIM)
    log_sums = jnp.transpose(log_blocks, (1, 0, 2)).reshape(HEADS, TOKENS)
    group_width = HEADS * HEAD_DIM // N_TP
    output = jnp.zeros((TOKENS, D), jnp.float32)
    for group_index in range(N_TP):
        lower = group_index * group_width
        partial_sum = jnp.dot(attended[:, lower:lower + group_width], w_out[lower:lower + group_width], preferred_element_type=jnp.float32)
        output = output + lax.optimization_barrier(partial_sum.astype(jnp.bfloat16)).astype(jnp.float32)
    return output.astype(jnp.bfloat16), log_sums
```

```python
import functools

import jax
import jax.numpy as jnp
import numpy as np
from jax import lax
from jax.experimental import pallas as pl
from jax.experimental.pallas import tpu as pltpu
from jax.sharding import PartitionSpec as P

HEAD_DIM = 64
BLK = 64
LANES = 128
VMEM_LIMIT = 65_000_000

rotary_base = 500000.0
masked_score = -1e30

MESH = pl.DeviceIdType.MESH


def in_vmem():
    return pl.BlockSpec(memory_space=pltpu.VMEM)


def in_smem():
    return pl.BlockSpec(memory_space=pltpu.SMEM)


def in_hbm():
    return pl.BlockSpec(memory_space=pltpu.HBM)


def swap_halves(tile):
    return pltpu.roll(tile, LANES // 2, 1)


def layer_kernel(
    devices, splits, chosen_ref, x_ref, wq_ref, wk_ref, wv_ref, wo_ref, cos_ref, sin_ref, base_ref,
    mine_ref, landed_ref, log_ref,
    x, wq, wkv, wo, cos_t, sin_t, kv_out, q_out, kv_in, vk_in, q_in, o_out, l_out, o_in, l_in, weight, total_log,
    attended, stage, load_sem, kv_send, kv_recv, q_send, q_recv, o_send, o_recv, l_send, l_recv, tp_send, tp_recv,
):
    heads = kv_out.shape[0]
    pairs = heads // 2
    groups = devices // heads
    blocks = kv_out.shape[1]
    tiles = blocks // 2
    rows = blocks * BLK
    entries = chosen_ref.shape[0]
    table_blocks = heads * blocks
    wide = wq.shape[2] // LANES

    me = lax.axis_index("kv")
    tp = lax.axis_index("tp")
    group = lax.div(me, heads)
    idx = lax.rem(me, heads)
    first_device = group * heads
    half = HEAD_DIM // 2

    def pair_of(i):
        return lax.rem(lax.div(idx, 2) + 1 + i, pairs)

    def strip(ref, i):
        return ref.at[:, pl.ds(pl.multiple_of(pair_of(i) * LANES, LANES), LANES)]

    def load_q(i):
        target = wq.at[i // wide, :, pl.ds((i % wide) * LANES, LANES)]
        return pltpu.make_async_copy(strip(wq_ref, i), target, load_sem.at[0, i])

    def load_k(i):
        return pltpu.make_async_copy(strip(wk_ref, i), wkv.at[i, :, pl.ds(0, LANES)], load_sem.at[1, i])

    def load_v(i):
        return pltpu.make_async_copy(strip(wv_ref, i), wkv.at[i, :, pl.ds(LANES, LANES)], load_sem.at[2, i])

    load_x = pltpu.make_async_copy(x_ref, x, load_sem.at[3, 0])
    load_cos = pltpu.make_async_copy(cos_ref, cos_t, load_sem.at[4, 0])
    load_sin = pltpu.make_async_copy(sin_ref, sin_t, load_sem.at[5, 0])
    load_o = pltpu.make_async_copy(wo_ref, wo, load_sem.at[6, 0])

    load_x.start()
    load_cos.start()
    load_sin.start()
    for i in range(pairs):
        load_k(i).start()
        load_v(i).start()
        if i % wide == 0:
            for e in range(wide):
                load_q(i + e).start()
    load_o.start()

    barrier = pltpu.get_barrier_semaphore()

    def greet(d, carry):
        pl.semaphore_signal(
            barrier, inc=1, device_id={"kv": lax.rem(me + d, devices)}, device_id_type=MESH
        )
        return carry

    lax.fori_loop(1, devices, greet, 0)
    for d in range(1, splits):
        pl.semaphore_signal(barrier, inc=1, device_id={"tp": lax.rem(tp + d, splits)}, device_id_type=MESH)

    def kv_copy(slot, head):
        return pltpu.make_async_remote_copy(
            src_ref=kv_out.at[slot],
            dst_ref=kv_in.at[idx],
            send_sem=kv_send.at[head],
            recv_sem=kv_recv.at[idx],
            device_id={"kv": first_device + head},
            device_id_type=MESH,
        )

    def q_copy(slot, target):
        return pltpu.make_async_remote_copy(
            src_ref=q_out.at[slot],
            dst_ref=q_in.at[me],
            send_sem=q_send.at[target],
            recv_sem=q_recv.at[me],
            device_id={"kv": target},
            device_id_type=MESH,
        )

    def o_copy(target):
        return pltpu.make_async_remote_copy(
            src_ref=o_out.at[target],
            dst_ref=o_in.at[group, idx],
            send_sem=o_send.at[target],
            recv_sem=o_recv.at[me],
            device_id={"kv": target},
            device_id_type=MESH,
        )

    def l_copy(target):
        return pltpu.make_async_remote_copy(
            src_ref=l_out.at[target],
            dst_ref=l_in.at[group, idx],
            send_sem=l_send.at[target],
            recv_sem=l_recv.at[me],
            device_id={"kv": target},
            device_id_type=MESH,
        )

    def arrival(copy, semaphore):
        return pltpu.make_async_remote_copy(
            src_ref=copy, dst_ref=copy, send_sem=semaphore, recv_sem=semaphore,
            device_id={"kv": me}, device_id_type=MESH,
        )

    load_x.wait()
    load_cos.wait()
    load_sin.wait()
    low_rows = lax.broadcasted_iota(jnp.int32, (rows, LANES), 1) < LANES // 2
    turn_low = lax.broadcasted_iota(jnp.int32, (rows, LANES), 1) % HEAD_DIM < half
    cos_base = base_ref[0, pl.ds(me, 1), :]
    sin_base = base_ref[1, pl.ds(me, 1), :]
    cos_part = cos_t[...] * cos_base - sin_t[...] * sin_base
    sin_part = sin_t[...] * cos_base + cos_t[...] * sin_base
    sin_part = jnp.where(turn_low, -sin_part, sin_part)

    def turned(part):
        other = jnp.where(turn_low, pltpu.roll(part, LANES - half, 1), pltpu.roll(part, half, 1))
        return part * cos_part + other * sin_part

    def make_kv(i):
        load_k(i).wait()
        load_v(i).wait()
        made = jnp.dot(x[...], wkv[i], preferred_element_type=jnp.float32)
        keys = turned(made[:, :LANES])
        values = made[:, LANES:]
        even = jnp.where(low_rows, keys, swap_halves(values)).astype(jnp.bfloat16)
        odd = jnp.where(low_rows, swap_halves(keys), values).astype(jnp.bfloat16)
        for r in range(blocks):
            kv_out[2 * i, r] = even[r * BLK : (r + 1) * BLK]
            kv_out[2 * i + 1, r] = odd[r * BLK : (r + 1) * BLK]

    def make_q(i):
        for e in range(wide):
            load_q(i + e).wait()
        made = jnp.dot(x[...], wq[i // wide], preferred_element_type=jnp.float32)
        for e in range(wide):
            part = turned(made[:, e * LANES : (e + 1) * LANES]) * (HEAD_DIM**-0.5)
            swapped = swap_halves(part)
            low = low_rows[:BLK]
            for m in range(tiles):
                a = slice(2 * m * BLK, (2 * m + 1) * BLK)
                b = slice((2 * m + 1) * BLK, (2 * m + 2) * BLK)
                q_out[2 * (i + e), m] = jnp.where(low, part[a], swapped[b]).astype(jnp.bfloat16)
                q_out[2 * (i + e) + 1, m] = jnp.where(low, swapped[a], part[b]).astype(jnp.bfloat16)

    def send_kv(i):
        for e in range(2):
            head = 2 * pair_of(i) + e
            if i < pairs - 1:
                kv_copy(2 * i + e, head).start()
            else:
                pl.when(head != idx)(lambda e=e, head=head: kv_copy(2 * i + e, head).start())

    def send_q(i):
        for e in range(2):
            head = 2 * pair_of(i) + e
            if i < pairs - 1:
                q_copy(2 * i + e, first_device + head).start()
            else:
                pl.when(head != idx)(lambda e=e, head=head: q_copy(2 * i + e, first_device + head).start())

    for i in range(pairs):
        make_kv(i)
        if i == 0:
            pl.semaphore_wait(barrier, devices - 1 + splits - 1)
        send_kv(i)
        if i % wide == 0:
            make_q(i)
        send_q(i)

    def send_down(a, carry):
        for i in range(pairs):
            for e in range(2):
                q_copy(2 * i + e, a * heads + 2 * pair_of(i) + e).start()
        return carry

    lax.fori_loop(0, group, send_down, 0)

    own_slot = 2 * (pairs - 1) + lax.rem(idx, 2)
    for r in range(blocks):
        kv_in[idx, r] = kv_out[own_slot, r]
    for m in range(tiles):
        q_in[me, m] = q_out[own_slot, m]

    low = lax.broadcasted_iota(jnp.int32, (BLK, LANES), 1) < LANES // 2
    lane = lax.broadcasted_iota(jnp.int32, (BLK, LANES), 1)
    low_line = lax.broadcasted_iota(jnp.int32, (1, LANES), 1) < LANES // 2

    def take_kv(k, carry):
        source = lax.rem(idx + k, heads)

        @pl.when(k > 0)
        def _():
            arrival(kv_in.at[source], kv_recv.at[source]).wait_recv()

        for r in range(blocks):
            vk_in[source, r] = swap_halves(kv_in[source, r].astype(jnp.float32)).astype(jnp.bfloat16)
        return carry

    lax.fori_loop(0, heads, take_kv, 0)

    def attend(j):
        logs = jnp.zeros((BLK, LANES), jnp.float32)
        for m in range(tiles):
            tile = q_in[j, m]
            swapped = swap_halves(tile.astype(jnp.float32)).astype(jnp.bfloat16)
            none = jnp.zeros_like(tile)
            results = []
            for e in range(2):
                r = 2 * m + e
                at_low, at_high = (tile, swapped) if e == 0 else (swapped, tile)
                stacked = jnp.concatenate([jnp.where(low, at_low, none), jnp.where(low, none, at_high)], axis=0)
                bias, places = [], []
                for s in range(entries):
                    place = chosen_ref[s, j * blocks + r] - first_device * blocks
                    held = (place >= 0) & (place < table_blocks)
                    bias.append(jnp.where(held, 0.0, masked_score).astype(jnp.float32))
                    places.append(jnp.where(held, place, 0))
                scores, values = [], []
                for lower in range(0, entries, 8):
                    keys_here, values_here = [], []
                    for s in range(lower, lower + 8, 2):
                        a_place, b_place = places[s], places[s + 1]
                        a = kv_in[lax.div(a_place, blocks), lax.rem(a_place, blocks)]
                        b = vk_in[lax.div(b_place, blocks), lax.rem(b_place, blocks)]
                        keys_here.append(jnp.where(low, a, b))
                        values_here.append(jnp.where(low, b, a))
                    made = lax.dot_general(
                        stacked, jnp.concatenate(keys_here, axis=0), (((1,), (1,)), ((), ())),
                        preferred_element_type=jnp.float32,
                    )
                    lines = []
                    for first in range(2):
                        lines.append(
                            jnp.concatenate(
                                [
                                    jnp.where(low_line, bias[s + first], bias[s + 2 + first])
                                    for s in range(lower, lower + 8, 4)
                                ],
                                axis=1,
                            )
                        )
                    scores.append((made[:BLK] + lines[0], made[BLK:] + lines[1]))
                    values.append(jnp.concatenate(values_here, axis=0))
                top = functools.reduce(jnp.maximum, [part for both in scores for part in both])
                top = jnp.max(top, axis=1, keepdims=True)
                total = 0.0
                made = 0.0
                for both, held_values in zip(scores, values):
                    weights = [jnp.exp(part - top) for part in both]
                    total = total + weights[0] + weights[1]
                    rounded = jnp.concatenate([part.astype(jnp.bfloat16) for part in weights], axis=0)
                    made = made + jnp.dot(rounded, held_values, preferred_element_type=jnp.float32)
                total = jnp.sum(total, axis=1, keepdims=True)
                if e == 0:
                    summed = swap_halves(made[:BLK]) + made[BLK:]
                else:
                    summed = made[:BLK] + swap_halves(made[BLK:])
                results.append(summed / total)
                logs = jnp.where(lane == r, top + jnp.log(total), logs)
            o_out[j, m] = jnp.where(low, results[0], results[1]).astype(jnp.bfloat16)
        lines = jnp.transpose(jnp.concatenate([logs, jnp.zeros_like(logs)], axis=0))
        l_out[j] = lines[:8]

    def serve(t, carry):
        other_group = group + lax.div(t, heads)
        j = other_group * heads + lax.rem(idx + t, heads)

        @pl.when(t > 0)
        def _():
            arrival(q_in.at[j], q_recv.at[j]).wait_recv()

        attend(j)

        @pl.when(t > 0)
        def _():
            o_copy(j).start()
            l_copy(j).start()

        @pl.when(t == 0)
        def _():
            for m in range(tiles):
                o_in[group, idx, m] = o_out[j, m]
            l_in[group, idx] = l_out[j]

        return carry

    lax.fori_loop(0, devices - first_device, serve, 0)

    def absent(a, carry):
        o_in[a] = jnp.zeros(o_in.shape[1:], o_in.dtype)
        l_in[a] = jnp.full(l_in.shape[1:], masked_score, jnp.float32)
        return carry

    lax.fori_loop(group + 1, groups, absent, 0)

    def take_results(k, carry):
        source = lax.rem(me + k, (group + 1) * heads)
        place = o_in.at[lax.div(source, heads), lax.rem(source, heads)]
        arrival(place, o_recv.at[source]).wait_recv()
        line = l_in.at[lax.div(source, heads), lax.rem(source, heads)]
        arrival(line, l_recv.at[source]).wait_recv()
        return carry

    lax.fori_loop(1, (group + 1) * heads, take_results, 0)

    load_o.wait()

    def spread(body, start):
        if groups <= 2:
            for a in range(groups):
                start = body(a, start)
            return start
        return lax.fori_loop(0, groups, body, start)

    highest = spread(lambda a, top: jnp.maximum(top, l_in[a]), jnp.full(l_in.shape[1:], masked_score, jnp.float32))
    sums = spread(lambda a, acc: acc + jnp.exp(l_in[a] - highest), jnp.zeros(l_in.shape[1:], jnp.float32))
    total_log[...] = highest + jnp.log(sums)
    for m in range(tiles):
        first, second = total_log[:, 2 * m, :], total_log[:, 2 * m + 1, :]
        log_ref[:, m * LANES : (m + 1) * LANES] = jnp.where(low_line, first, swap_halves(second))

    def columns(a):
        share = jnp.exp(l_in[a] - total_log[...]).reshape(heads * 8, LANES)
        missing = LANES - heads * 8
        if missing:
            share = jnp.concatenate([share, jnp.zeros((missing, LANES), jnp.float32)], axis=0)
        return jnp.transpose(share)

    def add_group(a, carry):
        weight[a] = columns(a)
        return carry

    spread(add_group, 0)
    for ch in range(pairs):
        for m in range(tiles):

            def add_part(a, sums, ch=ch, m=m):
                t0 = o_in[a, 2 * ch, m].astype(jnp.float32)
                t1 = o_in[a, 2 * ch + 1, m].astype(jnp.float32)
                parts = (jnp.where(low, t0, swap_halves(t1)), jnp.where(low, swap_halves(t0), t1))
                made = []
                for e in range(2):
                    at = 2 * ch * 8 + 2 * m + e
                    share = jnp.where(low, weight[a, :BLK, at : at + 1], weight[a, :BLK, at + 8 : at + 9])
                    made.append(sums[e] + parts[e] * share)
                return tuple(made)

            zero = jnp.zeros((BLK, LANES), jnp.float32)
            made = spread(add_part, (zero, zero))
            for e in range(2):
                r = 2 * m + e
                attended[r * BLK : (r + 1) * BLK, ch * LANES : (ch + 1) * LANES] = made[e].astype(jnp.bfloat16)

    out_rows = rows // splits
    tile_width = min(512, wo.shape[1])
    chunks = wo.shape[1] // tile_width
    peers = [lax.rem(tp + d, splits) for d in range(splits)]

    def partial_of(d, c):
        mine = attended[pl.ds(pl.multiple_of(peers[d] * out_rows, out_rows), out_rows), :]
        made = jnp.dot(mine, wo[:, c * tile_width : (c + 1) * tile_width], preferred_element_type=jnp.float32)
        return made.astype(jnp.bfloat16)

    def hop(d, c):
        return pltpu.make_async_remote_copy(
            src_ref=stage.at[d - 1, c],
            dst_ref=landed_ref.at[d - 1, c],
            send_sem=tp_send.at[d - 1, c],
            recv_sem=tp_recv.at[d - 1, c],
            device_id={"tp": peers[d]},
            device_id_type=MESH,
        )

    for d in range(1, splits):
        for c in range(chunks):
            stage[d - 1, c] = partial_of(d, c)
            hop(d, c).start()
    for c in range(chunks):
        mine_ref[c] = partial_of(0, c)

    def sent(copy):
        copy.wait_send()

    for i in range(pairs):
        for e in range(2):
            head = 2 * pair_of(i) + e

            def drain(i=i, e=e, head=head):
                kv_copy(2 * i + e, head).wait_send()
                q_copy(2 * i + e, first_device + head).wait_send()

            if i < pairs - 1:
                drain()
            else:
                pl.when(head != idx)(drain)

    def drain_down(a, carry):
        for i in range(pairs):
            for e in range(2):
                q_copy(2 * i + e, a * heads + 2 * pair_of(i) + e).wait_send()
        return carry

    lax.fori_loop(0, group, drain_down, 0)

    def drain_results(t, carry):
        j = (group + lax.div(t, heads)) * heads + lax.rem(idx + t, heads)
        o_copy(j).wait_send()
        l_copy(j).wait_send()
        return carry

    lax.fori_loop(1, devices - first_device, drain_results, 0)
    for d in range(1, splits):
        for c in range(chunks):
            hop(d, c).wait()


def local(devices, splits, tokens, w_query, w_key, w_value, w_out, chosen):
    rows, depth = tokens.shape
    width = w_query.shape[1]
    out_width = w_out.shape[1]
    heads = width // HEAD_DIM
    pairs = heads // 2
    groups = devices // heads
    blocks = rows // BLK
    tiles = blocks // 2
    half = HEAD_DIM // 2
    wide = 2 if pairs % 2 == 0 else 1

    inverse = rotary_base ** (-np.arange(half, dtype=np.float64) / half)
    within = np.tile(np.arange(rows)[:, None] * inverse[None, :], (1, LANES // half))
    start = np.tile((np.arange(devices) * rows)[:, None] * inverse[None, :], (1, LANES // half))
    cos_table = jnp.asarray(np.cos(within), jnp.float32)
    sin_table = jnp.asarray(np.sin(within), jnp.float32)
    base = jnp.asarray(np.stack([np.cos(start), np.sin(start)]), jnp.float32)

    out_rows = rows // splits
    tile_width = min(512, out_width)
    chunks = out_width // tile_width
    dma = pltpu.SemaphoreType.DMA
    bf16, f32 = jnp.bfloat16, jnp.float32
    mine, landed, logs = pl.pallas_call(
        functools.partial(layer_kernel, devices, splits),
        in_specs=[in_smem()] + [in_hbm()] * 7 + [in_vmem()],
        out_specs=[in_vmem()] * 3,
        out_shape=[
            jax.ShapeDtypeStruct((chunks, out_rows, tile_width), bf16),
            jax.ShapeDtypeStruct((splits - 1, chunks, out_rows, tile_width), bf16),
            jax.ShapeDtypeStruct((heads, rows), f32),
        ],
        scratch_shapes=[
            pltpu.VMEM((rows, depth), bf16),
            pltpu.VMEM((pairs // wide, depth, wide * LANES), bf16),
            pltpu.VMEM((pairs, depth, 2 * LANES), bf16),
            pltpu.VMEM((width, out_width), bf16),
            pltpu.VMEM((rows, LANES), f32),
            pltpu.VMEM((rows, LANES), f32),
            pltpu.VMEM((heads, blocks, BLK, LANES), bf16),
            pltpu.VMEM((heads, tiles, BLK, LANES), bf16),
            pltpu.VMEM((heads, blocks, BLK, LANES), bf16),
            pltpu.VMEM((heads, blocks, BLK, LANES), bf16),
            pltpu.VMEM((devices, tiles, BLK, LANES), bf16),
            pltpu.VMEM((devices, tiles, BLK, LANES), bf16),
            pltpu.VMEM((devices, 8, LANES), f32),
            pltpu.VMEM((groups, heads, tiles, BLK, LANES), bf16),
            pltpu.VMEM((groups, heads, 8, LANES), f32),
            pltpu.VMEM((groups, LANES, LANES), f32),
            pltpu.VMEM((heads, 8, LANES), f32),
            pltpu.VMEM((rows, width), bf16),
            pltpu.VMEM((splits - 1, chunks, out_rows, tile_width), bf16),
            dma((7, pairs)),
            dma((heads,)),
            dma((heads,)),
            dma((devices,)),
            dma((devices,)),
            dma((devices,)),
            dma((devices,)),
            dma((devices,)),
            dma((devices,)),
            dma((splits - 1, chunks)),
            dma((splits - 1, chunks)),
        ],
        compiler_params=pltpu.CompilerParams(
            collective_id=0, has_side_effects=True, vmem_limit_bytes=VMEM_LIMIT
        ),
        name="layer",
    )(jnp.transpose(chosen), tokens, w_query, w_key, w_value, w_out, cos_table, sin_table, base)
    total = mine.astype(f32) + jnp.sum(landed.astype(f32), axis=0)
    mixed = jnp.transpose(total.astype(bf16), (1, 0, 2)).reshape(out_rows, out_width)
    return mixed, logs


def solution(mesh):
    placed = (P("kv", None), P(None, "tp"), P(None, "tp"), P(None, "tp"), P("tp", None), P())
    return jax.shard_map(
        functools.partial(local, mesh.shape["kv"], mesh.shape["tp"]),
        mesh=mesh,
        in_specs=placed,
        out_specs=(P(("kv", "tp"), None), P("tp", "kv")),
        check_vma=False,
    )
```

```python
import functools

import jax
import jax.numpy as jnp
import numpy as np
from jax import lax
from jax.experimental import pallas as pl
from jax.experimental.pallas import tpu as pltpu
from jax.sharding import PartitionSpec as P

HEAD_DIM = 64
BLK = 64
LANES = 128
VMEM_LIMIT = 65_000_000
AHEAD = 2

rotary_base = 500000.0
masked_score = -1e30

MESH = pl.DeviceIdType.MESH


def in_vmem():
    return pl.BlockSpec(memory_space=pltpu.VMEM)


def in_hbm():
    return pl.BlockSpec(memory_space=pltpu.HBM)


def swap_halves(tile):
    return pltpu.roll(tile, LANES // 2, 1)


def layer_kernel(
    devices, splits, chosen_ref, x_ref, wq_ref, wk_ref, wv_ref, wo_ref, cos_ref, sin_ref, base_ref,
    mine_ref, landed_ref, log_ref,
    x, wq, wkv, wo, cos_t, sin_t, kv_out, q_out, kv_in, vk_in, lists, place_v, place_s, bias, q_in, o_out, l_out, o_in, l_in, weight, total_log,
    attended, stage, load_sem, kv_send, kv_recv, q_send, q_recv, o_send, o_recv, l_send, l_recv, tp_send, tp_recv,
):
    heads = kv_out.shape[0]
    pairs = heads // 2
    groups = devices // heads
    blocks = kv_out.shape[1]
    tiles = blocks // 2
    rows = blocks * BLK
    entries = chosen_ref.shape[0]
    table_blocks = heads * blocks
    wide = wq.shape[2] // LANES

    me = lax.axis_index("kv")
    tp = lax.axis_index("tp")
    group = lax.div(me, heads)
    idx = lax.rem(me, heads)
    first_device = group * heads
    half = HEAD_DIM // 2

    def pair_of(i):
        return lax.rem(lax.div(idx, 2) + 1 + i, pairs)

    def strip(ref, i):
        return ref.at[:, pl.ds(pl.multiple_of(pair_of(i) * LANES, LANES), LANES)]

    def load_q(i):
        target = wq.at[i // wide, :, pl.ds((i % wide) * LANES, LANES)]
        return pltpu.make_async_copy(strip(wq_ref, i), target, load_sem.at[0, i])

    def load_k(i):
        return pltpu.make_async_copy(strip(wk_ref, i), wkv.at[i, :, pl.ds(0, LANES)], load_sem.at[1, i])

    def load_v(i):
        return pltpu.make_async_copy(strip(wv_ref, i), wkv.at[i, :, pl.ds(LANES, LANES)], load_sem.at[2, i])

    load_x = pltpu.make_async_copy(x_ref, x, load_sem.at[3, 0])
    load_cos = pltpu.make_async_copy(cos_ref, cos_t, load_sem.at[4, 0])
    load_sin = pltpu.make_async_copy(sin_ref, sin_t, load_sem.at[5, 0])
    load_o = pltpu.make_async_copy(wo_ref, wo, load_sem.at[6, 0])

    load_lists = pltpu.make_async_copy(chosen_ref, lists, load_sem.at[7, 0])
    move_places = pltpu.make_async_copy(place_v, place_s, load_sem.at[8, 0])

    load_x.start()
    load_lists.start()
    load_cos.start()
    load_sin.start()
    for i in range(pairs):
        load_k(i).start()
        load_v(i).start()
        if i % wide == 0:
            for e in range(wide):
                load_q(i + e).start()
    load_o.start()

    barrier = pltpu.get_barrier_semaphore()

    def greet(d, carry):
        pl.semaphore_signal(
            barrier, inc=1, device_id={"kv": lax.rem(me + d, devices)}, device_id_type=MESH
        )
        return carry

    lax.fori_loop(1, devices, greet, 0)
    for d in range(1, splits):
        pl.semaphore_signal(barrier, inc=1, device_id={"tp": lax.rem(tp + d, splits)}, device_id_type=MESH)

    def kv_copy(slot, head):
        return pltpu.make_async_remote_copy(
            src_ref=kv_out.at[slot],
            dst_ref=kv_in.at[pl.ds(idx * blocks, blocks)],
            send_sem=kv_send.at[head],
            recv_sem=kv_recv.at[idx],
            device_id={"kv": first_device + head},
            device_id_type=MESH,
        )

    def q_copy(slot, target):
        return pltpu.make_async_remote_copy(
            src_ref=q_out.at[slot],
            dst_ref=q_in.at[me],
            send_sem=q_send.at[target],
            recv_sem=q_recv.at[me],
            device_id={"kv": target},
            device_id_type=MESH,
        )

    def o_copy(target):
        return pltpu.make_async_remote_copy(
            src_ref=o_out.at[target],
            dst_ref=o_in.at[group, idx],
            send_sem=o_send.at[target],
            recv_sem=o_recv.at[me],
            device_id={"kv": target},
            device_id_type=MESH,
        )

    def l_copy(target):
        return pltpu.make_async_remote_copy(
            src_ref=l_out.at[target],
            dst_ref=l_in.at[group, idx],
            send_sem=l_send.at[target],
            recv_sem=l_recv.at[me],
            device_id={"kv": target},
            device_id_type=MESH,
        )

    def arrival(copy, semaphore):
        return pltpu.make_async_remote_copy(
            src_ref=copy, dst_ref=copy, send_sem=semaphore, recv_sem=semaphore,
            device_id={"kv": me}, device_id_type=MESH,
        )

    load_x.wait()
    load_cos.wait()
    load_sin.wait()
    low_rows = lax.broadcasted_iota(jnp.int32, (rows, LANES), 1) < LANES // 2
    turn_low = lax.broadcasted_iota(jnp.int32, (rows, LANES), 1) % HEAD_DIM < half
    cos_base = base_ref[0, pl.ds(me, 1), :]
    sin_base = base_ref[1, pl.ds(me, 1), :]
    cos_part = cos_t[...] * cos_base - sin_t[...] * sin_base
    sin_part = sin_t[...] * cos_base + cos_t[...] * sin_base
    sin_part = jnp.where(turn_low, -sin_part, sin_part)

    def turned(part):
        other = jnp.where(turn_low, pltpu.roll(part, LANES - half, 1), pltpu.roll(part, half, 1))
        return part * cos_part + other * sin_part

    def make_kv(i):
        load_k(i).wait()
        load_v(i).wait()
        made = jnp.dot(x[...], wkv[i], preferred_element_type=jnp.float32)
        keys = turned(made[:, :LANES])
        values = made[:, LANES:]
        even = jnp.where(low_rows, keys, swap_halves(values)).astype(jnp.bfloat16)
        odd = jnp.where(low_rows, swap_halves(keys), values).astype(jnp.bfloat16)
        for r in range(blocks):
            kv_out[2 * i, r] = even[r * BLK : (r + 1) * BLK]
            kv_out[2 * i + 1, r] = odd[r * BLK : (r + 1) * BLK]

    def make_q(i):
        for e in range(wide):
            load_q(i + e).wait()
        made = jnp.dot(x[...], wq[i // wide], preferred_element_type=jnp.float32)
        for e in range(wide):
            part = turned(made[:, e * LANES : (e + 1) * LANES]) * (HEAD_DIM**-0.5)
            swapped = swap_halves(part)
            low = low_rows[:BLK]
            for m in range(tiles):
                a = slice(2 * m * BLK, (2 * m + 1) * BLK)
                b = slice((2 * m + 1) * BLK, (2 * m + 2) * BLK)
                q_out[2 * (i + e), m] = jnp.where(low, part[a], swapped[b]).astype(jnp.bfloat16)
                q_out[2 * (i + e) + 1, m] = jnp.where(low, swapped[a], part[b]).astype(jnp.bfloat16)

    def send_kv(i):
        for e in range(2):
            head = 2 * pair_of(i) + e
            if i < pairs - 1:
                kv_copy(2 * i + e, head).start()
            else:
                pl.when(head != idx)(lambda e=e, head=head: kv_copy(2 * i + e, head).start())

    def send_q(i):
        for e in range(2):
            head = 2 * pair_of(i) + e
            if i < pairs - 1:
                q_copy(2 * i + e, first_device + head).start()
            else:
                pl.when(head != idx)(lambda e=e, head=head: q_copy(2 * i + e, first_device + head).start())

    for i in range(pairs):
        make_kv(i)
        if i == 0:
            pl.semaphore_wait(barrier, devices - 1 + splits - 1)
        send_kv(i)
        if i % wide == 0:
            make_q(i)
        send_q(i)

    def send_down(a, carry):
        for i in range(pairs):
            for e in range(2):
                q_copy(2 * i + e, a * heads + 2 * pair_of(i) + e).start()
        return carry

    lax.fori_loop(0, group, send_down, 0)

    load_lists.wait()
    place = lists[...] - first_device * blocks
    held = (place >= 0) & (place < table_blocks)
    place_v[...] = jnp.where(held, place, 0)
    move_places.start()
    column = lax.broadcasted_iota(jnp.int32, (entries, entries * BLK), 1)
    slot = column // (8 * BLK) * 8 + column // BLK % 4 * 2 + column // (4 * BLK) % 2
    unit = (slot == lax.broadcasted_iota(jnp.int32, slot.shape, 0)).astype(jnp.float32)
    bias[...] = masked_score * (
        1.0
        - lax.dot_general(
            jnp.where(held, 1.0, 0.0), unit, (((0,), (0,)), ((), ())), preferred_element_type=jnp.float32
        )
    )
    move_places.wait()

    own_slot = 2 * (pairs - 1) + lax.rem(idx, 2)
    for r in range(blocks):
        kv_in[idx * blocks + r] = kv_out[own_slot, r]
    for m in range(tiles):
        q_in[me, m] = q_out[own_slot, m]

    low = lax.broadcasted_iota(jnp.int32, (BLK, LANES), 1) < LANES // 2
    lane = lax.broadcasted_iota(jnp.int32, (BLK, LANES), 1)
    low_line = lax.broadcasted_iota(jnp.int32, (1, LANES), 1) < LANES // 2

    def take_kv(k, carry):
        source = lax.rem(idx + k, heads)

        @pl.when(k > 0)
        def _():
            arrival(kv_in.at[pl.ds(source * blocks, blocks)], kv_recv.at[source]).wait_recv()

        for r in range(blocks):
            place = source * blocks + r
            vk_in[place] = swap_halves(kv_in[place].astype(jnp.float32)).astype(jnp.bfloat16)
        return carry

    lax.fori_loop(0, heads, take_kv, 0)

    def attend(j):
        stacks = []
        for m in range(tiles):
            tile = q_in[j, m]
            swapped = swap_halves(tile.astype(jnp.float32)).astype(jnp.bfloat16)
            none = jnp.zeros_like(tile)
            for at_low, at_high in ((tile, swapped), (swapped, tile)):
                stacks.append(jnp.concatenate([jnp.where(low, at_low, none), jnp.where(low, none, at_high)], axis=0))

        def score(r):
            scores, values = [], []
            for lower in range(0, entries, 8):
                keys_here, values_here = [], []
                for s in range(lower, lower + 8, 2):
                    a = kv_in[place_s[s, j * blocks + r]]
                    b = vk_in[place_s[s + 1, j * blocks + r]]
                    keys_here.append(jnp.where(low, a, b))
                    values_here.append(jnp.where(low, b, a))
                made = lax.dot_general(
                    stacks[r], jnp.concatenate(keys_here, axis=0), (((1,), (1,)), ((), ())),
                    preferred_element_type=jnp.float32,
                )
                line = bias[pl.ds(j * blocks + r, 1), lower * BLK : (lower + 8) * BLK]
                scores += [made[:BLK] + line[:, : 4 * BLK], made[BLK:] + line[:, 4 * BLK :]]
                values.append(jnp.concatenate(values_here, axis=0))
            top = jnp.max(functools.reduce(jnp.maximum, scores), axis=1, keepdims=True)
            return scores, values, top

        def gather(r, scores, values, top):
            weights = [jnp.exp(part - top) for part in scores]
            total = jnp.sum(functools.reduce(jnp.add, weights), axis=1, keepdims=True)
            made = 0.0
            for k, held_values in enumerate(values):
                rounded = jnp.concatenate([part.astype(jnp.bfloat16) for part in weights[2 * k : 2 * k + 2]], axis=0)
                made = made + jnp.dot(rounded, held_values, preferred_element_type=jnp.float32)
            if r % 2 == 0:
                summed = swap_halves(made[:BLK]) + made[BLK:]
            else:
                summed = made[:BLK] + swap_halves(made[BLK:])
            return summed / total, top + jnp.log(total)

        ready, results = [], []
        for r in range(blocks + AHEAD):
            if r < blocks:
                ready.append(score(r))
            if r >= AHEAD:
                results.append(gather(r - AHEAD, *ready[r - AHEAD]))
        logs = jnp.zeros((BLK, LANES), jnp.float32)
        for r in range(blocks):
            logs = jnp.where(lane == r, results[r][1], logs)
        for m in range(tiles):
            o_out[j, m] = jnp.where(low, results[2 * m][0], results[2 * m + 1][0]).astype(jnp.bfloat16)
        lines = jnp.transpose(jnp.concatenate([logs, jnp.zeros_like(logs)], axis=0))
        l_out[j] = lines[:8]

    def serve(t, carry):
        other_group = group + lax.div(t, heads)
        j = other_group * heads + lax.rem(idx + t, heads)

        @pl.when(t > 0)
        def _():
            arrival(q_in.at[j], q_recv.at[j]).wait_recv()

        attend(j)

        @pl.when(t > 0)
        def _():
            o_copy(j).start()
            l_copy(j).start()

        @pl.when(t == 0)
        def _():
            for m in range(tiles):
                o_in[group, idx, m] = o_out[j, m]
            l_in[group, idx] = l_out[j]

        return carry

    lax.fori_loop(0, devices - first_device, serve, 0)

    def absent(a, carry):
        o_in[a] = jnp.zeros(o_in.shape[1:], o_in.dtype)
        l_in[a] = jnp.full(l_in.shape[1:], masked_score, jnp.float32)
        return carry

    lax.fori_loop(group + 1, groups, absent, 0)

    def take_results(k, carry):
        source = lax.rem(me + k, (group + 1) * heads)
        place = o_in.at[lax.div(source, heads), lax.rem(source, heads)]
        arrival(place, o_recv.at[source]).wait_recv()
        line = l_in.at[lax.div(source, heads), lax.rem(source, heads)]
        arrival(line, l_recv.at[source]).wait_recv()
        return carry

    lax.fori_loop(1, (group + 1) * heads, take_results, 0)

    load_o.wait()

    def spread(body, start):
        if groups <= 2:
            for a in range(groups):
                start = body(a, start)
            return start
        return lax.fori_loop(0, groups, body, start)

    highest = spread(lambda a, top: jnp.maximum(top, l_in[a]), jnp.full(l_in.shape[1:], masked_score, jnp.float32))
    sums = spread(lambda a, acc: acc + jnp.exp(l_in[a] - highest), jnp.zeros(l_in.shape[1:], jnp.float32))
    total_log[...] = highest + jnp.log(sums)
    for m in range(tiles):
        first, second = total_log[:, 2 * m, :], total_log[:, 2 * m + 1, :]
        log_ref[:, m * LANES : (m + 1) * LANES] = jnp.where(low_line, first, swap_halves(second))

    def columns(a):
        share = jnp.exp(l_in[a] - total_log[...]).reshape(heads * 8, LANES)
        missing = LANES - heads * 8
        if missing:
            share = jnp.concatenate([share, jnp.zeros((missing, LANES), jnp.float32)], axis=0)
        return jnp.transpose(share)

    def add_group(a, carry):
        weight[a] = columns(a)
        return carry

    spread(add_group, 0)
    for ch in range(pairs):
        for m in range(tiles):

            def add_part(a, sums, ch=ch, m=m):
                t0 = o_in[a, 2 * ch, m].astype(jnp.float32)
                t1 = o_in[a, 2 * ch + 1, m].astype(jnp.float32)
                parts = (jnp.where(low, t0, swap_halves(t1)), jnp.where(low, swap_halves(t0), t1))
                made = []
                for e in range(2):
                    at = 2 * ch * 8 + 2 * m + e
                    share = jnp.where(low, weight[a, :BLK, at : at + 1], weight[a, :BLK, at + 8 : at + 9])
                    made.append(sums[e] + parts[e] * share)
                return tuple(made)

            zero = jnp.zeros((BLK, LANES), jnp.float32)
            made = spread(add_part, (zero, zero))
            for e in range(2):
                r = 2 * m + e
                attended[r * BLK : (r + 1) * BLK, ch * LANES : (ch + 1) * LANES] = made[e].astype(jnp.bfloat16)

    out_rows = rows // splits
    tile_width = min(512, wo.shape[1])
    chunks = wo.shape[1] // tile_width
    peers = [lax.rem(tp + d, splits) for d in range(splits)]

    def partial_of(d, c):
        mine = attended[pl.ds(pl.multiple_of(peers[d] * out_rows, out_rows), out_rows), :]
        made = jnp.dot(mine, wo[:, c * tile_width : (c + 1) * tile_width], preferred_element_type=jnp.float32)
        return made.astype(jnp.bfloat16)

    def hop(d, c):
        return pltpu.make_async_remote_copy(
            src_ref=stage.at[d - 1, c],
            dst_ref=landed_ref.at[d - 1, :, pl.ds(c * tile_width, tile_width)],
            send_sem=tp_send.at[d - 1, c],
            recv_sem=tp_recv.at[d - 1, c],
            device_id={"tp": peers[d]},
            device_id_type=MESH,
        )

    for d in range(1, splits):
        for c in range(chunks):
            stage[d - 1, c] = partial_of(d, c)
            hop(d, c).start()
    for c in range(chunks):
        mine_ref[:, c * tile_width : (c + 1) * tile_width] = partial_of(0, c)

    def sent(copy):
        copy.wait_send()

    for i in range(pairs):
        for e in range(2):
            head = 2 * pair_of(i) + e

            def drain(i=i, e=e, head=head):
                kv_copy(2 * i + e, head).wait_send()
                q_copy(2 * i + e, first_device + head).wait_send()

            if i < pairs - 1:
                drain()
            else:
                pl.when(head != idx)(drain)

    def drain_down(a, carry):
        for i in range(pairs):
            for e in range(2):
                q_copy(2 * i + e, a * heads + 2 * pair_of(i) + e).wait_send()
        return carry

    lax.fori_loop(0, group, drain_down, 0)

    def drain_results(t, carry):
        j = (group + lax.div(t, heads)) * heads + lax.rem(idx + t, heads)
        o_copy(j).wait_send()
        l_copy(j).wait_send()
        return carry

    lax.fori_loop(1, devices - first_device, drain_results, 0)
    for d in range(1, splits):
        for c in range(chunks):
            hop(d, c).wait()


def local(devices, splits, tokens, w_query, w_key, w_value, w_out, chosen):
    rows, depth = tokens.shape
    width = w_query.shape[1]
    out_width = w_out.shape[1]
    heads = width // HEAD_DIM
    pairs = heads // 2
    groups = devices // heads
    blocks = rows // BLK
    tiles = blocks // 2
    half = HEAD_DIM // 2
    wide = 2 if pairs % 2 == 0 else 1

    inverse = rotary_base ** (-np.arange(half, dtype=np.float64) / half)
    within = np.tile(np.arange(rows)[:, None] * inverse[None, :], (1, LANES // half))
    start = np.tile((np.arange(devices) * rows)[:, None] * inverse[None, :], (1, LANES // half))
    cos_table = jnp.asarray(np.cos(within), jnp.float32)
    sin_table = jnp.asarray(np.sin(within), jnp.float32)
    base = jnp.asarray(np.stack([np.cos(start), np.sin(start)]), jnp.float32)

    out_rows = rows // splits
    tile_width = min(512, out_width)
    chunks = out_width // tile_width
    dma = pltpu.SemaphoreType.DMA
    bf16, f32 = jnp.bfloat16, jnp.float32
    mine, landed, logs = pl.pallas_call(
        functools.partial(layer_kernel, devices, splits),
        in_specs=[in_hbm()] * 8 + [in_vmem()],
        out_specs=[in_vmem()] * 3,
        out_shape=[
            jax.ShapeDtypeStruct((out_rows, out_width), bf16),
            jax.ShapeDtypeStruct((splits - 1, out_rows, out_width), bf16),
            jax.ShapeDtypeStruct((heads, rows), f32),
        ],
        scratch_shapes=[
            pltpu.VMEM((rows, depth), bf16),
            pltpu.VMEM((pairs // wide, depth, wide * LANES), bf16),
            pltpu.VMEM((pairs, depth, 2 * LANES), bf16),
            pltpu.VMEM((width, out_width), bf16),
            pltpu.VMEM((rows, LANES), f32),
            pltpu.VMEM((rows, LANES), f32),
            pltpu.VMEM((heads, blocks, BLK, LANES), bf16),
            pltpu.VMEM((heads, tiles, BLK, LANES), bf16),
            pltpu.VMEM((heads * blocks, BLK, LANES), bf16),
            pltpu.VMEM((heads * blocks, BLK, LANES), bf16),
            pltpu.VMEM(chosen.shape[::-1], jnp.int32),
            pltpu.VMEM(chosen.shape[::-1], jnp.int32),
            pltpu.SMEM(chosen.shape[::-1], jnp.int32),
            pltpu.VMEM((chosen.shape[0], chosen.shape[1] * BLK), f32),
            pltpu.VMEM((devices, tiles, BLK, LANES), bf16),
            pltpu.VMEM((devices, tiles, BLK, LANES), bf16),
            pltpu.VMEM((devices, 8, LANES), f32),
            pltpu.VMEM((groups, heads, tiles, BLK, LANES), bf16),
            pltpu.VMEM((groups, heads, 8, LANES), f32),
            pltpu.VMEM((groups, LANES, LANES), f32),
            pltpu.VMEM((heads, 8, LANES), f32),
            pltpu.VMEM((rows, width), bf16),
            pltpu.VMEM((splits - 1, chunks, out_rows, tile_width), bf16),
            dma((9, pairs)),
            dma((heads,)),
            dma((heads,)),
            dma((devices,)),
            dma((devices,)),
            dma((devices,)),
            dma((devices,)),
            dma((devices,)),
            dma((devices,)),
            dma((splits - 1, chunks)),
            dma((splits - 1, chunks)),
        ],
        compiler_params=pltpu.CompilerParams(
            collective_id=0, has_side_effects=True, vmem_limit_bytes=VMEM_LIMIT
        ),
        name="layer",
    )(jnp.transpose(chosen), tokens, w_query, w_key, w_value, w_out, cos_table, sin_table, base)
    total = mine.astype(f32) + jnp.sum(landed.astype(f32), axis=0)
    return total.astype(bf16), logs


def solution(mesh):
    placed = (P("kv", None), P(None, "tp"), P(None, "tp"), P(None, "tp"), P("tp", None), P())
    return jax.shard_map(
        functools.partial(local, mesh.shape["kv"], mesh.shape["tp"]),
        mesh=mesh,
        in_specs=placed,
        out_specs=(P(("kv", "tp"), None), P("tp", "kv")),
        check_vma=False,
    )
```

```python
import functools

import jax
import jax.numpy as jnp
import numpy as np
from jax import lax
from jax.experimental import pallas as pl
from jax.experimental.pallas import tpu as pltpu
from jax.sharding import PartitionSpec as P

HEAD_DIM = 64
BLK = 64
LANES = 128
VMEM_LIMIT = 55_000_000
AHEAD = 2

rotary_base = 500000.0
masked_score = -1e30

MESH = pl.DeviceIdType.MESH


def in_vmem():
    return pl.BlockSpec(memory_space=pltpu.VMEM)


def in_hbm():
    return pl.BlockSpec(memory_space=pltpu.HBM)


def swap_halves(tile):
    return pltpu.roll(tile, LANES // 2, 1)


def layer_kernel(
    devices, splits, chosen_ref, x_ref, wq_ref, wk_ref, wv_ref, wo_ref,
    mine_ref, landed_ref, log_ref,
    x, wq, wkv, wo, kv_out, q_out, kv_in, vk_in, place_v, place_s, bias, q_in, o_out, l_out, o_in, l_in, weight, total_log,
    attended, stage, load_sem, kv_send, kv_recv, q_send, q_recv, o_send, o_recv, l_send, l_recv, tp_send, tp_recv,
):
    heads = kv_out.shape[0]
    pairs = heads // 2
    groups = devices // heads
    blocks = kv_out.shape[1]
    tiles = blocks // 2
    rows = blocks * BLK
    entries = chosen_ref.shape[0]
    table_blocks = heads * blocks
    wide = wq.shape[2] // LANES

    me = lax.axis_index("kv")
    tp = lax.axis_index("tp")
    group = lax.div(me, heads)
    idx = lax.rem(me, heads)
    first_device = group * heads
    half = HEAD_DIM // 2

    def pair_of(i):
        return lax.rem(lax.div(idx, 2) + pairs - i, pairs)

    def strip(ref, i):
        return ref.at[:, pl.ds(pl.multiple_of(pair_of(i) * LANES, LANES), LANES)]

    def load_q(i):
        target = wq.at[i // wide, :, pl.ds((i % wide) * LANES, LANES)]
        return pltpu.make_async_copy(strip(wq_ref, i), target, load_sem.at[0, i])

    def load_k(i):
        return pltpu.make_async_copy(strip(wk_ref, i), wkv.at[i, :, pl.ds(0, LANES)], load_sem.at[1, i])

    def load_v(i):
        return pltpu.make_async_copy(strip(wv_ref, i), wkv.at[i, :, pl.ds(LANES, LANES)], load_sem.at[2, i])

    load_x = pltpu.make_async_copy(x_ref, x, load_sem.at[3, 0])
    load_o = pltpu.make_async_copy(wo_ref, wo, load_sem.at[4, 0])

    move_places = pltpu.make_async_copy(place_v, place_s, load_sem.at[6, 0])

    load_x.start()
    for i in range(pairs):
        load_k(i).start()
        load_v(i).start()
    for i in range(pairs):
        load_q(i).start()
    load_o.start()

    barrier = pltpu.get_barrier_semaphore()

    def greet(d, carry):
        pl.semaphore_signal(
            barrier, inc=1, device_id={"kv": lax.rem(me + d, devices)}, device_id_type=MESH
        )
        return carry

    lax.fori_loop(1, devices, greet, 0)
    for d in range(1, splits):
        pl.semaphore_signal(barrier, inc=1, device_id={"tp": lax.rem(tp + d, splits)}, device_id_type=MESH)

    def kv_copy(slot, head):
        return pltpu.make_async_remote_copy(
            src_ref=kv_out.at[slot],
            dst_ref=kv_in.at[pl.ds(idx * blocks, blocks)],
            send_sem=kv_send.at[head],
            recv_sem=kv_recv.at[idx],
            device_id={"kv": first_device + head},
            device_id_type=MESH,
        )

    def q_copy(slot, target):
        return pltpu.make_async_remote_copy(
            src_ref=q_out.at[slot],
            dst_ref=q_in.at[me],
            send_sem=q_send.at[target],
            recv_sem=q_recv.at[me],
            device_id={"kv": target},
            device_id_type=MESH,
        )

    def o_copy(target):
        return pltpu.make_async_remote_copy(
            src_ref=o_out.at[target],
            dst_ref=o_in.at[group, idx],
            send_sem=o_send.at[target],
            recv_sem=o_recv.at[me],
            device_id={"kv": target},
            device_id_type=MESH,
        )

    def l_copy(target):
        return pltpu.make_async_remote_copy(
            src_ref=l_out.at[target],
            dst_ref=l_in.at[group, idx],
            send_sem=l_send.at[target],
            recv_sem=l_recv.at[me],
            device_id={"kv": target},
            device_id_type=MESH,
        )

    def arrival(copy, semaphore):
        return pltpu.make_async_remote_copy(
            src_ref=copy, dst_ref=copy, send_sem=semaphore, recv_sem=semaphore,
            device_id={"kv": me}, device_id_type=MESH,
        )

    load_x.wait()
    low_rows = lax.broadcasted_iota(jnp.int32, (rows, LANES), 1) < LANES // 2
    turn_low = lax.broadcasted_iota(jnp.int32, (rows, LANES), 1) % HEAD_DIM < half

    def angles(count, step, start):
        channel = (lax.broadcasted_iota(jnp.int32, (count, LANES), 1) % half).astype(jnp.float32)
        position = lax.broadcasted_iota(jnp.int32, (count, LANES), 0) * step + start
        turn = position.astype(jnp.float32) * jnp.exp(channel * (-np.log(rotary_base) / half))
        return jnp.cos(turn), jnp.sin(turn)

    cos_fine, sin_fine = angles(8, 1, 0)
    cos_coarse, sin_coarse = angles(rows // 8, 8, me * rows)
    cos_parts, sin_parts = [], []
    for k in range(rows // 8):
        cos_k, sin_k = cos_coarse[k : k + 1], sin_coarse[k : k + 1]
        cos_parts.append(cos_k * cos_fine - sin_k * sin_fine)
        sin_parts.append(sin_k * cos_fine + cos_k * sin_fine)
    cos_part = jnp.concatenate(cos_parts, axis=0)
    sin_part = jnp.concatenate(sin_parts, axis=0)
    sin_part = jnp.where(turn_low, -sin_part, sin_part)

    def turned(part):
        other = jnp.where(turn_low, pltpu.roll(part, LANES - half, 1), pltpu.roll(part, half, 1))
        return part * cos_part + other * sin_part

    def make_kv(i):
        load_k(i).wait()
        load_v(i).wait()
        made = jnp.dot(x[...], wkv[i], preferred_element_type=jnp.float32)
        keys = turned(made[:, :LANES])
        values = made[:, LANES:]
        even = jnp.where(low_rows, keys, swap_halves(values)).astype(jnp.bfloat16)
        odd = jnp.where(low_rows, swap_halves(keys), values).astype(jnp.bfloat16)
        for r in range(blocks):
            kv_out[2 * i, r] = even[r * BLK : (r + 1) * BLK]
            kv_out[2 * i + 1, r] = odd[r * BLK : (r + 1) * BLK]

    def make_q(i):
        for e in range(wide):
            load_q(i + e).wait()
        made = jnp.dot(x[...], wq[i // wide], preferred_element_type=jnp.float32)
        for e in range(wide):
            part = turned(made[:, e * LANES : (e + 1) * LANES]) * (HEAD_DIM**-0.5)
            swapped = swap_halves(part)
            low = low_rows[:BLK]
            for m in range(tiles):
                a = slice(2 * m * BLK, (2 * m + 1) * BLK)
                b = slice((2 * m + 1) * BLK, (2 * m + 2) * BLK)
                q_out[2 * (i + e), m] = jnp.where(low, part[a], swapped[b]).astype(jnp.bfloat16)
                q_out[2 * (i + e) + 1, m] = jnp.where(low, swapped[a], part[b]).astype(jnp.bfloat16)

    def send_kv(i):
        for e in range(2):
            head = 2 * pair_of(i) + e
            if i > 0:
                kv_copy(2 * i + e, head).start()
            else:
                pl.when(head != idx)(lambda e=e, head=head: kv_copy(2 * i + e, head).start())

    def send_q(i):
        for e in range(2):
            head = 2 * pair_of(i) + e
            if i > 0:
                q_copy(2 * i + e, first_device + head).start()
            else:
                pl.when(head != idx)(lambda e=e, head=head: q_copy(2 * i + e, first_device + head).start())

    for i in range(pairs):
        make_kv(i)
        if i == 0:
            pl.semaphore_wait(barrier, devices - 1 + splits - 1)
        send_kv(i)
    for i in range(0, pairs, wide):
        make_q(i)
        for e in range(wide):
            send_q(i + e)

    def send_down(a, carry):
        for i in range(pairs):
            for e in range(2):
                q_copy(2 * i + e, a * heads + 2 * pair_of(i) + e).start()
        return carry

    lax.fori_loop(0, group, send_down, 0)

    place = chosen_ref[...] - first_device * blocks
    held = (place >= 0) & (place < table_blocks)
    place_v[...] = jnp.where(held, place, 0)
    move_places.start()
    column = lax.broadcasted_iota(jnp.int32, (entries, entries * BLK), 1)
    slot = column // (8 * BLK) * 8 + column // BLK % 4 * 2 + column // (4 * BLK) % 2
    unit = (slot == lax.broadcasted_iota(jnp.int32, slot.shape, 0)).astype(jnp.float32)
    bias[...] = masked_score * (
        1.0
        - lax.dot_general(
            jnp.where(held, 1.0, 0.0), unit, (((0,), (0,)), ((), ())), preferred_element_type=jnp.float32
        )
    )
    move_places.wait()

    own_slot = lax.rem(idx, 2)
    for r in range(blocks):
        kv_in[idx * blocks + r] = kv_out[own_slot, r]
    for m in range(tiles):
        q_in[me, m] = q_out[own_slot, m]

    low = lax.broadcasted_iota(jnp.int32, (BLK, LANES), 1) < LANES // 2
    lane = lax.broadcasted_iota(jnp.int32, (BLK, LANES), 1)
    low_line = lax.broadcasted_iota(jnp.int32, (1, LANES), 1) < LANES // 2

    def take_kv(k, carry):
        source = lax.rem(idx + k, heads)

        @pl.when(k > 0)
        def _():
            arrival(kv_in.at[pl.ds(source * blocks, blocks)], kv_recv.at[source]).wait_recv()

        for r in range(blocks):
            place = source * blocks + r
            vk_in[place] = swap_halves(kv_in[place].astype(jnp.float32)).astype(jnp.bfloat16)
        return carry

    lax.fori_loop(0, heads, take_kv, 0)

    def attend(j):
        stacks = []
        for m in range(tiles):
            tile = q_in[j, m]
            swapped = swap_halves(tile.astype(jnp.float32)).astype(jnp.bfloat16)
            none = jnp.zeros_like(tile)
            for at_low, at_high in ((tile, swapped), (swapped, tile)):
                stacks.append(jnp.concatenate([jnp.where(low, at_low, none), jnp.where(low, none, at_high)], axis=0))

        def score(r):
            scores, values = [], []
            for lower in range(0, entries, 8):
                keys_here, values_here = [], []
                for s in range(lower, lower + 8, 2):
                    a = kv_in[place_s[s, j * blocks + r]]
                    b = vk_in[place_s[s + 1, j * blocks + r]]
                    keys_here.append(jnp.where(low, a, b))
                    values_here.append(jnp.where(low, b, a))
                made = lax.dot_general(
                    stacks[r], jnp.concatenate(keys_here, axis=0), (((1,), (1,)), ((), ())),
                    preferred_element_type=jnp.float32,
                )
                line = bias[pl.ds(j * blocks + r, 1), lower * BLK : (lower + 8) * BLK]
                scores += [made[:BLK] + line[:, : 4 * BLK], made[BLK:] + line[:, 4 * BLK :]]
                values.append(jnp.concatenate(values_here, axis=0))
            top = jnp.max(functools.reduce(jnp.maximum, scores), axis=1, keepdims=True)
            return scores, values, top

        def gather(r, scores, values, top):
            weights = [jnp.exp(part - top) for part in scores]
            total = jnp.sum(functools.reduce(jnp.add, weights), axis=1, keepdims=True)
            made = 0.0
            for k, held_values in enumerate(values):
                rounded = jnp.concatenate([part.astype(jnp.bfloat16) for part in weights[2 * k : 2 * k + 2]], axis=0)
                made = made + jnp.dot(rounded, held_values, preferred_element_type=jnp.float32)
            if r % 2 == 0:
                summed = swap_halves(made[:BLK]) + made[BLK:]
            else:
                summed = made[:BLK] + swap_halves(made[BLK:])
            return summed / total, top + jnp.log(total)

        ready, results = [], []
        for r in range(blocks + AHEAD):
            if r < blocks:
                ready.append(score(r))
            if r >= AHEAD:
                results.append(gather(r - AHEAD, *ready[r - AHEAD]))
        logs = jnp.zeros((BLK, LANES), jnp.float32)
        for r in range(blocks):
            logs = jnp.where(lane == r, results[r][1], logs)
        for m in range(tiles):
            o_out[j, m] = jnp.where(low, results[2 * m][0], results[2 * m + 1][0]).astype(jnp.bfloat16)
        lines = jnp.transpose(jnp.concatenate([logs, jnp.zeros_like(logs)], axis=0))
        l_out[j] = lines[:8]

    def served(t):
        opening = heads // 2
        cycle = 2 * (groups - group) - 1
        after = jnp.maximum(t - opening, 0)
        owns = lax.div(after, cycle)
        own = (t < opening) | (lax.rem(after, cycle) == cycle - 1)
        visitor = after - owns
        step = jnp.where(own, jnp.where(t < opening, t, opening + owns), visitor)
        target = group + jnp.where(own, 0, 1 + lax.div(visitor, heads))
        return target * heads + lax.rem(idx + lax.rem(step, heads), heads)

    def serve(t, carry):
        j = served(t)

        @pl.when(t > 0)
        def _():
            arrival(q_in.at[j], q_recv.at[j]).wait_recv()

        attend(j)

        @pl.when(t > 0)
        def _():
            o_copy(j).start()
            l_copy(j).start()

        @pl.when(t == 0)
        def _():
            for m in range(tiles):
                o_in[group, idx, m] = o_out[j, m]
            l_in[group, idx] = l_out[j]

        return carry

    lax.fori_loop(0, devices - first_device, serve, 0)

    def absent(a, carry):
        o_in[a] = jnp.zeros(o_in.shape[1:], o_in.dtype)
        l_in[a] = jnp.full(l_in.shape[1:], masked_score, jnp.float32)
        return carry

    lax.fori_loop(group + 1, groups, absent, 0)

    def take_results(k, carry):
        source = lax.rem(me + k, (group + 1) * heads)
        place = o_in.at[lax.div(source, heads), lax.rem(source, heads)]
        arrival(place, o_recv.at[source]).wait_recv()
        line = l_in.at[lax.div(source, heads), lax.rem(source, heads)]
        arrival(line, l_recv.at[source]).wait_recv()
        return carry

    lax.fori_loop(1, (group + 1) * heads, take_results, 0)

    load_o.wait()

    def spread(body, start):
        if groups <= 2:
            for a in range(groups):
                start = body(a, start)
            return start
        return lax.fori_loop(0, groups, body, start)

    highest = spread(lambda a, top: jnp.maximum(top, l_in[a]), jnp.full(l_in.shape[1:], masked_score, jnp.float32))
    sums = spread(lambda a, acc: acc + jnp.exp(l_in[a] - highest), jnp.zeros(l_in.shape[1:], jnp.float32))
    total_log[...] = highest + jnp.log(sums)
    for m in range(tiles):
        first, second = total_log[:, 2 * m, :], total_log[:, 2 * m + 1, :]
        log_ref[:, m * LANES : (m + 1) * LANES] = jnp.where(low_line, first, swap_halves(second))

    def columns(a):
        share = jnp.exp(l_in[a] - total_log[...]).reshape(heads * 8, LANES)
        missing = LANES - heads * 8
        if missing:
            share = jnp.concatenate([share, jnp.zeros((missing, LANES), jnp.float32)], axis=0)
        return jnp.transpose(share)

    def add_group(a, carry):
        weight[a] = columns(a)
        return carry

    spread(add_group, 0)
    for ch in range(pairs):
        for m in range(tiles):

            def add_part(a, sums, ch=ch, m=m):
                t0 = o_in[a, 2 * ch, m].astype(jnp.float32)
                t1 = o_in[a, 2 * ch + 1, m].astype(jnp.float32)
                parts = (jnp.where(low, t0, swap_halves(t1)), jnp.where(low, swap_halves(t0), t1))
                made = []
                for e in range(2):
                    at = 2 * ch * 8 + 2 * m + e
                    share = jnp.where(low, weight[a, :BLK, at : at + 1], weight[a, :BLK, at + 8 : at + 9])
                    made.append(sums[e] + parts[e] * share)
                return tuple(made)

            zero = jnp.zeros((BLK, LANES), jnp.float32)
            made = spread(add_part, (zero, zero))
            for e in range(2):
                r = 2 * m + e
                attended[r * BLK : (r + 1) * BLK, ch * LANES : (ch + 1) * LANES] = made[e].astype(jnp.bfloat16)

    out_rows = rows // splits
    tile_width = min(512, wo.shape[1])
    chunks = wo.shape[1] // tile_width
    peers = [lax.rem(tp + d, splits) for d in range(splits)]

    def partial_of(d, c):
        mine = attended[pl.ds(pl.multiple_of(peers[d] * out_rows, out_rows), out_rows), :]
        made = jnp.dot(mine, wo[:, c * tile_width : (c + 1) * tile_width], preferred_element_type=jnp.float32)
        return made.astype(jnp.bfloat16)

    def hop(d, c):
        return pltpu.make_async_remote_copy(
            src_ref=stage.at[d - 1, c],
            dst_ref=landed_ref.at[d - 1, :, pl.ds(c * tile_width, tile_width)],
            send_sem=tp_send.at[d - 1, c],
            recv_sem=tp_recv.at[d - 1, c],
            device_id={"tp": peers[d]},
            device_id_type=MESH,
        )

    for d in range(1, splits):
        for c in range(chunks):
            stage[d - 1, c] = partial_of(d, c)
            hop(d, c).start()
    for c in range(chunks):
        mine_ref[:, c * tile_width : (c + 1) * tile_width] = partial_of(0, c)

    def sent(copy):
        copy.wait_send()

    for i in range(pairs):
        for e in range(2):
            head = 2 * pair_of(i) + e

            def drain(i=i, e=e, head=head):
                kv_copy(2 * i + e, head).wait_send()
                q_copy(2 * i + e, first_device + head).wait_send()

            if i > 0:
                drain()
            else:
                pl.when(head != idx)(drain)

    def drain_down(a, carry):
        for i in range(pairs):
            for e in range(2):
                q_copy(2 * i + e, a * heads + 2 * pair_of(i) + e).wait_send()
        return carry

    lax.fori_loop(0, group, drain_down, 0)

    def drain_results(t, carry):
        j = served(t)
        o_copy(j).wait_send()
        l_copy(j).wait_send()
        return carry

    lax.fori_loop(1, devices - first_device, drain_results, 0)
    for d in range(1, splits):
        for c in range(chunks):
            hop(d, c).wait()


def local(devices, splits, tokens, w_query, w_key, w_value, w_out, chosen):
    rows, depth = tokens.shape
    width = w_query.shape[1]
    out_width = w_out.shape[1]
    heads = width // HEAD_DIM
    pairs = heads // 2
    groups = devices // heads
    blocks = rows // BLK
    tiles = blocks // 2
    wide = 2 if pairs % 2 == 0 else 1

    out_rows = rows // splits
    tile_width = min(512, out_width)
    chunks = out_width // tile_width
    dma = pltpu.SemaphoreType.DMA
    bf16, f32 = jnp.bfloat16, jnp.float32
    mine, landed, logs = pl.pallas_call(
        functools.partial(layer_kernel, devices, splits),
        in_specs=[in_vmem()] + [in_hbm()] * 5,
        out_specs=[in_vmem()] * 3,
        out_shape=[
            jax.ShapeDtypeStruct((out_rows, out_width), bf16),
            jax.ShapeDtypeStruct((splits - 1, out_rows, out_width), bf16),
            jax.ShapeDtypeStruct((heads, rows), f32),
        ],
        scratch_shapes=[
            pltpu.VMEM((rows, depth), bf16),
            pltpu.VMEM((pairs // wide, depth, wide * LANES), bf16),
            pltpu.VMEM((pairs, depth, 2 * LANES), bf16),
            pltpu.VMEM((width, out_width), bf16),
            pltpu.VMEM((heads, blocks, BLK, LANES), bf16),
            pltpu.VMEM((heads, tiles, BLK, LANES), bf16),
            pltpu.VMEM((heads * blocks, BLK, LANES), bf16),
            pltpu.VMEM((heads * blocks, BLK, LANES), bf16),
            pltpu.VMEM(chosen.shape[::-1], jnp.int32),
            pltpu.SMEM(chosen.shape[::-1], jnp.int32),
            pltpu.VMEM((chosen.shape[0], chosen.shape[1] * BLK), f32),
            pltpu.VMEM((devices, tiles, BLK, LANES), bf16),
            pltpu.VMEM((devices, tiles, BLK, LANES), bf16),
            pltpu.VMEM((devices, 8, LANES), f32),
            pltpu.VMEM((groups, heads, tiles, BLK, LANES), bf16),
            pltpu.VMEM((groups, heads, 8, LANES), f32),
            pltpu.VMEM((groups, LANES, LANES), f32),
            pltpu.VMEM((heads, 8, LANES), f32),
            pltpu.VMEM((rows, width), bf16),
            pltpu.VMEM((splits - 1, chunks, out_rows, tile_width), bf16),
            dma((7, pairs)),
            dma((heads,)),
            dma((heads,)),
            dma((devices,)),
            dma((devices,)),
            dma((devices,)),
            dma((devices,)),
            dma((devices,)),
            dma((devices,)),
            dma((splits - 1, chunks)),
            dma((splits - 1, chunks)),
        ],
        compiler_params=pltpu.CompilerParams(
            collective_id=0, has_side_effects=True, vmem_limit_bytes=VMEM_LIMIT
        ),
        name="layer",
    )(jnp.transpose(chosen), tokens, w_query, w_key, w_value, w_out)
    total = mine.astype(f32) + jnp.sum(landed.astype(f32), axis=0)
    return total.astype(bf16), logs


def solution(mesh):
    placed = (P("kv", None), P(None, "tp"), P(None, "tp"), P(None, "tp"), P("tp", None), P())
    return jax.shard_map(
        functools.partial(local, mesh.shape["kv"], mesh.shape["tp"]),
        mesh=mesh,
        in_specs=placed,
        out_specs=(P(("kv", "tp"), None), P("tp", "kv")),
        check_vma=False,
    )
```

```python
import functools

import jax
import jax.numpy as jnp
import numpy as np
from jax import lax
from jax.experimental import pallas as pl
from jax.experimental.pallas import tpu as pltpu
from jax.sharding import PartitionSpec as P

HEAD_DIM = 64
BLK = 64
LANES = 128
VMEM_LIMIT = 55_000_000
AHEAD = 2
LOG2_E = float(np.log2(np.e))

rotary_base = 500000.0
masked_score = -1e30

MESH = pl.DeviceIdType.MESH


def in_vmem():
    return pl.BlockSpec(memory_space=pltpu.VMEM)


def in_hbm():
    return pl.BlockSpec(memory_space=pltpu.HBM)


def swap_halves(tile):
    return pltpu.roll(tile, LANES // 2, 1)


def layer_kernel(
    devices, splits, chosen_ref, x_ref, wq_ref, wk_ref, wv_ref, wo_ref,
    mine_ref, landed_ref, log_ref,
    x, wq, wkv, wo, kv_out, q_out, kv_in, vk_in, place_v, place_s, bias, q_in, o_out, l_out, o_in, l_in, total_log,
    attended, stage, load_sem, kv_load, q_load, kv_send, kv_recv, q_send, q_recv, o_send, o_recv, l_send, l_recv, tp_send, tp_recv,
):
    heads = kv_out.shape[0]
    pairs = heads // 2
    groups = devices // heads
    blocks = kv_out.shape[1]
    tiles = blocks // 2
    rows = blocks * BLK
    entries = chosen_ref.shape[0]
    table_blocks = heads * blocks
    wide = wq.shape[2] // LANES

    me = lax.axis_index("kv")
    tp = lax.axis_index("tp")
    group = lax.div(me, heads)
    idx = lax.rem(me, heads)
    first_device = group * heads
    half = HEAD_DIM // 2

    def pair_of(i):
        return lax.rem(lax.div(idx, 2) + pairs - i, pairs)

    def strip(ref, i):
        return ref.at[:, pl.ds(pl.multiple_of(pair_of(i) * LANES, LANES), LANES)]

    def load_q(i):
        target = wq.at[i // wide, :, pl.ds((i % wide) * LANES, LANES)]
        return pltpu.make_async_copy(strip(wq_ref, i), target, q_load.at[i // wide])

    def load_k(i):
        return pltpu.make_async_copy(strip(wk_ref, i), wkv.at[i, :, pl.ds(0, LANES)], kv_load.at[i])

    def load_v(i):
        return pltpu.make_async_copy(strip(wv_ref, i), wkv.at[i, :, pl.ds(LANES, LANES)], kv_load.at[i])

    def loaded(ref, semaphore):
        pltpu.make_async_copy(ref, ref, semaphore).wait()

    load_x = pltpu.make_async_copy(x_ref, x, load_sem.at[0])
    load_o = pltpu.make_async_copy(wo_ref, wo, load_sem.at[1])
    move_places = pltpu.make_async_copy(place_v, place_s, load_sem.at[2])

    load_x.start()
    for i in range(pairs):
        load_k(i).start()
        load_v(i).start()
    for i in range(pairs):
        load_q(i).start()
    load_o.start()

    barrier = pltpu.get_barrier_semaphore()

    def greet(d, carry):
        pl.semaphore_signal(
            barrier, inc=1, device_id={"kv": lax.rem(me + d, devices)}, device_id_type=MESH
        )
        return carry

    lax.fori_loop(1, devices, greet, 0)
    for d in range(1, splits):
        pl.semaphore_signal(barrier, inc=1, device_id={"tp": lax.rem(tp + d, splits)}, device_id_type=MESH)

    def kv_copy(slot, head):
        return pltpu.make_async_remote_copy(
            src_ref=kv_out.at[slot],
            dst_ref=kv_in.at[pl.ds(idx * blocks, blocks)],
            send_sem=kv_send.at[0],
            recv_sem=kv_recv.at[0],
            device_id={"kv": first_device + head},
            device_id_type=MESH,
        )

    def q_copy(slot, target):
        return pltpu.make_async_remote_copy(
            src_ref=q_out.at[slot],
            dst_ref=q_in.at[me],
            send_sem=q_send.at[lax.div(target, heads)],
            recv_sem=q_recv.at[me],
            device_id={"kv": target},
            device_id_type=MESH,
        )

    def o_copy(target):
        return pltpu.make_async_remote_copy(
            src_ref=o_out.at[target],
            dst_ref=o_in.at[group, idx],
            send_sem=o_send.at[lax.div(target, heads)],
            recv_sem=o_recv.at[group, lax.div(idx, 2)],
            device_id={"kv": target},
            device_id_type=MESH,
        )

    def l_copy(target):
        return pltpu.make_async_remote_copy(
            src_ref=l_out.at[target],
            dst_ref=l_in.at[group, idx],
            send_sem=l_send.at[lax.div(target, heads)],
            recv_sem=l_recv.at[group, lax.div(idx, 2)],
            device_id={"kv": target},
            device_id_type=MESH,
        )

    def arrival(ref, semaphore):
        return pltpu.make_async_remote_copy(
            src_ref=ref, dst_ref=ref, send_sem=semaphore, recv_sem=semaphore,
            device_id={"kv": me}, device_id_type=MESH,
        )

    load_x.wait()
    low_rows = lax.broadcasted_iota(jnp.int32, (rows, LANES), 1) < LANES // 2
    turn_low = lax.broadcasted_iota(jnp.int32, (rows, LANES), 1) % HEAD_DIM < half

    def angles(count, step, start):
        channel = (lax.broadcasted_iota(jnp.int32, (count, LANES), 1) % half).astype(jnp.float32)
        position = lax.broadcasted_iota(jnp.int32, (count, LANES), 0) * step + start
        turn = position.astype(jnp.float32) * jnp.exp(channel * (-np.log(rotary_base) / half))
        return jnp.cos(turn), jnp.sin(turn)

    cos_fine, sin_fine = angles(8, 1, 0)
    cos_coarse, sin_coarse = angles(rows // 8, 8, me * rows)
    cos_parts, sin_parts = [], []
    for k in range(rows // 8):
        cos_k, sin_k = cos_coarse[k : k + 1], sin_coarse[k : k + 1]
        cos_parts.append(cos_k * cos_fine - sin_k * sin_fine)
        sin_parts.append(sin_k * cos_fine + cos_k * sin_fine)
    cos_part = jnp.concatenate(cos_parts, axis=0)
    sin_part = jnp.concatenate(sin_parts, axis=0)
    sin_part = jnp.where(turn_low, -sin_part, sin_part)

    def turned(part):
        other = jnp.where(turn_low, pltpu.roll(part, LANES - half, 1), pltpu.roll(part, half, 1))
        return part * cos_part + other * sin_part

    def make_kv(i):
        loaded(wkv.at[i], kv_load.at[i])
        made = jnp.dot(x[...], wkv[i], preferred_element_type=jnp.float32)
        keys = turned(made[:, :LANES])
        values = made[:, LANES:]
        even = jnp.where(low_rows, keys, swap_halves(values)).astype(jnp.bfloat16)
        odd = jnp.where(low_rows, swap_halves(keys), values).astype(jnp.bfloat16)
        for r in range(blocks):
            kv_out[2 * i, r] = even[r * BLK : (r + 1) * BLK]
            kv_out[2 * i + 1, r] = odd[r * BLK : (r + 1) * BLK]

    def make_q(i):
        loaded(wq.at[i // wide], q_load.at[i // wide])
        made = jnp.dot(x[...], wq[i // wide], preferred_element_type=jnp.float32)
        for e in range(wide):
            part = turned(made[:, e * LANES : (e + 1) * LANES]) * (HEAD_DIM**-0.5 * LOG2_E)
            swapped = swap_halves(part)
            low = low_rows[:BLK]
            for m in range(tiles):
                a = slice(2 * m * BLK, (2 * m + 1) * BLK)
                b = slice((2 * m + 1) * BLK, (2 * m + 2) * BLK)
                q_out[2 * (i + e), m] = jnp.where(low, part[a], swapped[b]).astype(jnp.bfloat16)
                q_out[2 * (i + e) + 1, m] = jnp.where(low, swapped[a], part[b]).astype(jnp.bfloat16)

    def send_kv(i):
        for e in range(2):
            head = 2 * pair_of(i) + e
            if i > 0:
                kv_copy(2 * i + e, head).start()
            else:
                pl.when(head != idx)(lambda e=e, head=head: kv_copy(2 * i + e, head).start())

    def send_q(i):
        for e in range(2):
            head = 2 * pair_of(i) + e
            if i > 0:
                q_copy(2 * i + e, first_device + head).start()
            else:
                pl.when(head != idx)(lambda e=e, head=head: q_copy(2 * i + e, first_device + head).start())

    for i in range(pairs):
        make_kv(i)
        if i == 0:
            pl.semaphore_wait(barrier, devices - 1 + splits - 1)
        send_kv(i)
    for i in range(0, pairs, wide):
        make_q(i)
        if i == 0:
            for e in range(wide):
                send_q(e)

    def send_down(a, carry):
        for i in range(pairs):
            for e in range(2):
                q_copy(2 * i + e, a * heads + 2 * pair_of(i) + e).start()
        return carry

    place = chosen_ref[...] - first_device * blocks
    held = (place >= 0) & (place < table_blocks)
    place_v[...] = jnp.where(held, place, 0)
    move_places.start()
    column = lax.broadcasted_iota(jnp.int32, (entries, entries * BLK), 1)
    slot = column // (8 * BLK) * 8 + column // BLK % 4 * 2 + column // (4 * BLK) % 2
    unit = (slot == lax.broadcasted_iota(jnp.int32, slot.shape, 0)).astype(jnp.float32)
    bias[...] = masked_score * (
        1.0
        - lax.dot_general(
            jnp.where(held, 1.0, 0.0), unit, (((0,), (0,)), ((), ())), preferred_element_type=jnp.float32
        )
    )
    move_places.wait()

    own_slot = lax.rem(idx, 2)
    for r in range(blocks):
        kv_in[idx * blocks + r] = kv_out[own_slot, r]
    for m in range(tiles):
        q_in[me, m] = q_out[own_slot, m]

    low = lax.broadcasted_iota(jnp.int32, (BLK, LANES), 1) < LANES // 2
    lane = lax.broadcasted_iota(jnp.int32, (BLK, LANES), 1)
    low_line = lax.broadcasted_iota(jnp.int32, (1, LANES), 1) < LANES // 2

    arrival(kv_in.at[pl.ds(0, (heads - 1) * blocks)], kv_recv.at[0]).wait_recv()
    for i in range(wide, pairs):
        send_q(i)
    lax.fori_loop(0, group, send_down, 0)

    def swap_kv(k, carry):
        for r in range(blocks):
            place = k * blocks + r
            vk_in[place] = swap_halves(kv_in[place].astype(jnp.float32)).astype(jnp.bfloat16)
        return carry

    lax.fori_loop(0, heads, swap_kv, 0)

    def attend(js):
        stacks = []
        for j in js:
            for m in range(tiles):
                tile = q_in[j, m]
                swapped = swap_halves(tile.astype(jnp.float32)).astype(jnp.bfloat16)
                none = jnp.zeros_like(tile)
                for at_low, at_high in ((tile, swapped), (swapped, tile)):
                    stacks.append(
                        jnp.concatenate([jnp.where(low, at_low, none), jnp.where(low, none, at_high)], axis=0)
                    )

        def score(n):
            block = js[n // blocks] * blocks + n % blocks
            scores, values = [], []
            for lower in range(0, entries, 8):
                keys_here, values_here = [], []
                for s in range(lower, lower + 8, 2):
                    a = kv_in[place_s[s, block]]
                    b = vk_in[place_s[s + 1, block]]
                    keys_here.append(jnp.where(low, a, b))
                    values_here.append(jnp.where(low, b, a))
                made = lax.dot_general(
                    stacks[n], jnp.concatenate(keys_here, axis=0), (((1,), (1,)), ((), ())),
                    preferred_element_type=jnp.float32,
                )
                line = bias[pl.ds(block, 1), lower * BLK : (lower + 8) * BLK]
                scores += [made[:BLK] + line[:, : 4 * BLK], made[BLK:] + line[:, 4 * BLK :]]
                values.append(jnp.concatenate(values_here, axis=0))
            top = jnp.max(functools.reduce(jnp.maximum, scores), axis=1, keepdims=True)
            return scores, values, top

        def gather(n, scores, values, top):
            weights = [jnp.exp2(part - top) for part in scores]
            total = jnp.sum(functools.reduce(jnp.add, weights), axis=1, keepdims=True)
            made = 0.0
            for k, held_values in enumerate(values):
                rounded = jnp.concatenate([part.astype(jnp.bfloat16) for part in weights[2 * k : 2 * k + 2]], axis=0)
                made = made + jnp.dot(rounded, held_values, preferred_element_type=jnp.float32)
            if n % 2 == 0:
                summed = swap_halves(made[:BLK]) + made[BLK:]
            else:
                summed = made[:BLK] + swap_halves(made[BLK:])
            return summed / total, (top + jnp.log2(total)) * (1.0 / LOG2_E)

        ready, results = [], []
        for n in range(len(js) * blocks + AHEAD):
            if n < len(js) * blocks:
                ready.append(score(n))
            if n >= AHEAD:
                results.append(gather(n - AHEAD, *ready[n - AHEAD]))
        for k, j in enumerate(js):
            found = results[k * blocks : (k + 1) * blocks]
            logs = jnp.zeros((BLK, LANES), jnp.float32)
            for r in range(blocks):
                logs = jnp.where(lane == r, found[r][1], logs)
            for m in range(tiles):
                o_out[j, m] = jnp.where(low, found[2 * m][0], found[2 * m + 1][0]).astype(jnp.bfloat16)
            lines = jnp.transpose(jnp.concatenate([logs, jnp.zeros_like(logs)], axis=0))
            l_out[j] = lines[:8]

    def served(t):
        opening = heads // 2
        cycle = 2 * (groups - group) - 1
        after = jnp.maximum(t - opening, 0)
        owns = lax.div(after, cycle)
        own = (t < opening) | (lax.rem(after, cycle) == cycle - 1)
        visitor = after - owns
        step = jnp.where(own, jnp.where(t < opening, t, opening + owns), visitor)
        target = group + jnp.where(own, 0, 1 + lax.div(visitor, heads))
        return target * heads + lax.rem(idx + lax.rem(step, heads), heads)

    def serve(u, carry):
        js = [served(2 * u), served(2 * u + 1)]

        @pl.when(u > 0)
        def _():
            arrival(q_in.at[js[0]], q_recv.at[js[0]]).wait_recv()

        arrival(q_in.at[js[1]], q_recv.at[js[1]]).wait_recv()
        attend(js)

        @pl.when(u > 0)
        def _():
            o_copy(js[0]).start()
            l_copy(js[0]).start()

        o_copy(js[1]).start()
        l_copy(js[1]).start()

        @pl.when(u == 0)
        def _():
            for m in range(tiles):
                o_in[group, idx, m] = o_out[js[0], m]
            l_in[group, idx] = l_out[js[0]]

        return carry

    lax.fori_loop(0, (devices - first_device) // 2, serve, 0)

    def absent(a, carry):
        o_in[a] = jnp.zeros(o_in.shape[1:], o_in.dtype)
        l_in[a] = jnp.full(l_in.shape[1:], masked_score, jnp.float32)
        return carry

    lax.fori_loop(group + 1, groups, absent, 0)

    def spread(body, start):
        if groups <= 2:
            for a in range(groups):
                start = body(a, start)
            return start
        return lax.fori_loop(0, groups, body, start)

    for i in range(pairs):
        ch = pair_of(i)

        def take_results(a, carry, i=i, ch=ch):
            def take(count):
                o_place = o_in.at[a, pl.ds(2 * ch, count)]
                arrival(o_place, o_recv.at[a, ch]).wait_recv()
                l_place = l_in.at[a, pl.ds(2 * ch, count)]
                arrival(l_place, l_recv.at[a, ch]).wait_recv()

            if i > 0:
                take(2)
            else:
                pl.when(a == group)(lambda: take(1))
                pl.when(a != group)(lambda: take(2))
            return carry

        lax.fori_loop(0, group + 1, take_results, 0)

        def lines(a, ch=ch):
            return l_in[a, pl.ds(2 * ch, 2)]

        start = jnp.full((2, 8, LANES), masked_score, jnp.float32)
        highest = spread(lambda a, top: jnp.maximum(top, lines(a)), start)
        sums = spread(lambda a, acc: acc + jnp.exp(lines(a) - highest), jnp.zeros_like(start))
        logs = highest + jnp.log(sums)
        total_log[pl.ds(2 * ch, 2)] = logs

        def add_share(a, parts, ch=ch, logs=logs):
            share = jnp.exp(lines(a) - logs).reshape(16, LANES)
            columns = jnp.transpose(jnp.concatenate([share, jnp.zeros((LANES - 16, LANES), jnp.float32)], axis=0))
            made = []
            for m in range(tiles):
                t0 = o_in[a, 2 * ch, m].astype(jnp.float32)
                t1 = o_in[a, 2 * ch + 1, m].astype(jnp.float32)
                both = (jnp.where(low, t0, swap_halves(t1)), jnp.where(low, swap_halves(t0), t1))
                for e in range(2):
                    r = 2 * m + e
                    scale = jnp.where(low, columns[:BLK, r : r + 1], columns[:BLK, 8 + r : 9 + r])
                    made.append(parts[r] + both[e] * scale)
            return tuple(made)

        made = spread(add_share, tuple(jnp.zeros((BLK, LANES), jnp.float32) for _ in range(blocks)))
        for r in range(blocks):
            columns = pl.ds(pl.multiple_of(ch * LANES, LANES), LANES)
            attended[r * BLK : (r + 1) * BLK, columns] = made[r].astype(jnp.bfloat16)

    for m in range(tiles):
        first, second = total_log[:, 2 * m, :], total_log[:, 2 * m + 1, :]
        log_ref[:, m * LANES : (m + 1) * LANES] = jnp.where(low_line, first, swap_halves(second))

    load_o.wait()
    out_rows = rows // splits
    tile_width = min(512, wo.shape[1])
    chunks = wo.shape[1] // tile_width
    peers = [lax.rem(tp + d, splits) for d in range(splits)]

    def partial_of(d, c):
        mine = attended[pl.ds(pl.multiple_of(peers[d] * out_rows, out_rows), out_rows), :]
        made = jnp.dot(mine, wo[:, c * tile_width : (c + 1) * tile_width], preferred_element_type=jnp.float32)
        return made.astype(jnp.bfloat16)

    def hop(d, c):
        return pltpu.make_async_remote_copy(
            src_ref=stage.at[d - 1, c],
            dst_ref=landed_ref.at[d - 1, :, pl.ds(c * tile_width, tile_width)],
            send_sem=tp_send.at[d - 1],
            recv_sem=tp_recv.at[d - 1],
            device_id={"tp": peers[d]},
            device_id_type=MESH,
        )

    for d in range(1, splits):
        for c in range(chunks):
            stage[d - 1, c] = partial_of(d, c)
            hop(d, c).start()
    for c in range(chunks):
        mine_ref[:, c * tile_width : (c + 1) * tile_width] = partial_of(0, c)

    def sent(ref, semaphore):
        arrival(ref, semaphore).wait_send()

    sent(kv_out.at[pl.ds(0, heads - 1)], kv_send.at[0])
    sent(q_out.at[pl.ds(0, heads - 1)], q_send.at[group])

    def sent_down(a, carry):
        sent(q_out, q_send.at[a])
        return carry

    lax.fori_loop(0, group, sent_down, 0)
    sent(o_out.at[pl.ds(0, heads - 1)], o_send.at[group])
    sent(l_out.at[pl.ds(0, heads - 1)], l_send.at[group])

    def sent_up(a, carry):
        sent(o_out.at[pl.ds(0, heads)], o_send.at[a])
        sent(l_out.at[pl.ds(0, heads)], l_send.at[a])
        return carry

    lax.fori_loop(group + 1, groups, sent_up, 0)
    for d in range(1, splits):
        sent(stage.at[d - 1], tp_send.at[d - 1])
        arrival(landed_ref.at[d - 1], tp_recv.at[d - 1]).wait_recv()


def local(devices, splits, tokens, w_query, w_key, w_value, w_out, chosen):
    rows, depth = tokens.shape
    width = w_query.shape[1]
    out_width = w_out.shape[1]
    heads = width // HEAD_DIM
    pairs = heads // 2
    groups = devices // heads
    blocks = rows // BLK
    tiles = blocks // 2
    wide = 2 if pairs % 2 == 0 else 1

    out_rows = rows // splits
    tile_width = min(512, out_width)
    chunks = out_width // tile_width
    dma = pltpu.SemaphoreType.DMA
    bf16, f32 = jnp.bfloat16, jnp.float32
    mine, landed, logs = pl.pallas_call(
        functools.partial(layer_kernel, devices, splits),
        in_specs=[in_vmem()] + [in_hbm()] * 5,
        out_specs=[in_vmem()] * 3,
        out_shape=[
            jax.ShapeDtypeStruct((out_rows, out_width), bf16),
            jax.ShapeDtypeStruct((splits - 1, out_rows, out_width), bf16),
            jax.ShapeDtypeStruct((heads, rows), f32),
        ],
        scratch_shapes=[
            pltpu.VMEM((rows, depth), bf16),
            pltpu.VMEM((pairs // wide, depth, wide * LANES), bf16),
            pltpu.VMEM((pairs, depth, 2 * LANES), bf16),
            pltpu.VMEM((width, out_width), bf16),
            pltpu.VMEM((heads, blocks, BLK, LANES), bf16),
            pltpu.VMEM((heads, tiles, BLK, LANES), bf16),
            pltpu.VMEM((heads * blocks, BLK, LANES), bf16),
            pltpu.VMEM((heads * blocks, BLK, LANES), bf16),
            pltpu.VMEM(chosen.shape[::-1], jnp.int32),
            pltpu.SMEM(chosen.shape[::-1], jnp.int32),
            pltpu.VMEM((chosen.shape[0], chosen.shape[1] * BLK), f32),
            pltpu.VMEM((devices, tiles, BLK, LANES), bf16),
            pltpu.VMEM((devices, tiles, BLK, LANES), bf16),
            pltpu.VMEM((devices, 8, LANES), f32),
            pltpu.VMEM((groups, heads, tiles, BLK, LANES), bf16),
            pltpu.VMEM((groups, heads, 8, LANES), f32),
            pltpu.VMEM((heads, 8, LANES), f32),
            pltpu.VMEM((rows, width), bf16),
            pltpu.VMEM((splits - 1, chunks, out_rows, tile_width), bf16),
            dma((3,)),
            dma((pairs,)),
            dma((pairs // wide,)),
            dma((1,)),
            dma((1,)),
            dma((groups,)),
            dma((devices,)),
            dma((groups,)),
            dma((groups, pairs)),
            dma((groups,)),
            dma((groups, pairs)),
            dma((splits - 1,)),
            dma((splits - 1,)),
        ],
        compiler_params=pltpu.CompilerParams(
            collective_id=0, has_side_effects=True, vmem_limit_bytes=VMEM_LIMIT
        ),
        name="layer",
    )(jnp.transpose(chosen), tokens, w_query, w_key, w_value, w_out)
    total = mine.astype(f32) + jnp.sum(landed.astype(f32), axis=0)
    return total.astype(bf16), logs


def solution(mesh):
    placed = (P("kv", None), P(None, "tp"), P(None, "tp"), P(None, "tp"), P("tp", None), P())
    return jax.shard_map(
        functools.partial(local, mesh.shape["kv"], mesh.shape["tp"]),
        mesh=mesh,
        in_specs=placed,
        out_specs=(P(("kv", "tp"), None), P("tp", "kv")),
        check_vma=False,
    )
```

```python
import functools

import jax
import jax.numpy as jnp
import numpy as np
from jax import lax
from jax.experimental import pallas as pl
from jax.experimental.pallas import tpu as pltpu
from jax.sharding import PartitionSpec as P

HEAD_DIM = 64
BLK = 64
LANES = 128
VMEM_LIMIT = 55_000_000
AHEAD = 2
LOG2_E = float(np.log2(np.e))

rotary_base = 500000.0
masked_score = -1e30

MESH = pl.DeviceIdType.MESH


def in_vmem():
    return pl.BlockSpec(memory_space=pltpu.VMEM)


def in_hbm():
    return pl.BlockSpec(memory_space=pltpu.HBM)


def partner(place, step, count):
    if count & (count - 1):
        return lax.rem(place + step, count)
    mixed, bit = 0, 1
    while bit < count:
        mixed = mixed + bit * lax.rem(lax.div(place, bit) + lax.div(step, bit), 2)
        bit *= 2
    return mixed


def swap_halves(tile):
    return pltpu.roll(tile, LANES // 2, 1)


def layer_kernel(
    devices, splits, chosen_ref, x_ref, wq_ref, wk_ref, wv_ref, wo_ref,
    mine_ref, landed_ref, log_ref,
    x, wq, wkv, wo, kv_out, q_out, kv_in, vk_in, place_v, place_s, bias, q_in, o_out, l_out, o_in, l_in, total_log,
    attended, stage, load_sem, kv_load, q_load, kv_send, kv_recv, q_send, q_recv, o_send, o_recv, l_send, l_recv, tp_send, tp_recv,
):
    heads = kv_out.shape[0]
    pairs = heads // 2
    groups = devices // heads
    blocks = kv_out.shape[1]
    tiles = blocks // 2
    rows = blocks * BLK
    entries = chosen_ref.shape[0]
    table_blocks = heads * blocks
    wide = wq.shape[2] // LANES

    me = lax.axis_index("kv")
    tp = lax.axis_index("tp")
    group = lax.div(me, heads)
    idx = lax.rem(me, heads)
    first_device = group * heads
    half = HEAD_DIM // 2

    def pair_of(i):
        return partner(lax.div(idx, 2), jnp.int32(i), pairs)

    def strip(ref, i):
        return ref.at[:, pl.ds(pl.multiple_of(pair_of(i) * LANES, LANES), LANES)]

    def load_q(i):
        target = wq.at[i // wide, :, pl.ds((i % wide) * LANES, LANES)]
        return pltpu.make_async_copy(strip(wq_ref, i), target, q_load.at[i // wide])

    def load_k(i):
        return pltpu.make_async_copy(strip(wk_ref, i), wkv.at[i, :, pl.ds(0, LANES)], kv_load.at[i])

    def load_v(i):
        return pltpu.make_async_copy(strip(wv_ref, i), wkv.at[i, :, pl.ds(LANES, LANES)], kv_load.at[i])

    def loaded(ref, semaphore):
        pltpu.make_async_copy(ref, ref, semaphore).wait()

    load_x = pltpu.make_async_copy(x_ref, x, load_sem.at[0])
    load_o = pltpu.make_async_copy(wo_ref, wo, load_sem.at[1])
    move_places = pltpu.make_async_copy(place_v, place_s, load_sem.at[2])

    load_x.start()
    lowest = group == 0
    early = min(2, pairs)

    def start_kv(first, last):
        for i in range(first, last):
            load_k(i).start()
            load_v(i).start()

    def start_q():
        for i in range(pairs):
            load_q(i).start()

    pl.when(lowest)(lambda: start_kv(0, early))
    pl.when(jnp.logical_not(lowest))(start_q)

    barrier = pltpu.get_barrier_semaphore()

    def greet(d, carry):
        pl.semaphore_signal(
            barrier, inc=1, device_id={"kv": lax.rem(me + d, devices)}, device_id_type=MESH
        )
        return carry

    lax.fori_loop(1, devices, greet, 0)
    for d in range(1, splits):
        pl.semaphore_signal(barrier, inc=1, device_id={"tp": lax.rem(tp + d, splits)}, device_id_type=MESH)

    def kv_copy(slot, head):
        return pltpu.make_async_remote_copy(
            src_ref=kv_out.at[slot],
            dst_ref=kv_in.at[pl.ds(idx * blocks, blocks)],
            send_sem=kv_send.at[0],
            recv_sem=kv_recv.at[0],
            device_id={"kv": first_device + head},
            device_id_type=MESH,
        )

    def q_copy(slot, target):
        return pltpu.make_async_remote_copy(
            src_ref=q_out.at[slot],
            dst_ref=q_in.at[me],
            send_sem=q_send.at[lax.div(target, heads)],
            recv_sem=q_recv.at[me],
            device_id={"kv": target},
            device_id_type=MESH,
        )

    def o_copy(target):
        return pltpu.make_async_remote_copy(
            src_ref=o_out.at[target],
            dst_ref=o_in.at[group, idx],
            send_sem=o_send.at[lax.div(target, heads)],
            recv_sem=o_recv.at[group, lax.div(idx, 2)],
            device_id={"kv": target},
            device_id_type=MESH,
        )

    def l_copy(target):
        return pltpu.make_async_remote_copy(
            src_ref=l_out.at[target],
            dst_ref=l_in.at[group, idx],
            send_sem=l_send.at[lax.div(target, heads)],
            recv_sem=l_recv.at[group, lax.div(idx, 2)],
            device_id={"kv": target},
            device_id_type=MESH,
        )

    def arrival(ref, semaphore):
        return pltpu.make_async_remote_copy(
            src_ref=ref, dst_ref=ref, send_sem=semaphore, recv_sem=semaphore,
            device_id={"kv": me}, device_id_type=MESH,
        )

    load_x.wait()

    @pl.when(lowest)
    def _():
        start_kv(early, pairs)
        start_q()

    @pl.when(jnp.logical_not(lowest))
    def _():
        start_kv(0, pairs)

    low_rows = lax.broadcasted_iota(jnp.int32, (rows, LANES), 1) < LANES // 2
    turn_low = lax.broadcasted_iota(jnp.int32, (rows, LANES), 1) % HEAD_DIM < half

    def angles(count, step, start):
        channel = (lax.broadcasted_iota(jnp.int32, (count, LANES), 1) % half).astype(jnp.float32)
        position = lax.broadcasted_iota(jnp.int32, (count, LANES), 0) * step + start
        turn = position.astype(jnp.float32) * jnp.exp(channel * (-np.log(rotary_base) / half))
        return jnp.cos(turn), jnp.sin(turn)

    cos_fine, sin_fine = angles(8, 1, 0)
    cos_coarse, sin_coarse = angles(rows // 8, 8, me * rows)
    cos_parts, sin_parts = [], []
    for k in range(rows // 8):
        cos_k, sin_k = cos_coarse[k : k + 1], sin_coarse[k : k + 1]
        cos_parts.append(cos_k * cos_fine - sin_k * sin_fine)
        sin_parts.append(sin_k * cos_fine + cos_k * sin_fine)
    cos_part = jnp.concatenate(cos_parts, axis=0)
    sin_part = jnp.concatenate(sin_parts, axis=0)
    sin_part = jnp.where(turn_low, -sin_part, sin_part)

    def turned(part):
        other = jnp.where(turn_low, pltpu.roll(part, LANES - half, 1), pltpu.roll(part, half, 1))
        return part * cos_part + other * sin_part

    def make_kv(i):
        loaded(wkv.at[i], kv_load.at[i])
        made = jnp.dot(x[...], wkv[i], preferred_element_type=jnp.float32)
        keys = turned(made[:, :LANES])
        values = made[:, LANES:]
        even = jnp.where(low_rows, keys, swap_halves(values)).astype(jnp.bfloat16)
        odd = jnp.where(low_rows, swap_halves(keys), values).astype(jnp.bfloat16)
        for r in range(blocks):
            kv_out[2 * i, r] = even[r * BLK : (r + 1) * BLK]
            kv_out[2 * i + 1, r] = odd[r * BLK : (r + 1) * BLK]

    def make_q(i):
        loaded(wq.at[i // wide], q_load.at[i // wide])
        made = jnp.dot(x[...], wq[i // wide], preferred_element_type=jnp.float32)
        for e in range(wide):
            part = turned(made[:, e * LANES : (e + 1) * LANES]) * (HEAD_DIM**-0.5 * LOG2_E)
            swapped = swap_halves(part)
            low = low_rows[:BLK]
            for m in range(tiles):
                a = slice(2 * m * BLK, (2 * m + 1) * BLK)
                b = slice((2 * m + 1) * BLK, (2 * m + 2) * BLK)
                q_out[2 * (i + e), m] = jnp.where(low, part[a], swapped[b]).astype(jnp.bfloat16)
                q_out[2 * (i + e) + 1, m] = jnp.where(low, swapped[a], part[b]).astype(jnp.bfloat16)

    def send_kv(i):
        for e in range(2):
            head = 2 * pair_of(i) + e
            if i > 0:
                kv_copy(2 * i + e, head).start()
            else:
                pl.when(head != idx)(lambda e=e, head=head: kv_copy(2 * i + e, head).start())

    def send_q(i):
        for e in range(2):
            head = 2 * pair_of(i) + e
            if i > 0:
                q_copy(2 * i + e, first_device + head).start()
            else:
                pl.when(head != idx)(lambda e=e, head=head: q_copy(2 * i + e, first_device + head).start())

    def send_down(near):
        def send(a, carry):
            for i in range(pairs):
                ch = pair_of(i)

                @pl.when((2 * ch >= heads // 2) == near)
                def _(i=i, ch=ch):
                    for e in range(2):
                        q_copy(2 * i + e, a * heads + 2 * ch + e).start()

            return carry

        lax.fori_loop(0, group, send, 0)

    def make_queries():
        for i in range(0, pairs, wide):
            make_q(i)

    @pl.when(jnp.logical_not(lowest))
    def _():
        make_queries()
        pl.semaphore_wait(barrier, devices - 1 + splits - 1)
        send_down(True)

    for i in range(pairs):
        make_kv(i)
        if i == 0:
            pl.when(lowest)(lambda: pl.semaphore_wait(barrier, devices - 1 + splits - 1))
        send_kv(i)
    pl.when(lowest)(make_queries)
    for i in range(pairs):
        send_q(i)
    load_o.start()

    place = chosen_ref[...] - first_device * blocks
    held = (place >= 0) & (place < table_blocks)
    place_v[...] = jnp.where(held, place, 0)
    move_places.start()
    column = lax.broadcasted_iota(jnp.int32, (entries, entries * BLK), 1)
    slot = column // (8 * BLK) * 8 + column // BLK % 4 * 2 + column // (4 * BLK) % 2
    unit = (slot == lax.broadcasted_iota(jnp.int32, slot.shape, 0)).astype(jnp.float32)
    bias[...] = masked_score * (
        1.0
        - lax.dot_general(
            jnp.where(held, 1.0, 0.0), unit, (((0,), (0,)), ((), ())), preferred_element_type=jnp.float32
        )
    )
    move_places.wait()

    own_slot = lax.rem(idx, 2)
    for r in range(blocks):
        kv_in[idx * blocks + r] = kv_out[own_slot, r]
    for m in range(tiles):
        q_in[me, m] = q_out[own_slot, m]

    low = lax.broadcasted_iota(jnp.int32, (BLK, LANES), 1) < LANES // 2
    lane = lax.broadcasted_iota(jnp.int32, (BLK, LANES), 1)
    low_line = lax.broadcasted_iota(jnp.int32, (1, LANES), 1) < LANES // 2

    arrival(kv_in.at[pl.ds(0, (heads - 1) * blocks)], kv_recv.at[0]).wait_recv()
    send_down(False)

    def swap_kv(k, carry):
        for r in range(blocks):
            place = k * blocks + r
            vk_in[place] = swap_halves(kv_in[place].astype(jnp.float32)).astype(jnp.bfloat16)
        return carry

    lax.fori_loop(0, heads, swap_kv, 0)

    def attend(js):
        stacks = []
        for j in js:
            for m in range(tiles):
                tile = q_in[j, m]
                swapped = swap_halves(tile.astype(jnp.float32)).astype(jnp.bfloat16)
                none = jnp.zeros_like(tile)
                for at_low, at_high in ((tile, swapped), (swapped, tile)):
                    stacks.append(
                        jnp.concatenate([jnp.where(low, at_low, none), jnp.where(low, none, at_high)], axis=0)
                    )

        def score(n):
            block = js[n // blocks] * blocks + n % blocks
            scores, values = [], []
            for lower in range(0, entries, 8):
                keys_here, values_here = [], []
                for s in range(lower, lower + 8, 2):
                    a = kv_in[place_s[s, block]]
                    b = vk_in[place_s[s + 1, block]]
                    keys_here.append(jnp.where(low, a, b))
                    values_here.append(jnp.where(low, b, a))
                made = lax.dot_general(
                    stacks[n], jnp.concatenate(keys_here, axis=0), (((1,), (1,)), ((), ())),
                    preferred_element_type=jnp.float32,
                )
                line = bias[pl.ds(block, 1), lower * BLK : (lower + 8) * BLK]
                scores += [made[:BLK] + line[:, : 4 * BLK], made[BLK:] + line[:, 4 * BLK :]]
                values.append(jnp.concatenate(values_here, axis=0))
            top = jnp.max(functools.reduce(jnp.maximum, scores), axis=1, keepdims=True)
            return scores, values, top

        def gather(n, scores, values, top):
            weights = [jnp.exp2(part - top) for part in scores]
            total = jnp.sum(functools.reduce(jnp.add, weights), axis=1, keepdims=True)
            made = 0.0
            for k, held_values in enumerate(values):
                rounded = jnp.concatenate([part.astype(jnp.bfloat16) for part in weights[2 * k : 2 * k + 2]], axis=0)
                made = made + jnp.dot(rounded, held_values, preferred_element_type=jnp.float32)
            if n % 2 == 0:
                summed = swap_halves(made[:BLK]) + made[BLK:]
            else:
                summed = made[:BLK] + swap_halves(made[BLK:])
            return summed / total, (top + jnp.log2(total)) * (1.0 / LOG2_E)

        ready, results = [], []
        for n in range(len(js) * blocks + AHEAD):
            if n < len(js) * blocks:
                ready.append(score(n))
            if n >= AHEAD:
                results.append(gather(n - AHEAD, *ready[n - AHEAD]))
        for k, j in enumerate(js):
            found = results[k * blocks : (k + 1) * blocks]
            logs = jnp.zeros((BLK, LANES), jnp.float32)
            for r in range(blocks):
                logs = jnp.where(lane == r, found[r][1], logs)
            for m in range(tiles):
                o_out[j, m] = jnp.where(low, found[2 * m][0], found[2 * m + 1][0]).astype(jnp.bfloat16)
            lines = jnp.transpose(jnp.concatenate([logs, jnp.zeros_like(logs)], axis=0))
            for m in range(tiles):
                first, second = lines[2 * m : 2 * m + 1], lines[2 * m + 1 : 2 * m + 2]
                l_out[j, m : m + 1] = jnp.where(low_line, first, swap_halves(second))

    visits = (groups - 1 - group) * heads
    opening = jnp.where((idx < heads // 2) | (visits == 0), heads, 2)

    def served(t):
        visiting = (t >= opening) & (t < opening + visits)
        visitor = jnp.where(visiting, t - opening, 0)
        visitor = jnp.where(opening < heads, visitor, visits - 1 - visitor)
        own = jnp.where(t < opening, t, jnp.where(visiting, 0, heads + 1 - (t - visits)))
        target = group + jnp.where(visiting, 1 + lax.div(visitor, heads), 0)
        step = jnp.where(visiting, lax.rem(visitor, heads), own)
        return target * heads + partner(idx, step, heads)

    def serve(u, carry):
        js = [served(2 * u), served(2 * u + 1)]
        for j in js:

            @pl.when(j != me)
            def _(j=j):
                arrival(q_in.at[j], q_recv.at[j]).wait_recv()

        attend(js)
        for j in js:

            @pl.when(j != me)
            def _(j=j):
                o_copy(j).start()
                l_copy(j).start()

            @pl.when(j == me)
            def _(j=j):
                for m in range(tiles):
                    o_in[group, idx, m] = o_out[j, m]
                l_in[group, idx] = l_out[j]

        return carry

    lax.fori_loop(0, (devices - first_device) // 2, serve, 0)

    def absent(a, carry):
        o_in[a] = jnp.zeros(o_in.shape[1:], o_in.dtype)
        l_in[a] = jnp.full(l_in.shape[1:], masked_score, jnp.float32)
        return carry

    lax.fori_loop(group + 1, groups, absent, 0)

    def spread(body, start):
        if groups <= 2:
            for a in range(groups):
                start = body(a, start)
            return start
        return lax.fori_loop(0, groups, body, start)

    for i in range(pairs):
        ch = pair_of(i)

        def take_results(a, carry, i=i, ch=ch):
            def take(count):
                o_place = o_in.at[a, pl.ds(2 * ch, count)]
                arrival(o_place, o_recv.at[a, ch]).wait_recv()
                l_place = l_in.at[a, pl.ds(2 * ch, count)]
                arrival(l_place, l_recv.at[a, ch]).wait_recv()

            if i > 0:
                take(2)
            else:
                pl.when(a == group)(lambda: take(1))
                pl.when(a != group)(lambda: take(2))
            return carry

        lax.fori_loop(0, group + 1, take_results, 0)

        def lines(a, ch=ch):
            return l_in[a, pl.ds(2 * ch, 2)]

        start = jnp.full((2, tiles, LANES), masked_score, jnp.float32)
        highest = spread(lambda a, top: jnp.maximum(top, lines(a)), start)
        sums = spread(lambda a, acc: acc + jnp.exp(lines(a) - highest), jnp.zeros_like(start))
        logs = highest + jnp.log(sums)
        total_log[pl.ds(2 * ch, 2)] = logs

        def add_share(a, parts, ch=ch, logs=logs):
            share = jnp.exp(lines(a) - logs)
            share = [share[e, m : m + 1] for e in range(2) for m in range(tiles)]
            share.append(jnp.zeros((LANES - 2 * tiles, LANES), jnp.float32))
            columns = jnp.transpose(jnp.concatenate(share, axis=0))
            made = []
            for m in range(tiles):
                t0 = o_in[a, 2 * ch, m].astype(jnp.float32)
                t1 = o_in[a, 2 * ch + 1, m].astype(jnp.float32)
                both = (jnp.where(low, t0, swap_halves(t1)), jnp.where(low, swap_halves(t0), t1))
                for e in range(2):
                    r = 2 * m + e
                    here = columns[e * BLK : (e + 1) * BLK]
                    scale = jnp.where(low, here[:, m : m + 1], here[:, tiles + m : tiles + m + 1])
                    made.append(parts[r] + both[e] * scale)
            return tuple(made)

        made = spread(add_share, tuple(jnp.zeros((BLK, LANES), jnp.float32) for _ in range(blocks)))
        for r in range(blocks):
            columns = pl.ds(pl.multiple_of(ch * LANES, LANES), LANES)
            attended[r * BLK : (r + 1) * BLK, columns] = made[r].astype(jnp.bfloat16)

    for m in range(tiles):
        log_ref[:, m * LANES : (m + 1) * LANES] = total_log[:, m, :]

    load_o.wait()
    out_rows = rows // splits
    tile_width = min(512, wo.shape[1])
    chunks = wo.shape[1] // tile_width
    peers = [lax.rem(tp + d, splits) for d in range(splits)]

    def own_rows(d):
        return pl.ds(pl.multiple_of(peers[d] * out_rows, out_rows), out_rows)

    def hop(d, c):
        return pltpu.make_async_remote_copy(
            src_ref=stage.at[c, own_rows(d)],
            dst_ref=landed_ref.at[d - 1, :, pl.ds(c * tile_width, tile_width)],
            send_sem=tp_send.at[d - 1],
            recv_sem=tp_recv.at[d - 1],
            device_id={"tp": peers[d]},
            device_id_type=MESH,
        )

    def product(place, c):
        columns = slice(c * tile_width, (c + 1) * tile_width)
        made = jnp.dot(attended[place], wo[:, columns], preferred_element_type=jnp.float32)
        stage[c, place] = made.astype(jnp.bfloat16)

    for c in range(chunks):
        if c < chunks - 1:
            product(pl.ds(0, rows), c)
        else:
            for d in range(1, splits):
                product(own_rows(d), c)
        for d in range(1, splits):
            hop(d, c).start()
    product(own_rows(0), chunks - 1)
    for c in range(chunks):
        mine_ref[:, c * tile_width : (c + 1) * tile_width] = stage[c, own_rows(0)]

    def sent(ref, semaphore):
        arrival(ref, semaphore).wait_send()

    sent(kv_out.at[pl.ds(0, heads - 1)], kv_send.at[0])
    sent(q_out.at[pl.ds(0, heads - 1)], q_send.at[group])

    def sent_down(a, carry):
        sent(q_out, q_send.at[a])
        return carry

    lax.fori_loop(0, group, sent_down, 0)
    sent(o_out.at[pl.ds(0, heads - 1)], o_send.at[group])
    sent(l_out.at[pl.ds(0, heads - 1)], l_send.at[group])

    def sent_up(a, carry):
        sent(o_out.at[pl.ds(0, heads)], o_send.at[a])
        sent(l_out.at[pl.ds(0, heads)], l_send.at[a])
        return carry

    lax.fori_loop(group + 1, groups, sent_up, 0)
    for d in range(1, splits):
        sent(stage.at[:, own_rows(d)], tp_send.at[d - 1])
        arrival(landed_ref.at[d - 1], tp_recv.at[d - 1]).wait_recv()


def local(devices, splits, tokens, w_query, w_key, w_value, w_out, chosen):
    rows, depth = tokens.shape
    width = w_query.shape[1]
    out_width = w_out.shape[1]
    heads = width // HEAD_DIM
    pairs = heads // 2
    groups = devices // heads
    blocks = rows // BLK
    tiles = blocks // 2
    wide = 2 if pairs % 2 == 0 else 1

    out_rows = rows // splits
    tile_width = min(512, out_width)
    chunks = out_width // tile_width
    dma = pltpu.SemaphoreType.DMA
    bf16, f32 = jnp.bfloat16, jnp.float32
    mine, landed, logs = pl.pallas_call(
        functools.partial(layer_kernel, devices, splits),
        in_specs=[in_vmem()] + [in_hbm()] * 5,
        out_specs=[in_vmem()] * 3,
        out_shape=[
            jax.ShapeDtypeStruct((out_rows, out_width), bf16),
            jax.ShapeDtypeStruct((splits - 1, out_rows, out_width), bf16),
            jax.ShapeDtypeStruct((heads, rows), f32),
        ],
        scratch_shapes=[
            pltpu.VMEM((rows, depth), bf16),
            pltpu.VMEM((pairs // wide, depth, wide * LANES), bf16),
            pltpu.VMEM((pairs, depth, 2 * LANES), bf16),
            pltpu.VMEM((width, out_width), bf16),
            pltpu.VMEM((heads, blocks, BLK, LANES), bf16),
            pltpu.VMEM((heads, tiles, BLK, LANES), bf16),
            pltpu.VMEM((heads * blocks, BLK, LANES), bf16),
            pltpu.VMEM((heads * blocks, BLK, LANES), bf16),
            pltpu.VMEM(chosen.shape[::-1], jnp.int32),
            pltpu.SMEM(chosen.shape[::-1], jnp.int32),
            pltpu.VMEM((chosen.shape[0], chosen.shape[1] * BLK), f32),
            pltpu.VMEM((devices, tiles, BLK, LANES), bf16),
            pltpu.VMEM((devices, tiles, BLK, LANES), bf16),
            pltpu.VMEM((devices, tiles, LANES), f32),
            pltpu.VMEM((groups, heads, tiles, BLK, LANES), bf16),
            pltpu.VMEM((groups, heads, tiles, LANES), f32),
            pltpu.VMEM((heads, tiles, LANES), f32),
            pltpu.VMEM((rows, width), bf16),
            pltpu.VMEM((chunks, rows, tile_width), bf16),
            dma((3,)),
            dma((pairs,)),
            dma((pairs // wide,)),
            dma((1,)),
            dma((1,)),
            dma((groups,)),
            dma((devices,)),
            dma((groups,)),
            dma((groups, pairs)),
            dma((groups,)),
            dma((groups, pairs)),
            dma((splits - 1,)),
            dma((splits - 1,)),
        ],
        compiler_params=pltpu.CompilerParams(
            collective_id=0, has_side_effects=True, vmem_limit_bytes=VMEM_LIMIT
        ),
        name="layer",
    )(jnp.transpose(chosen), tokens, w_query, w_key, w_value, w_out)
    total = mine.astype(f32) + jnp.sum(landed.astype(f32), axis=0)
    return total.astype(bf16), logs


def solution(mesh):
    placed = (P("kv", None), P(None, "tp"), P(None, "tp"), P(None, "tp"), P("tp", None), P())
    return jax.shard_map(
        functools.partial(local, mesh.shape["kv"], mesh.shape["tp"]),
        mesh=mesh,
        in_specs=placed,
        out_specs=(P(("kv", "tp"), None), P("tp", "kv")),
        check_vma=False,
    )
```

```python
import functools

import jax
import jax.numpy as jnp
import numpy as np
from jax import lax
from jax.experimental import pallas as pl
from jax.experimental.pallas import tpu as pltpu
from jax.sharding import PartitionSpec as P

HEAD_DIM = 64
BLK = 64
LANES = 128
VMEM_LIMIT = 55_000_000
AHEAD = 2
LOG2_E = float(np.log2(np.e))

rotary_base = 500000.0
masked_score = -1e30

MESH = pl.DeviceIdType.MESH


def in_vmem():
    return pl.BlockSpec(memory_space=pltpu.VMEM)


def in_hbm():
    return pl.BlockSpec(memory_space=pltpu.HBM)


def partner(place, step, count):
    if count & (count - 1):
        return lax.rem(place + step, count)
    mixed, bit = 0, 1
    while bit < count:
        mixed = mixed + bit * lax.rem(lax.div(place, bit) + lax.div(step, bit), 2)
        bit *= 2
    return mixed


def swap_halves(tile):
    return pltpu.roll(tile, LANES // 2, 1)


def layer_kernel(
    devices, splits, chosen_ref, x_ref, wq_ref, wk_ref, wv_ref, wo_ref,
    mine_ref, landed_ref, log_ref,
    x, wq, wkv, wo, kv_out, q_out, kv_in, vk_in, lists, place_v, place_s, bias, q_in, o_out, l_out, o_in, l_in, total_log,
    attended, stage, load_sem, kv_load, q_load, kv_send, kv_recv, q_send, q_recv, o_send, o_recv, l_send, l_recv, tp_send, tp_recv,
):
    heads = kv_out.shape[0]
    pairs = heads // 2
    groups = devices // heads
    blocks = kv_out.shape[1]
    tiles = blocks // 2
    rows = blocks * BLK
    entries = chosen_ref.shape[0]
    high = heads // 2
    wide = wq.shape[2] // LANES

    me = lax.axis_index("kv")
    tp = lax.axis_index("tp")
    group = lax.div(me, heads)
    idx = lax.rem(me, heads)
    first_device = group * heads
    visited = idx >= high
    half = HEAD_DIM // 2

    def pair_of(i):
        return partner(lax.div(idx, 2), jnp.int32(i), pairs)

    def strip(ref, i):
        return ref.at[:, pl.ds(pl.multiple_of(pair_of(i) * LANES, LANES), LANES)]

    def load_q(i):
        target = wq.at[i // wide, :, pl.ds((i % wide) * LANES, LANES)]
        return pltpu.make_async_copy(strip(wq_ref, i), target, q_load.at[i // wide])

    def load_k(i):
        return pltpu.make_async_copy(strip(wk_ref, i), wkv.at[i, :, pl.ds(0, LANES)], kv_load.at[i])

    def load_v(i):
        return pltpu.make_async_copy(strip(wv_ref, i), wkv.at[i, :, pl.ds(LANES, LANES)], kv_load.at[i])

    def loaded(ref, semaphore):
        pltpu.make_async_copy(ref, ref, semaphore).wait()

    load_x = pltpu.make_async_copy(x_ref, x, load_sem.at[0])
    load_o = pltpu.make_async_copy(wo_ref, wo, load_sem.at[1])
    load_lists = pltpu.make_async_copy(chosen_ref, lists, load_sem.at[3])
    move_places = pltpu.make_async_copy(place_v, place_s, load_sem.at[2])

    load_x.start()
    load_lists.start()
    lowest = group == 0
    early = 1

    def start_kv(first, last):
        for i in range(first, last):
            load_k(i).start()
            load_v(i).start()

    def start_q():
        for i in range(pairs):
            load_q(i).start()

    pl.when(lowest)(lambda: start_kv(0, early))
    pl.when(jnp.logical_not(lowest))(start_q)

    barrier = pltpu.get_barrier_semaphore()

    def greet(d, carry):
        pl.semaphore_signal(
            barrier, inc=1, device_id={"kv": lax.rem(me + d, devices)}, device_id_type=MESH
        )
        return carry

    lax.fori_loop(1, devices, greet, 0)
    for d in range(1, splits):
        pl.semaphore_signal(barrier, inc=1, device_id={"tp": lax.rem(tp + d, splits)}, device_id_type=MESH)

    def kv_copy(slot, target):
        return pltpu.make_async_remote_copy(
            src_ref=kv_out.at[slot],
            dst_ref=kv_in.at[pl.ds(me * blocks, blocks)],
            send_sem=kv_send.at[lax.div(target, heads)],
            recv_sem=kv_recv.at[group],
            device_id={"kv": target},
            device_id_type=MESH,
        )

    def q_copy(slot, target):
        return pltpu.make_async_remote_copy(
            src_ref=q_out.at[slot],
            dst_ref=q_in.at[me],
            send_sem=q_send.at[lax.div(target, heads)],
            recv_sem=q_recv.at[me],
            device_id={"kv": target},
            device_id_type=MESH,
        )

    def o_copy(target):
        return pltpu.make_async_remote_copy(
            src_ref=o_out.at[target],
            dst_ref=o_in.at[group, idx],
            send_sem=o_send.at[lax.div(target, heads)],
            recv_sem=o_recv.at[group, lax.div(idx, 2)],
            device_id={"kv": target},
            device_id_type=MESH,
        )

    def l_copy(target):
        return pltpu.make_async_remote_copy(
            src_ref=l_out.at[target],
            dst_ref=l_in.at[group, idx],
            send_sem=l_send.at[lax.div(target, heads)],
            recv_sem=l_recv.at[group, lax.div(idx, 2)],
            device_id={"kv": target},
            device_id_type=MESH,
        )

    def arrival(ref, semaphore):
        return pltpu.make_async_remote_copy(
            src_ref=ref, dst_ref=ref, send_sem=semaphore, recv_sem=semaphore,
            device_id={"kv": me}, device_id_type=MESH,
        )

    load_x.wait()

    @pl.when(lowest)
    def _():
        start_kv(early, pairs)
        start_q()

    @pl.when(jnp.logical_not(lowest))
    def _():
        start_kv(0, pairs)

    low_rows = lax.broadcasted_iota(jnp.int32, (rows, LANES), 1) < LANES // 2
    turn_low = lax.broadcasted_iota(jnp.int32, (rows, LANES), 1) % HEAD_DIM < half

    def angles(count, step, start):
        channel = (lax.broadcasted_iota(jnp.int32, (count, LANES), 1) % half).astype(jnp.float32)
        position = lax.broadcasted_iota(jnp.int32, (count, LANES), 0) * step + start
        turn = position.astype(jnp.float32) * jnp.exp(channel * (-np.log(rotary_base) / half))
        return jnp.cos(turn), jnp.sin(turn)

    cos_fine, sin_fine = angles(8, 1, 0)
    cos_coarse, sin_coarse = angles(rows // 8, 8, me * rows)
    cos_parts, sin_parts = [], []
    for k in range(rows // 8):
        cos_k, sin_k = cos_coarse[k : k + 1], sin_coarse[k : k + 1]
        cos_parts.append(cos_k * cos_fine - sin_k * sin_fine)
        sin_parts.append(sin_k * cos_fine + cos_k * sin_fine)
    cos_part = jnp.concatenate(cos_parts, axis=0)
    sin_part = jnp.concatenate(sin_parts, axis=0)
    sin_part = jnp.where(turn_low, -sin_part, sin_part)

    def turned(part):
        other = jnp.where(turn_low, pltpu.roll(part, LANES - half, 1), pltpu.roll(part, half, 1))
        return part * cos_part + other * sin_part

    def make_kv(i):
        loaded(wkv.at[i], kv_load.at[i])
        made = jnp.dot(x[...], wkv[i], preferred_element_type=jnp.float32)
        keys = turned(made[:, :LANES])
        values = made[:, LANES:]
        even = jnp.where(low_rows, keys, swap_halves(values)).astype(jnp.bfloat16)
        odd = jnp.where(low_rows, swap_halves(keys), values).astype(jnp.bfloat16)
        for r in range(blocks):
            kv_out[2 * i, r] = even[r * BLK : (r + 1) * BLK]
            kv_out[2 * i + 1, r] = odd[r * BLK : (r + 1) * BLK]

    def make_q(i):
        loaded(wq.at[i // wide], q_load.at[i // wide])
        made = jnp.dot(x[...], wq[i // wide], preferred_element_type=jnp.float32)
        for e in range(wide):
            part = turned(made[:, e * LANES : (e + 1) * LANES]) * (HEAD_DIM**-0.5 * LOG2_E)
            swapped = swap_halves(part)
            low = low_rows[:BLK]
            for m in range(tiles):
                a = slice(2 * m * BLK, (2 * m + 1) * BLK)
                b = slice((2 * m + 1) * BLK, (2 * m + 2) * BLK)
                q_out[2 * (i + e), m] = jnp.where(low, part[a], swapped[b]).astype(jnp.bfloat16)
                q_out[2 * (i + e) + 1, m] = jnp.where(low, swapped[a], part[b]).astype(jnp.bfloat16)

    def send_kv(i):
        for e in range(2):
            head = 2 * pair_of(i) + e
            if i > 0:
                kv_copy(2 * i + e, first_device + head).start()
            else:
                pl.when(head != idx)(lambda e=e, head=head: kv_copy(2 * i + e, first_device + head).start())

    def send_q(i):
        for e in range(2):
            head = 2 * pair_of(i) + e
            if i > 0:
                q_copy(2 * i + e, first_device + head).start()
            else:
                pl.when(head != idx)(lambda e=e, head=head: q_copy(2 * i + e, first_device + head).start())

    def send_down():
        def send(a, carry):
            for i in range(pairs):
                for e in range(2):
                    head = 2 * pair_of(i) + e

                    @pl.when(head >= high)
                    def _(i=i, e=e, head=head):
                        q_copy(2 * i + e, a * heads + head).start()

            return carry

        lax.fori_loop(0, group, send, 0)

    def send_up():
        def send(a, carry):
            for i in range(pairs):
                for e in range(2):
                    head = 2 * pair_of(i) + e

                    @pl.when(head < high)
                    def _(i=i, e=e, head=head):
                        kv_copy(2 * i + e, a * heads + head).start()

            return carry

        lax.fori_loop(group + 1, groups, send, 0)

    def make_queries():
        for i in range(0, pairs, wide):
            make_q(i)

    @pl.when(jnp.logical_not(lowest))
    def _():
        make_queries()
        pl.semaphore_wait(barrier, devices - 1 + splits - 1)
        send_down()

    for i in range(pairs):
        make_kv(i)
        if i == 0:
            pl.when(lowest)(lambda: pl.semaphore_wait(barrier, devices - 1 + splits - 1))
        send_kv(i)
    send_up()
    pl.when(lowest)(make_queries)
    for i in range(pairs):
        send_q(i)
    load_o.start()

    load_lists.wait()
    place = lists[...]
    lowest_block = jnp.where(visited, first_device * blocks, 0)
    held = (place >= lowest_block) & (place < (first_device + heads) * blocks)
    place_v[...] = jnp.where(held, place, lowest_block)
    move_places.start()
    column = lax.broadcasted_iota(jnp.int32, (entries, entries * BLK), 1)
    slot = column // (8 * BLK) * 8 + column // BLK % 4 * 2 + column // (4 * BLK) % 2
    unit = (slot == lax.broadcasted_iota(jnp.int32, slot.shape, 0)).astype(jnp.float32)
    bias[...] = masked_score * (
        1.0
        - lax.dot_general(
            jnp.where(held, 1.0, 0.0), unit, (((0,), (0,)), ((), ())), preferred_element_type=jnp.float32
        )
    )
    move_places.wait()

    own_slot = lax.rem(idx, 2)
    for r in range(blocks):
        kv_in[me * blocks + r] = kv_out[own_slot, r]
    for m in range(tiles):
        q_in[me, m] = q_out[own_slot, m]

    low = lax.broadcasted_iota(jnp.int32, (BLK, LANES), 1) < LANES // 2
    lane = lax.broadcasted_iota(jnp.int32, (BLK, LANES), 1)
    low_line = lax.broadcasted_iota(jnp.int32, (1, LANES), 1) < LANES // 2

    arrival(kv_in.at[pl.ds(0, (heads - 1) * blocks)], kv_recv.at[group]).wait_recv()

    def swap_kv(k, carry):
        for r in range(blocks):
            place = k * blocks + r
            vk_in[place] = swap_halves(kv_in[place].astype(jnp.float32)).astype(jnp.bfloat16)
        return carry

    lax.fori_loop(first_device, first_device + heads, swap_kv, 0)

    def take_lower(a, carry):
        arrival(kv_in.at[pl.ds(0, heads * blocks)], kv_recv.at[a]).wait_recv()
        return lax.fori_loop(a * heads, (a + 1) * heads, swap_kv, carry)

    lax.fori_loop(0, jnp.where(visited, 0, group), take_lower, 0)

    def attend(js):
        stacks = []
        for j in js:
            for m in range(tiles):
                tile = q_in[j, m]
                swapped = swap_halves(tile.astype(jnp.float32)).astype(jnp.bfloat16)
                none = jnp.zeros_like(tile)
                for at_low, at_high in ((tile, swapped), (swapped, tile)):
                    stacks.append(
                        jnp.concatenate([jnp.where(low, at_low, none), jnp.where(low, none, at_high)], axis=0)
                    )

        def score(n):
            block = js[n // blocks] * blocks + n % blocks
            scores, values = [], []
            for lower in range(0, entries, 8):
                keys_here, values_here = [], []
                for s in range(lower, lower + 8, 2):
                    a = kv_in[place_s[s, block]]
                    b = vk_in[place_s[s + 1, block]]
                    keys_here.append(jnp.where(low, a, b))
                    values_here.append(jnp.where(low, b, a))
                made = lax.dot_general(
                    stacks[n], jnp.concatenate(keys_here, axis=0), (((1,), (1,)), ((), ())),
                    preferred_element_type=jnp.float32,
                )
                line = bias[pl.ds(block, 1), lower * BLK : (lower + 8) * BLK]
                scores += [made[:BLK] + line[:, : 4 * BLK], made[BLK:] + line[:, 4 * BLK :]]
                values.append(jnp.concatenate(values_here, axis=0))
            top = jnp.max(functools.reduce(jnp.maximum, scores), axis=1, keepdims=True)
            return scores, values, top

        def gather(n, scores, values, top):
            weights = [jnp.exp2(part - top) for part in scores]
            total = jnp.sum(functools.reduce(jnp.add, weights), axis=1, keepdims=True)
            made = 0.0
            for k, held_values in enumerate(values):
                rounded = jnp.concatenate([part.astype(jnp.bfloat16) for part in weights[2 * k : 2 * k + 2]], axis=0)
                made = made + jnp.dot(rounded, held_values, preferred_element_type=jnp.float32)
            if n % 2 == 0:
                summed = swap_halves(made[:BLK]) + made[BLK:]
            else:
                summed = made[:BLK] + swap_halves(made[BLK:])
            return summed / total, (top + jnp.log2(total)) * (1.0 / LOG2_E)

        ready, results = [], []
        for n in range(len(js) * blocks + AHEAD):
            if n < len(js) * blocks:
                ready.append(score(n))
            if n >= AHEAD:
                results.append(gather(n - AHEAD, *ready[n - AHEAD]))
        for k, j in enumerate(js):
            found = results[k * blocks : (k + 1) * blocks]
            logs = jnp.zeros((BLK, LANES), jnp.float32)
            for r in range(blocks):
                logs = jnp.where(lane == r, found[r][1], logs)
            for m in range(tiles):
                o_out[j, m] = jnp.where(low, found[2 * m][0], found[2 * m + 1][0]).astype(jnp.bfloat16)
            lines = jnp.transpose(jnp.concatenate([logs, jnp.zeros_like(logs)], axis=0))
            for m in range(tiles):
                first, second = lines[2 * m : 2 * m + 1], lines[2 * m + 1 : 2 * m + 2]
                l_out[j, m : m + 1] = jnp.where(low_line, first, swap_halves(second))

    batch = 2
    visits = jnp.where(visited, (groups - 1 - group) * heads, 0)
    opening = jnp.where(visits == 0, heads, 2)

    def served(t):
        visiting = (t >= opening) & (t < opening + visits)
        visitor = jnp.where(visiting, t - opening, 0)
        own = jnp.where(t < opening, t, jnp.where(visiting, 0, heads + 1 - (t - visits)))
        target = group + jnp.where(visiting, 1 + lax.div(visitor, heads), 0)
        step = jnp.where(visiting, lax.rem(visitor, heads), own)
        return target * heads + partner(idx, step, heads)

    def serve(u, carry):
        js = [served(batch * u + k) for k in range(batch)]
        for j in js:

            @pl.when(j != me)
            def _(j=j):
                arrival(q_in.at[j], q_recv.at[j]).wait_recv()

        attend(js)
        for j in js:

            @pl.when(j != me)
            def _(j=j):
                o_copy(j).start()
                l_copy(j).start()

            @pl.when(j == me)
            def _(j=j):
                for m in range(tiles):
                    o_in[group, idx, m] = o_out[j, m]
                l_in[group, idx] = l_out[j]

        return carry

    lax.fori_loop(0, lax.div(heads + visits, batch), serve, 0)

    def absent(a, carry):
        o_in[a] = jnp.zeros(o_in.shape[1:], o_in.dtype)
        l_in[a] = jnp.full(l_in.shape[1:], masked_score, jnp.float32)
        return carry

    lax.fori_loop(group + 1, groups, absent, 0)

    def partly_absent(a, carry):
        o_in[a, :high] = jnp.zeros((high,) + o_in.shape[2:], o_in.dtype)
        l_in[a, :high] = jnp.full((high,) + l_in.shape[2:], masked_score, jnp.float32)
        return carry

    lax.fori_loop(0, group, partly_absent, 0)

    def spread(body, start):
        if groups <= 2:
            for a in range(groups):
                start = body(a, start)
            return start
        return lax.fori_loop(0, groups, body, start)

    for i in range(pairs):
        ch = pair_of(i)

        def take_results(a, carry, i=i, ch=ch):
            def take(count):
                o_place = o_in.at[a, pl.ds(2 * ch, count)]
                arrival(o_place, o_recv.at[a, ch]).wait_recv()
                l_place = l_in.at[a, pl.ds(2 * ch, count)]
                arrival(l_place, l_recv.at[a, ch]).wait_recv()

            pl.when(a == group)(lambda: take(2 if i > 0 else 1))
            pl.when((a < group) & (2 * ch + 1 >= high))(lambda: take(min(2, high)))
            return carry

        lax.fori_loop(0, group + 1, take_results, 0)

        def lines(a, ch=ch):
            return l_in[a, pl.ds(2 * ch, 2)]

        start = jnp.full((2, tiles, LANES), masked_score, jnp.float32)
        highest = spread(lambda a, top: jnp.maximum(top, lines(a)), start)
        sums = spread(lambda a, acc: acc + jnp.exp(lines(a) - highest), jnp.zeros_like(start))
        logs = highest + jnp.log(sums)
        total_log[pl.ds(2 * ch, 2)] = logs

        def add_share(a, parts, ch=ch, logs=logs):
            share = jnp.exp(lines(a) - logs)
            share = [share[e, m : m + 1] for e in range(2) for m in range(tiles)]
            share.append(jnp.zeros((LANES - 2 * tiles, LANES), jnp.float32))
            columns = jnp.transpose(jnp.concatenate(share, axis=0))
            made = []
            for m in range(tiles):
                t0 = o_in[a, 2 * ch, m].astype(jnp.float32)
                t1 = o_in[a, 2 * ch + 1, m].astype(jnp.float32)
                both = (jnp.where(low, t0, swap_halves(t1)), jnp.where(low, swap_halves(t0), t1))
                for e in range(2):
                    r = 2 * m + e
                    here = columns[e * BLK : (e + 1) * BLK]
                    scale = jnp.where(low, here[:, m : m + 1], here[:, tiles + m : tiles + m + 1])
                    made.append(parts[r] + both[e] * scale)
            return tuple(made)

        made = spread(add_share, tuple(jnp.zeros((BLK, LANES), jnp.float32) for _ in range(blocks)))
        for r in range(blocks):
            columns = pl.ds(pl.multiple_of(ch * LANES, LANES), LANES)
            attended[r * BLK : (r + 1) * BLK, columns] = made[r].astype(jnp.bfloat16)

    for m in range(tiles):
        log_ref[:, m * LANES : (m + 1) * LANES] = total_log[:, m, :]

    load_o.wait()
    out_rows = rows // splits
    tile_width = min(512, wo.shape[1])
    chunks = wo.shape[1] // tile_width
    peers = [lax.rem(tp + d, splits) for d in range(splits)]

    def own_rows(d):
        return pl.ds(pl.multiple_of(peers[d] * out_rows, out_rows), out_rows)

    def hop(d, c):
        return pltpu.make_async_remote_copy(
            src_ref=stage.at[c, own_rows(d)],
            dst_ref=landed_ref.at[d - 1, :, pl.ds(c * tile_width, tile_width)],
            send_sem=tp_send.at[d - 1],
            recv_sem=tp_recv.at[d - 1],
            device_id={"tp": peers[d]},
            device_id_type=MESH,
        )

    def product(place, c):
        columns = slice(c * tile_width, (c + 1) * tile_width)
        made = jnp.dot(attended[place], wo[:, columns], preferred_element_type=jnp.float32)
        stage[c, place] = made.astype(jnp.bfloat16)

    for d in range(1, splits):
        for c in range(chunks):
            product(own_rows(d), c)
            hop(d, c).start()
    for c in range(chunks):
        columns = slice(c * tile_width, (c + 1) * tile_width)
        made = jnp.dot(attended[own_rows(0)], wo[:, columns], preferred_element_type=jnp.float32)
        mine_ref[:, columns] = made.astype(jnp.bfloat16)

    def sent(ref, semaphore):
        arrival(ref, semaphore).wait_send()

    sent(kv_out.at[pl.ds(0, heads - 1)], kv_send.at[group])
    sent(q_out.at[pl.ds(0, heads - 1)], q_send.at[group])

    def sent_down(a, carry):
        sent(q_out.at[pl.ds(0, heads - high)], q_send.at[a])
        return carry

    lax.fori_loop(0, group, sent_down, 0)
    sent(o_out.at[pl.ds(0, heads - 1)], o_send.at[group])
    sent(l_out.at[pl.ds(0, heads - 1)], l_send.at[group])

    def sent_up(a, carry):
        sent(kv_out.at[pl.ds(0, high)], kv_send.at[a])

        @pl.when(visited)
        def _():
            sent(o_out.at[pl.ds(0, heads)], o_send.at[a])
            sent(l_out.at[pl.ds(0, heads)], l_send.at[a])

        return carry

    lax.fori_loop(group + 1, groups, sent_up, 0)
    for d in range(1, splits):
        sent(stage.at[:, own_rows(d)], tp_send.at[d - 1])
        arrival(landed_ref.at[d - 1], tp_recv.at[d - 1]).wait_recv()


def local(devices, splits, tokens, w_query, w_key, w_value, w_out, chosen):
    rows, depth = tokens.shape
    width = w_query.shape[1]
    out_width = w_out.shape[1]
    heads = width // HEAD_DIM
    pairs = heads // 2
    groups = devices // heads
    blocks = rows // BLK
    tiles = blocks // 2
    wide = 2 if pairs % 2 == 0 else 1

    out_rows = rows // splits
    tile_width = min(512, out_width)
    chunks = out_width // tile_width
    dma = pltpu.SemaphoreType.DMA
    bf16, f32 = jnp.bfloat16, jnp.float32
    mine, landed, logs = pl.pallas_call(
        functools.partial(layer_kernel, devices, splits),
        in_specs=[in_hbm()] * 6,
        out_specs=[in_vmem()] * 3,
        out_shape=[
            jax.ShapeDtypeStruct((out_rows, out_width), bf16),
            jax.ShapeDtypeStruct((splits - 1, out_rows, out_width), bf16),
            jax.ShapeDtypeStruct((heads, rows), f32),
        ],
        scratch_shapes=[
            pltpu.VMEM((rows, depth), bf16),
            pltpu.VMEM((pairs // wide, depth, wide * LANES), bf16),
            pltpu.VMEM((pairs, depth, 2 * LANES), bf16),
            pltpu.VMEM((width, out_width), bf16),
            pltpu.VMEM((heads, blocks, BLK, LANES), bf16),
            pltpu.VMEM((heads, tiles, BLK, LANES), bf16),
            pltpu.VMEM((devices * blocks, BLK, LANES), bf16),
            pltpu.VMEM((devices * blocks, BLK, LANES), bf16),
            pltpu.VMEM(chosen.shape[::-1], jnp.int32),
            pltpu.VMEM(chosen.shape[::-1], jnp.int32),
            pltpu.SMEM(chosen.shape[::-1], jnp.int32),
            pltpu.VMEM((chosen.shape[0], chosen.shape[1] * BLK), f32),
            pltpu.VMEM((devices, tiles, BLK, LANES), bf16),
            pltpu.VMEM((devices, tiles, BLK, LANES), bf16),
            pltpu.VMEM((devices, tiles, LANES), f32),
            pltpu.VMEM((groups, heads, tiles, BLK, LANES), bf16),
            pltpu.VMEM((groups, heads, tiles, LANES), f32),
            pltpu.VMEM((heads, tiles, LANES), f32),
            pltpu.VMEM((rows, width), bf16),
            pltpu.VMEM((chunks, rows, tile_width), bf16),
            dma((4,)),
            dma((pairs,)),
            dma((pairs // wide,)),
            dma((groups,)),
            dma((groups,)),
            dma((groups,)),
            dma((devices,)),
            dma((groups,)),
            dma((groups, pairs)),
            dma((groups,)),
            dma((groups, pairs)),
            dma((splits - 1,)),
            dma((splits - 1,)),
        ],
        compiler_params=pltpu.CompilerParams(
            collective_id=0, has_side_effects=True, vmem_limit_bytes=VMEM_LIMIT
        ),
        name="layer",
    )(pltpu.with_memory_space_constraint(jnp.transpose(chosen), pltpu.HBM), tokens, w_query, w_key, w_value, w_out)
    total = mine.astype(f32) + jnp.sum(landed.astype(f32), axis=0)
    return total.astype(bf16), logs


def solution(mesh):
    placed = (P("kv", None), P(None, "tp"), P(None, "tp"), P(None, "tp"), P("tp", None), P())
    return jax.shard_map(
        functools.partial(local, mesh.shape["kv"], mesh.shape["tp"]),
        mesh=mesh,
        in_specs=placed,
        out_specs=(P(("kv", "tp"), None), P("tp", "kv")),
        check_vma=False,
    )
```

```python
import functools

import jax
import jax.numpy as jnp
import numpy as np
from jax import lax
from jax.experimental import pallas as pl
from jax.experimental.pallas import tpu as pltpu
from jax.sharding import PartitionSpec as P

HEAD_DIM = 64
BLK = 64
LANES = 128
VMEM_LIMIT = 55_000_000
AHEAD = 2
LOG2_E = float(np.log2(np.e))

rotary_base = 500000.0
masked_score = -1e30

MESH = pl.DeviceIdType.MESH


def in_vmem():
    return pl.BlockSpec(memory_space=pltpu.VMEM)


def in_hbm():
    return pl.BlockSpec(memory_space=pltpu.HBM)


def partner(place, step, count):
    if count & (count - 1):
        return lax.rem(place + step, count)
    mixed, bit = 0, 1
    while bit < count:
        mixed = mixed + bit * lax.rem(lax.div(place, bit) + lax.div(step, bit), 2)
        bit *= 2
    return mixed


def swap_halves(tile):
    return pltpu.roll(tile, LANES // 2, 1)


def layer_kernel(
    devices, splits, chosen_ref, x_ref, wq_ref, wk_ref, wv_ref, wo_ref,
    mine_ref, landed_ref, log_ref,
    x, wq, wkv, wo, kv_out, q_out, kv_in, vk_in, lists, place_v, place_s, bias, q_in, o_out, l_out, o_in, l_in, total_log,
    attended, stage, load_sem, kv_load, q_load, kv_send, kv_recv, q_send, q_recv, o_send, o_recv, l_send, l_recv, tp_send, tp_recv,
):
    heads = kv_out.shape[0]
    pairs = heads // 2
    groups = devices // heads
    blocks = kv_out.shape[1]
    tiles = blocks // 2
    rows = blocks * BLK
    entries = chosen_ref.shape[0]
    high = heads // 2
    wide = wq.shape[2] // LANES
    both = wkv.shape[2] // (2 * LANES)

    me = lax.axis_index("kv")
    tp = lax.axis_index("tp")
    group = lax.div(me, heads)
    idx = lax.rem(me, heads)
    first_device = group * heads
    visited = idx >= high
    half = HEAD_DIM // 2

    def pair_of(i):
        return partner(lax.div(idx, 2), jnp.int32(i), pairs)

    def strip(ref, i):
        return ref.at[:, pl.ds(pl.multiple_of(pair_of(i) * LANES, LANES), LANES)]

    def load_q(i):
        target = wq.at[i // wide, :, pl.ds((i % wide) * LANES, LANES)]
        return pltpu.make_async_copy(strip(wq_ref, i), target, q_load.at[i // wide])

    def load_k(i):
        target = wkv.at[i // both, :, pl.ds(i % both * 2 * LANES, LANES)]
        return pltpu.make_async_copy(strip(wk_ref, i), target, kv_load.at[i // both])

    def load_v(i):
        target = wkv.at[i // both, :, pl.ds((i % both * 2 + 1) * LANES, LANES)]
        return pltpu.make_async_copy(strip(wv_ref, i), target, kv_load.at[i // both])

    def loaded(ref, semaphore):
        pltpu.make_async_copy(ref, ref, semaphore).wait()

    load_x = pltpu.make_async_copy(x_ref, x, load_sem.at[0])
    load_o = pltpu.make_async_copy(wo_ref, wo, load_sem.at[1])
    load_lists = pltpu.make_async_copy(chosen_ref, lists, load_sem.at[3])
    move_places = pltpu.make_async_copy(place_v, place_s, load_sem.at[2])

    load_x.start()
    load_lists.start()
    lowest = group == 0
    early = both

    def start_kv(first, last):
        for i in range(first, last):
            load_k(i).start()
            load_v(i).start()

    def start_q():
        for i in range(pairs):
            load_q(i).start()

    pl.when(lowest)(lambda: start_kv(0, early))
    pl.when(jnp.logical_not(lowest))(start_q)

    barrier = pltpu.get_barrier_semaphore()

    def greet(d, carry):
        pl.semaphore_signal(
            barrier, inc=1, device_id={"kv": lax.rem(me + d, devices)}, device_id_type=MESH
        )
        return carry

    lax.fori_loop(1, devices, greet, 0)
    for d in range(1, splits):
        pl.semaphore_signal(barrier, inc=1, device_id={"tp": lax.rem(tp + d, splits)}, device_id_type=MESH)

    def kv_copy(slot, target):
        return pltpu.make_async_remote_copy(
            src_ref=kv_out.at[slot],
            dst_ref=kv_in.at[pl.ds(me * blocks, blocks)],
            send_sem=kv_send.at[lax.div(target, heads)],
            recv_sem=kv_recv.at[group],
            device_id={"kv": target},
            device_id_type=MESH,
        )

    def q_copy(slot, target):
        return pltpu.make_async_remote_copy(
            src_ref=q_out.at[slot],
            dst_ref=q_in.at[me],
            send_sem=q_send.at[lax.div(target, heads)],
            recv_sem=q_recv.at[me],
            device_id={"kv": target},
            device_id_type=MESH,
        )

    def o_copy(target):
        return pltpu.make_async_remote_copy(
            src_ref=o_out.at[target],
            dst_ref=o_in.at[group, idx],
            send_sem=o_send.at[lax.div(target, heads)],
            recv_sem=o_recv.at[group, lax.div(idx, 2)],
            device_id={"kv": target},
            device_id_type=MESH,
        )

    def l_copy(target):
        return pltpu.make_async_remote_copy(
            src_ref=l_out.at[target],
            dst_ref=l_in.at[group, idx],
            send_sem=l_send.at[lax.div(target, heads)],
            recv_sem=l_recv.at[group, lax.div(idx, 2)],
            device_id={"kv": target},
            device_id_type=MESH,
        )

    def arrival(ref, semaphore):
        return pltpu.make_async_remote_copy(
            src_ref=ref, dst_ref=ref, send_sem=semaphore, recv_sem=semaphore,
            device_id={"kv": me}, device_id_type=MESH,
        )

    load_x.wait()

    @pl.when(lowest)
    def _():
        start_kv(early, pairs)
        start_q()

    @pl.when(jnp.logical_not(lowest))
    def _():
        start_kv(0, pairs)

    low_rows = lax.broadcasted_iota(jnp.int32, (rows, LANES), 1) < LANES // 2
    turn_low = lax.broadcasted_iota(jnp.int32, (rows, LANES), 1) % HEAD_DIM < half

    def angles(count, step, start):
        channel = (lax.broadcasted_iota(jnp.int32, (count, LANES), 1) % half).astype(jnp.float32)
        position = lax.broadcasted_iota(jnp.int32, (count, LANES), 0) * step + start
        turn = position.astype(jnp.float32) * jnp.exp(channel * (-np.log(rotary_base) / half))
        return jnp.cos(turn), jnp.sin(turn)

    cos_fine, sin_fine = angles(8, 1, 0)
    cos_coarse, sin_coarse = angles(rows // 8, 8, me * rows)
    cos_parts, sin_parts = [], []
    for k in range(rows // 8):
        cos_k, sin_k = cos_coarse[k : k + 1], sin_coarse[k : k + 1]
        cos_parts.append(cos_k * cos_fine - sin_k * sin_fine)
        sin_parts.append(sin_k * cos_fine + cos_k * sin_fine)
    cos_part = jnp.concatenate(cos_parts, axis=0)
    sin_part = jnp.concatenate(sin_parts, axis=0)
    sin_part = jnp.where(turn_low, -sin_part, sin_part)

    def turned(part):
        other = jnp.where(turn_low, pltpu.roll(part, LANES - half, 1), pltpu.roll(part, half, 1))
        return part * cos_part + other * sin_part

    def make_kv(first):
        loaded(wkv.at[first // both], kv_load.at[first // both])
        made = jnp.dot(x[...], wkv[first // both], preferred_element_type=jnp.float32)
        for i in range(first, first + both):
            lane = (i - first) * 2 * LANES
            keys = turned(made[:, lane : lane + LANES])
            values = made[:, lane + LANES : lane + 2 * LANES]
            even = jnp.where(low_rows, keys, swap_halves(values)).astype(jnp.bfloat16)
            odd = jnp.where(low_rows, swap_halves(keys), values).astype(jnp.bfloat16)
            for r in range(blocks):
                kv_out[2 * i, r] = even[r * BLK : (r + 1) * BLK]
                kv_out[2 * i + 1, r] = odd[r * BLK : (r + 1) * BLK]

    def make_q(i):
        loaded(wq.at[i // wide], q_load.at[i // wide])
        made = jnp.dot(x[...], wq[i // wide], preferred_element_type=jnp.float32)
        for e in range(wide):
            part = turned(made[:, e * LANES : (e + 1) * LANES]) * (HEAD_DIM**-0.5 * LOG2_E)
            swapped = swap_halves(part)
            low = low_rows[:BLK]
            for m in range(tiles):
                a = slice(2 * m * BLK, (2 * m + 1) * BLK)
                b = slice((2 * m + 1) * BLK, (2 * m + 2) * BLK)
                q_out[2 * (i + e), m] = jnp.where(low, part[a], swapped[b]).astype(jnp.bfloat16)
                q_out[2 * (i + e) + 1, m] = jnp.where(low, swapped[a], part[b]).astype(jnp.bfloat16)

    def send_kv(i):
        for e in range(2):
            head = 2 * pair_of(i) + e
            if i > 0:
                kv_copy(2 * i + e, first_device + head).start()
            else:
                pl.when(head != idx)(lambda e=e, head=head: kv_copy(2 * i + e, first_device + head).start())

    def send_q(i):
        for e in range(2):
            head = 2 * pair_of(i) + e
            if i > 0:
                q_copy(2 * i + e, first_device + head).start()
            else:
                pl.when(head != idx)(lambda e=e, head=head: q_copy(2 * i + e, first_device + head).start())

    def send_down():
        def send(a, carry):
            for i in range(pairs):
                for e in range(2):
                    head = 2 * pair_of(i) + e

                    @pl.when(head >= high)
                    def _(i=i, e=e, head=head):
                        q_copy(2 * i + e, a * heads + head).start()

            return carry

        lax.fori_loop(0, group, send, 0)

    def send_up():
        def send(a, carry):
            for i in range(pairs):
                for e in range(2):
                    head = 2 * pair_of(i) + e

                    @pl.when(head < high)
                    def _(i=i, e=e, head=head):
                        kv_copy(2 * i + e, a * heads + head).start()

            return carry

        lax.fori_loop(group + 1, groups, send, 0)

    def make_queries():
        for i in range(0, pairs, wide):
            make_q(i)

    @pl.when(jnp.logical_not(lowest))
    def _():
        make_queries()
        pl.semaphore_wait(barrier, devices - 1 + splits - 1)
        send_down()

    for i in range(0, pairs, both):
        make_kv(i)
        if i == 0:
            pl.when(lowest)(lambda: pl.semaphore_wait(barrier, devices - 1 + splits - 1))
        for e in range(both):
            send_kv(i + e)
    send_up()
    pl.when(lowest)(make_queries)
    for i in range(pairs):
        send_q(i)
    load_o.start()

    load_lists.wait()
    place = lists[...]
    lowest_block = jnp.where(visited, first_device * blocks, 0)
    held = (place >= lowest_block) & (place < (first_device + heads) * blocks)
    place_v[...] = jnp.where(held, place, lowest_block)
    move_places.start()
    column = lax.broadcasted_iota(jnp.int32, (entries, entries * BLK), 1)
    slot = column // (8 * BLK) * 8 + column // BLK % 4 * 2 + column // (4 * BLK) % 2
    unit = (slot == lax.broadcasted_iota(jnp.int32, slot.shape, 0)).astype(jnp.float32)
    bias[...] = masked_score * (
        1.0
        - lax.dot_general(
            jnp.where(held, 1.0, 0.0), unit, (((0,), (0,)), ((), ())), preferred_element_type=jnp.float32
        )
    )
    move_places.wait()

    own_slot = lax.rem(idx, 2)
    for r in range(blocks):
        kv_in[me * blocks + r] = kv_out[own_slot, r]
    for m in range(tiles):
        q_in[me, m] = q_out[own_slot, m]

    low = lax.broadcasted_iota(jnp.int32, (BLK, LANES), 1) < LANES // 2
    lane = lax.broadcasted_iota(jnp.int32, (BLK, LANES), 1)
    low_line = lax.broadcasted_iota(jnp.int32, (1, LANES), 1) < LANES // 2

    arrival(kv_in.at[pl.ds(0, (heads - 1) * blocks)], kv_recv.at[group]).wait_recv()

    def swap_kv(k, carry):
        for r in range(blocks):
            place = k * blocks + r
            vk_in[place] = swap_halves(kv_in[place].astype(jnp.float32)).astype(jnp.bfloat16)
        return carry

    lax.fori_loop(first_device, first_device + heads, swap_kv, 0)

    def take_lower(a, carry):
        arrival(kv_in.at[pl.ds(0, heads * blocks)], kv_recv.at[a]).wait_recv()
        return lax.fori_loop(a * heads, (a + 1) * heads, swap_kv, carry)

    lax.fori_loop(0, jnp.where(visited, 0, group), take_lower, 0)

    def attend(js, entries):
        stacks = []
        for j in js:
            for m in range(tiles):
                tile = q_in[j, m]
                swapped = swap_halves(tile.astype(jnp.float32)).astype(jnp.bfloat16)
                none = jnp.zeros_like(tile)
                for at_low, at_high in ((tile, swapped), (swapped, tile)):
                    stacks.append(
                        jnp.concatenate([jnp.where(low, at_low, none), jnp.where(low, none, at_high)], axis=0)
                    )

        def score(n):
            block = js[n // blocks] * blocks + n % blocks
            scores, values = [], []
            for lower in range(0, entries, 8):
                keys_here, values_here = [], []
                for s in range(lower, lower + 8, 2):
                    a = kv_in[place_s[s, block]]
                    b = vk_in[place_s[s + 1, block]]
                    keys_here.append(jnp.where(low, a, b))
                    values_here.append(jnp.where(low, b, a))
                made = lax.dot_general(
                    stacks[n], jnp.concatenate(keys_here, axis=0), (((1,), (1,)), ((), ())),
                    preferred_element_type=jnp.float32,
                )
                line = bias[pl.ds(block, 1), lower * BLK : (lower + 8) * BLK]
                scores += [made[:BLK] + line[:, : 4 * BLK], made[BLK:] + line[:, 4 * BLK :]]
                values.append(jnp.concatenate(values_here, axis=0))
            top = jnp.max(functools.reduce(jnp.maximum, scores), axis=1, keepdims=True)
            return scores, values, top

        def gather(n, scores, values, top):
            weights = [jnp.exp2(part - top) for part in scores]
            total = jnp.sum(functools.reduce(jnp.add, weights), axis=1, keepdims=True)
            made = 0.0
            for k, held_values in enumerate(values):
                rounded = jnp.concatenate([part.astype(jnp.bfloat16) for part in weights[2 * k : 2 * k + 2]], axis=0)
                made = made + jnp.dot(rounded, held_values, preferred_element_type=jnp.float32)
            if n % 2 == 0:
                summed = swap_halves(made[:BLK]) + made[BLK:]
            else:
                summed = made[:BLK] + swap_halves(made[BLK:])
            return summed / total, (top + jnp.log2(total)) * (1.0 / LOG2_E)

        ready, results = [], []
        for n in range(len(js) * blocks + AHEAD):
            if n < len(js) * blocks:
                ready.append(score(n))
            if n >= AHEAD:
                results.append(gather(n - AHEAD, *ready[n - AHEAD]))
        for k, j in enumerate(js):
            found = results[k * blocks : (k + 1) * blocks]
            logs = jnp.zeros((BLK, LANES), jnp.float32)
            for r in range(blocks):
                logs = jnp.where(lane == r, found[r][1], logs)
            for m in range(tiles):
                o_out[j, m] = jnp.where(low, found[2 * m][0], found[2 * m + 1][0]).astype(jnp.bfloat16)
            lines = jnp.transpose(jnp.concatenate([logs, jnp.zeros_like(logs)], axis=0))
            for m in range(tiles):
                first, second = lines[2 * m : 2 * m + 1], lines[2 * m + 1 : 2 * m + 2]
                l_out[j, m : m + 1] = jnp.where(low_line, first, swap_halves(second))

    batch = 2
    visits = jnp.where(visited, (groups - 1 - group) * heads, 0)
    opening = jnp.where(visits == 0, heads, 2)

    def served(t):
        visiting = (t >= opening) & (t < opening + visits)
        visitor = jnp.where(visiting, t - opening, 0)
        own = jnp.where(t < opening, t, jnp.where(visiting, 0, heads + 1 - (t - visits)))
        target = group + jnp.where(visiting, 1 + lax.div(visitor, heads), 0)
        step = jnp.where(visiting, lax.rem(visitor, heads), own)
        return target * heads + partner(idx, step, heads)

    def serve(u, carry):
        js = [served(batch * u + k) for k in range(batch)]
        for j in js:

            @pl.when(j != me)
            def _(j=j):
                arrival(q_in.at[j], q_recv.at[j]).wait_recv()

        short = functools.reduce(jnp.maximum, js) < 8 // blocks
        pl.when(short)(lambda: attend(js, 8))
        pl.when(jnp.logical_not(short))(lambda: attend(js, entries))
        for j in js:

            @pl.when(j != me)
            def _(j=j):
                o_copy(j).start()
                l_copy(j).start()

            @pl.when(j == me)
            def _(j=j):
                for m in range(tiles):
                    o_in[group, idx, m] = o_out[j, m]
                l_in[group, idx] = l_out[j]

        return carry

    lax.fori_loop(0, lax.div(heads + visits, batch), serve, 0)

    def absent(a, carry):
        o_in[a] = jnp.zeros(o_in.shape[1:], o_in.dtype)
        l_in[a] = jnp.full(l_in.shape[1:], masked_score, jnp.float32)
        return carry

    lax.fori_loop(group + 1, groups, absent, 0)

    def partly_absent(a, carry):
        o_in[a, :high] = jnp.zeros((high,) + o_in.shape[2:], o_in.dtype)
        l_in[a, :high] = jnp.full((high,) + l_in.shape[2:], masked_score, jnp.float32)
        return carry

    lax.fori_loop(0, group, partly_absent, 0)

    def spread(body, start):
        if groups <= 2:
            for a in range(groups):
                start = body(a, start)
            return start
        return lax.fori_loop(0, groups, body, start)

    for i in range(pairs):
        ch = pair_of(i)

        def take_results(a, carry, i=i, ch=ch):
            def take(count):
                o_place = o_in.at[a, pl.ds(2 * ch, count)]
                arrival(o_place, o_recv.at[a, ch]).wait_recv()
                l_place = l_in.at[a, pl.ds(2 * ch, count)]
                arrival(l_place, l_recv.at[a, ch]).wait_recv()

            pl.when(a == group)(lambda: take(2 if i > 0 else 1))
            pl.when((a < group) & (2 * ch + 1 >= high))(lambda: take(min(2, high)))
            return carry

        lax.fori_loop(0, group + 1, take_results, 0)

        def lines(a, ch=ch):
            return l_in[a, pl.ds(2 * ch, 2)]

        start = jnp.full((2, tiles, LANES), masked_score, jnp.float32)
        highest = spread(lambda a, top: jnp.maximum(top, lines(a)), start)
        sums = spread(lambda a, acc: acc + jnp.exp(lines(a) - highest), jnp.zeros_like(start))
        logs = highest + jnp.log(sums)
        total_log[pl.ds(2 * ch, 2)] = logs

        def add_share(a, parts, ch=ch, logs=logs):
            share = jnp.exp(lines(a) - logs)
            share = [share[e, m : m + 1] for e in range(2) for m in range(tiles)]
            share.append(jnp.zeros((LANES - 2 * tiles, LANES), jnp.float32))
            columns = jnp.transpose(jnp.concatenate(share, axis=0))
            made = []
            for m in range(tiles):
                t0 = o_in[a, 2 * ch, m].astype(jnp.float32)
                t1 = o_in[a, 2 * ch + 1, m].astype(jnp.float32)
                both = (jnp.where(low, t0, swap_halves(t1)), jnp.where(low, swap_halves(t0), t1))
                for e in range(2):
                    r = 2 * m + e
                    here = columns[e * BLK : (e + 1) * BLK]
                    scale = jnp.where(low, here[:, m : m + 1], here[:, tiles + m : tiles + m + 1])
                    made.append(parts[r] + both[e] * scale)
            return tuple(made)

        made = spread(add_share, tuple(jnp.zeros((BLK, LANES), jnp.float32) for _ in range(blocks)))
        for r in range(blocks):
            columns = pl.ds(pl.multiple_of(ch * LANES, LANES), LANES)
            attended[r * BLK : (r + 1) * BLK, columns] = made[r].astype(jnp.bfloat16)

    for m in range(tiles):
        log_ref[:, m * LANES : (m + 1) * LANES] = total_log[:, m, :]

    load_o.wait()
    out_rows = rows // splits
    tile_width = min(512, wo.shape[1])
    chunks = wo.shape[1] // tile_width
    peers = [lax.rem(tp + d, splits) for d in range(splits)]

    def own_rows(d):
        return pl.ds(pl.multiple_of(peers[d] * out_rows, out_rows), out_rows)

    def hop(d, c):
        return pltpu.make_async_remote_copy(
            src_ref=stage.at[c, own_rows(d)],
            dst_ref=landed_ref.at[d - 1, :, pl.ds(c * tile_width, tile_width)],
            send_sem=tp_send.at[d - 1],
            recv_sem=tp_recv.at[d - 1],
            device_id={"tp": peers[d]},
            device_id_type=MESH,
        )

    def product(place, c):
        columns = slice(c * tile_width, (c + 1) * tile_width)
        made = jnp.dot(attended[place], wo[:, columns], preferred_element_type=jnp.float32)
        stage[c, place] = made.astype(jnp.bfloat16)

    for d in range(1, splits):
        for c in range(chunks):
            product(own_rows(d), c)
            hop(d, c).start()
    for c in range(chunks):
        columns = slice(c * tile_width, (c + 1) * tile_width)
        made = jnp.dot(attended[own_rows(0)], wo[:, columns], preferred_element_type=jnp.float32)
        mine_ref[:, columns] = made.astype(jnp.bfloat16)

    def sent(ref, semaphore):
        arrival(ref, semaphore).wait_send()

    sent(kv_out.at[pl.ds(0, heads - 1)], kv_send.at[group])
    sent(q_out.at[pl.ds(0, heads - 1)], q_send.at[group])

    def sent_down(a, carry):
        sent(q_out.at[pl.ds(0, heads - high)], q_send.at[a])
        return carry

    lax.fori_loop(0, group, sent_down, 0)
    sent(o_out.at[pl.ds(0, heads - 1)], o_send.at[group])
    sent(l_out.at[pl.ds(0, heads - 1)], l_send.at[group])

    def sent_up(a, carry):
        sent(kv_out.at[pl.ds(0, high)], kv_send.at[a])

        @pl.when(visited)
        def _():
            sent(o_out.at[pl.ds(0, heads)], o_send.at[a])
            sent(l_out.at[pl.ds(0, heads)], l_send.at[a])

        return carry

    lax.fori_loop(group + 1, groups, sent_up, 0)
    for d in range(1, splits):
        sent(stage.at[:, own_rows(d)], tp_send.at[d - 1])
        arrival(landed_ref.at[d - 1], tp_recv.at[d - 1]).wait_recv()


def local(devices, splits, tokens, w_query, w_key, w_value, w_out, chosen):
    rows, depth = tokens.shape
    width = w_query.shape[1]
    out_width = w_out.shape[1]
    heads = width // HEAD_DIM
    pairs = heads // 2
    groups = devices // heads
    blocks = rows // BLK
    tiles = blocks // 2
    wide = pairs
    both = 2 if pairs % 2 == 0 else 1

    out_rows = rows // splits
    tile_width = min(512, out_width)
    chunks = out_width // tile_width
    dma = pltpu.SemaphoreType.DMA
    bf16, f32 = jnp.bfloat16, jnp.float32
    mine, landed, logs = pl.pallas_call(
        functools.partial(layer_kernel, devices, splits),
        in_specs=[in_hbm()] * 6,
        out_specs=[in_vmem()] * 3,
        out_shape=[
            jax.ShapeDtypeStruct((out_rows, out_width), bf16),
            jax.ShapeDtypeStruct((splits - 1, out_rows, out_width), bf16),
            jax.ShapeDtypeStruct((heads, rows), f32),
        ],
        scratch_shapes=[
            pltpu.VMEM((rows, depth), bf16),
            pltpu.VMEM((pairs // wide, depth, wide * LANES), bf16),
            pltpu.VMEM((pairs // both, depth, both * 2 * LANES), bf16),
            pltpu.VMEM((width, out_width), bf16),
            pltpu.VMEM((heads, blocks, BLK, LANES), bf16),
            pltpu.VMEM((heads, tiles, BLK, LANES), bf16),
            pltpu.VMEM((devices * blocks, BLK, LANES), bf16),
            pltpu.VMEM((devices * blocks, BLK, LANES), bf16),
            pltpu.VMEM(chosen.shape[::-1], jnp.int32),
            pltpu.VMEM(chosen.shape[::-1], jnp.int32),
            pltpu.SMEM(chosen.shape[::-1], jnp.int32),
            pltpu.VMEM((chosen.shape[0], chosen.shape[1] * BLK), f32),
            pltpu.VMEM((devices, tiles, BLK, LANES), bf16),
            pltpu.VMEM((devices, tiles, BLK, LANES), bf16),
            pltpu.VMEM((devices, tiles, LANES), f32),
            pltpu.VMEM((groups, heads, tiles, BLK, LANES), bf16),
            pltpu.VMEM((groups, heads, tiles, LANES), f32),
            pltpu.VMEM((heads, tiles, LANES), f32),
            pltpu.VMEM((rows, width), bf16),
            pltpu.VMEM((chunks, rows, tile_width), bf16),
            dma((4,)),
            dma((pairs // both,)),
            dma((pairs // wide,)),
            dma((groups,)),
            dma((groups,)),
            dma((groups,)),
            dma((devices,)),
            dma((groups,)),
            dma((groups, pairs)),
            dma((groups,)),
            dma((groups, pairs)),
            dma((splits - 1,)),
            dma((splits - 1,)),
        ],
        compiler_params=pltpu.CompilerParams(
            collective_id=0, has_side_effects=True, vmem_limit_bytes=VMEM_LIMIT
        ),
        name="layer",
    )(pltpu.with_memory_space_constraint(jnp.transpose(chosen), pltpu.HBM), tokens, w_query, w_key, w_value, w_out)
    total = mine.astype(f32) + jnp.sum(landed.astype(f32), axis=0)
    return total.astype(bf16), logs


def solution(mesh):
    placed = (P("kv", None), P(None, "tp"), P(None, "tp"), P(None, "tp"), P("tp", None), P())
    return jax.shard_map(
        functools.partial(local, mesh.shape["kv"], mesh.shape["tp"]),
        mesh=mesh,
        in_specs=placed,
        out_specs=(P(("kv", "tp"), None), P("tp", "kv")),
        check_vma=False,
    )
```

```python
import functools

import jax
import jax.numpy as jnp
import numpy as np
from jax import lax
from jax.experimental import pallas as pl
from jax.experimental.pallas import tpu as pltpu
from jax.sharding import PartitionSpec as P

HEAD_DIM = 64
BLK = 64
LANES = 128
VMEM_LIMIT = 55_000_000
AHEAD = 3
LOG2_E = float(np.log2(np.e))

rotary_base = 500000.0
masked_score = -1e30

MESH = pl.DeviceIdType.MESH


def in_vmem():
    return pl.BlockSpec(memory_space=pltpu.VMEM)


def in_hbm():
    return pl.BlockSpec(memory_space=pltpu.HBM)


def partner(place, step, count):
    if count & (count - 1):
        return lax.rem(place + step, count)
    mixed, bit = 0, 1
    while bit < count:
        mixed = mixed + bit * lax.rem(lax.div(place, bit) + lax.div(step, bit), 2)
        bit *= 2
    return mixed


def swap_halves(tile):
    return pltpu.roll(tile, LANES // 2, 1)


def layer_kernel(
    devices, splits, chosen_ref, x_ref, wq_ref, wk_ref, wv_ref, wo_ref,
    mine_ref, landed_ref, log_ref,
    x, wq, wkv, wo, kv_out, q_out, kv_in, vk_in, lists, place_v, place_s, bias, q_in, o_out, l_out, o_in, l_in, total_log,
    attended, stage, load_sem, kv_load, q_load, kv_send, kv_recv, q_send, q_recv, o_send, o_recv, l_send, l_recv, tp_send, tp_recv,
):
    heads = kv_out.shape[0]
    pairs = heads // 2
    groups = devices // heads
    blocks = kv_out.shape[1]
    tiles = blocks // 2
    rows = blocks * BLK
    entries = chosen_ref.shape[0]
    high = heads // 2
    wide = wq.shape[2] // LANES
    both = wkv.shape[2] // (2 * LANES)

    me = lax.axis_index("kv")
    tp = lax.axis_index("tp")
    group = lax.div(me, heads)
    idx = lax.rem(me, heads)
    first_device = group * heads
    visited = idx >= high
    half = HEAD_DIM // 2

    def pair_of(i):
        return partner(lax.div(idx, 2), jnp.int32(i), pairs)

    def strip(ref, i):
        return ref.at[:, pl.ds(pl.multiple_of(pair_of(i) * LANES, LANES), LANES)]

    def load_q(i):
        target = wq.at[i // wide, :, pl.ds((i % wide) * LANES, LANES)]
        return pltpu.make_async_copy(strip(wq_ref, i), target, q_load.at[i // wide])

    def load_k(i):
        target = wkv.at[i // both, :, pl.ds(i % both * 2 * LANES, LANES)]
        return pltpu.make_async_copy(strip(wk_ref, i), target, kv_load.at[i // both])

    def load_v(i):
        target = wkv.at[i // both, :, pl.ds((i % both * 2 + 1) * LANES, LANES)]
        return pltpu.make_async_copy(strip(wv_ref, i), target, kv_load.at[i // both])

    def loaded(ref, semaphore):
        pltpu.make_async_copy(ref, ref, semaphore).wait()

    load_x = pltpu.make_async_copy(x_ref, x, load_sem.at[0])
    load_o = pltpu.make_async_copy(wo_ref, wo, load_sem.at[1])
    load_lists = pltpu.make_async_copy(chosen_ref, lists, load_sem.at[3])
    move_places = pltpu.make_async_copy(place_v, place_s, load_sem.at[2])

    load_x.start()
    load_lists.start()
    lowest = group == 0
    early = both

    def start_kv(first, last):
        for i in range(first, last):
            load_k(i).start()
            load_v(i).start()

    def start_q():
        for i in range(pairs):
            load_q(i).start()

    pl.when(lowest)(lambda: start_kv(0, early))
    pl.when(jnp.logical_not(lowest))(start_q)

    barrier = pltpu.get_barrier_semaphore()

    def greet(d, carry):
        pl.semaphore_signal(
            barrier, inc=1, device_id={"kv": lax.rem(me + d, devices)}, device_id_type=MESH
        )
        return carry

    lax.fori_loop(1, devices, greet, 0)
    for d in range(1, splits):
        pl.semaphore_signal(barrier, inc=1, device_id={"tp": lax.rem(tp + d, splits)}, device_id_type=MESH)

    def kv_copy(slot, target):
        return pltpu.make_async_remote_copy(
            src_ref=kv_out.at[slot],
            dst_ref=kv_in.at[pl.ds(me * blocks, blocks)],
            send_sem=kv_send.at[lax.div(target, heads)],
            recv_sem=kv_recv.at[group],
            device_id={"kv": target},
            device_id_type=MESH,
        )

    def q_copy(slot, target):
        return pltpu.make_async_remote_copy(
            src_ref=q_out.at[slot],
            dst_ref=q_in.at[me],
            send_sem=q_send.at[lax.div(target, heads)],
            recv_sem=q_recv.at[me],
            device_id={"kv": target},
            device_id_type=MESH,
        )

    def o_copy(target):
        return pltpu.make_async_remote_copy(
            src_ref=o_out.at[target],
            dst_ref=o_in.at[group, idx],
            send_sem=o_send.at[lax.div(target, heads)],
            recv_sem=o_recv.at[group, lax.div(idx, 2)],
            device_id={"kv": target},
            device_id_type=MESH,
        )

    def l_copy(target):
        return pltpu.make_async_remote_copy(
            src_ref=l_out.at[target],
            dst_ref=l_in.at[group, idx],
            send_sem=l_send.at[lax.div(target, heads)],
            recv_sem=l_recv.at[group, lax.div(idx, 2)],
            device_id={"kv": target},
            device_id_type=MESH,
        )

    def arrival(ref, semaphore):
        return pltpu.make_async_remote_copy(
            src_ref=ref, dst_ref=ref, send_sem=semaphore, recv_sem=semaphore,
            device_id={"kv": me}, device_id_type=MESH,
        )

    load_x.wait()

    @pl.when(lowest)
    def _():
        start_kv(early, pairs)
        start_q()

    @pl.when(jnp.logical_not(lowest))
    def _():
        start_kv(0, pairs)

    low_rows = lax.broadcasted_iota(jnp.int32, (rows, LANES), 1) < LANES // 2
    turn_low = lax.broadcasted_iota(jnp.int32, (rows, LANES), 1) % HEAD_DIM < half

    def angles(count, step, start):
        channel = (lax.broadcasted_iota(jnp.int32, (count, LANES), 1) % half).astype(jnp.float32)
        position = lax.broadcasted_iota(jnp.int32, (count, LANES), 0) * step + start
        turn = position.astype(jnp.float32) * jnp.exp(channel * (-np.log(rotary_base) / half))
        return jnp.cos(turn), jnp.sin(turn)

    cos_fine, sin_fine = angles(8, 1, 0)
    cos_coarse, sin_coarse = angles(rows // 8, 8, me * rows)
    cos_parts, sin_parts = [], []
    for k in range(rows // 8):
        cos_k, sin_k = cos_coarse[k : k + 1], sin_coarse[k : k + 1]
        cos_parts.append(cos_k * cos_fine - sin_k * sin_fine)
        sin_parts.append(sin_k * cos_fine + cos_k * sin_fine)
    cos_part = jnp.concatenate(cos_parts, axis=0)
    sin_part = jnp.concatenate(sin_parts, axis=0)
    sin_part = jnp.where(turn_low, -sin_part, sin_part)

    def turned(part):
        other = jnp.where(turn_low, pltpu.roll(part, LANES - half, 1), pltpu.roll(part, half, 1))
        return part * cos_part + other * sin_part

    def make_kv(first):
        loaded(wkv.at[first // both], kv_load.at[first // both])
        made = jnp.dot(x[...], wkv[first // both], preferred_element_type=jnp.float32)
        for i in range(first, first + both):
            lane = (i - first) * 2 * LANES
            keys = turned(made[:, lane : lane + LANES])
            values = made[:, lane + LANES : lane + 2 * LANES]
            even = jnp.where(low_rows, keys, swap_halves(values)).astype(jnp.bfloat16)
            odd = jnp.where(low_rows, swap_halves(keys), values).astype(jnp.bfloat16)
            for r in range(blocks):
                kv_out[2 * i, r] = even[r * BLK : (r + 1) * BLK]
                kv_out[2 * i + 1, r] = odd[r * BLK : (r + 1) * BLK]

    def make_q(i):
        loaded(wq.at[i // wide], q_load.at[i // wide])
        made = jnp.dot(x[...], wq[i // wide], preferred_element_type=jnp.float32)
        for e in range(wide):
            part = turned(made[:, e * LANES : (e + 1) * LANES]) * (HEAD_DIM**-0.5 * LOG2_E)
            swapped = swap_halves(part)
            low = low_rows[:BLK]
            for m in range(tiles):
                a = slice(2 * m * BLK, (2 * m + 1) * BLK)
                b = slice((2 * m + 1) * BLK, (2 * m + 2) * BLK)
                q_out[2 * (i + e), m] = jnp.where(low, part[a], swapped[b]).astype(jnp.bfloat16)
                q_out[2 * (i + e) + 1, m] = jnp.where(low, swapped[a], part[b]).astype(jnp.bfloat16)

    def send_kv(i):
        for e in range(2):
            head = 2 * pair_of(i) + e
            if i > 0:
                kv_copy(2 * i + e, first_device + head).start()
            else:
                pl.when(head != idx)(lambda e=e, head=head: kv_copy(2 * i + e, first_device + head).start())

    def send_q(i):
        for e in range(2):
            head = 2 * pair_of(i) + e
            if i > 0:
                q_copy(2 * i + e, first_device + head).start()
            else:
                pl.when(head != idx)(lambda e=e, head=head: q_copy(2 * i + e, first_device + head).start())

    def send_down():
        def send(a, carry):
            for i in range(pairs):
                for e in range(2):
                    head = 2 * pair_of(i) + e

                    @pl.when(head >= high)
                    def _(i=i, e=e, head=head):
                        q_copy(2 * i + e, a * heads + head).start()

            return carry

        lax.fori_loop(0, group, send, 0)

    def send_up():
        def send(a, carry):
            for i in range(pairs):
                for e in range(2):
                    head = 2 * pair_of(i) + e

                    @pl.when(head < high)
                    def _(i=i, e=e, head=head):
                        kv_copy(2 * i + e, a * heads + head).start()

            return carry

        lax.fori_loop(group + 1, groups, send, 0)

    def make_queries():
        for i in range(0, pairs, wide):
            make_q(i)

    @pl.when(jnp.logical_not(lowest))
    def _():
        make_queries()
        pl.semaphore_wait(barrier, devices - 1 + splits - 1)
        send_down()

    for i in range(0, pairs, both):
        make_kv(i)
        if i == 0:
            pl.when(lowest)(lambda: pl.semaphore_wait(barrier, devices - 1 + splits - 1))
        for e in range(both):
            send_kv(i + e)
    send_up()
    pl.when(lowest)(make_queries)
    for i in range(pairs):
        send_q(i)
    load_o.start()

    load_lists.wait()
    place = lists[...]
    lowest_block = jnp.where(visited, first_device * blocks, 0)
    held = (place >= lowest_block) & (place < (first_device + heads) * blocks)
    place_v[...] = jnp.where(held, place, lowest_block)
    move_places.start()
    column = lax.broadcasted_iota(jnp.int32, (entries, entries * BLK), 1)
    slot = column // (8 * BLK) * 8 + column // BLK % 4 * 2 + column // (4 * BLK) % 2
    unit = (slot == lax.broadcasted_iota(jnp.int32, slot.shape, 0)).astype(jnp.float32)
    bias[...] = masked_score * (
        1.0
        - lax.dot_general(
            jnp.where(held, 1.0, 0.0), unit, (((0,), (0,)), ((), ())), preferred_element_type=jnp.float32
        )
    )
    move_places.wait()

    own_slot = lax.rem(idx, 2)
    for r in range(blocks):
        kv_in[me * blocks + r] = kv_out[own_slot, r]
    for m in range(tiles):
        q_in[me, m] = q_out[own_slot, m]

    low = lax.broadcasted_iota(jnp.int32, (BLK, LANES), 1) < LANES // 2
    lane = lax.broadcasted_iota(jnp.int32, (BLK, LANES), 1)
    low_line = lax.broadcasted_iota(jnp.int32, (1, LANES), 1) < LANES // 2

    arrival(kv_in.at[pl.ds(0, (heads - 1) * blocks)], kv_recv.at[group]).wait_recv()

    def swap_kv(k, carry):
        for r in range(blocks):
            place = k * blocks + r
            vk_in[place] = swap_halves(kv_in[place].astype(jnp.float32)).astype(jnp.bfloat16)
        return carry

    lax.fori_loop(first_device, first_device + heads, swap_kv, 0)

    def take_lower(a, carry):
        arrival(kv_in.at[pl.ds(0, heads * blocks)], kv_recv.at[a]).wait_recv()
        return lax.fori_loop(a * heads, (a + 1) * heads, swap_kv, carry)

    lax.fori_loop(0, jnp.where(visited, 0, group), take_lower, 0)

    def attend(js, entries):
        stacks = []
        for j in js:
            for m in range(tiles):
                tile = q_in[j, m]
                swapped = swap_halves(tile.astype(jnp.float32)).astype(jnp.bfloat16)
                none = jnp.zeros_like(tile)
                for at_low, at_high in ((tile, swapped), (swapped, tile)):
                    stacks.append(
                        jnp.concatenate([jnp.where(low, at_low, none), jnp.where(low, none, at_high)], axis=0)
                    )

        def score(n):
            block = js[n // blocks] * blocks + n % blocks
            scores, values = [], []
            for lower in range(0, entries, 8):
                keys_here, values_here = [], []
                for s in range(lower, lower + 8, 2):
                    a = kv_in[place_s[s, block]]
                    b = vk_in[place_s[s + 1, block]]
                    keys_here.append(jnp.where(low, a, b))
                    values_here.append(jnp.where(low, b, a))
                made = lax.dot_general(
                    stacks[n], jnp.concatenate(keys_here, axis=0), (((1,), (1,)), ((), ())),
                    preferred_element_type=jnp.float32,
                )
                line = bias[pl.ds(block, 1), lower * BLK : (lower + 8) * BLK]
                scores += [made[:BLK] + line[:, : 4 * BLK], made[BLK:] + line[:, 4 * BLK :]]
                values.append(jnp.concatenate(values_here, axis=0))
            top = jnp.max(functools.reduce(jnp.maximum, scores), axis=1, keepdims=True)
            return scores, values, top

        def gather(n, scores, values, top):
            weights = [jnp.exp2(part - top) for part in scores]
            total = jnp.sum(functools.reduce(jnp.add, weights), axis=1, keepdims=True)
            made = 0.0
            for k, held_values in enumerate(values):
                rounded = jnp.concatenate([part.astype(jnp.bfloat16) for part in weights[2 * k : 2 * k + 2]], axis=0)
                made = made + jnp.dot(rounded, held_values, preferred_element_type=jnp.float32)
            if n % 2 == 0:
                summed = swap_halves(made[:BLK]) + made[BLK:]
            else:
                summed = made[:BLK] + swap_halves(made[BLK:])
            return summed / total, (top + jnp.log2(total)) * (1.0 / LOG2_E)

        ready, results = [], []
        for n in range(len(js) * blocks + AHEAD):
            if n < len(js) * blocks:
                ready.append(score(n))
            if n >= AHEAD:
                results.append(gather(n - AHEAD, *ready[n - AHEAD]))
        for k, j in enumerate(js):
            found = results[k * blocks : (k + 1) * blocks]
            logs = jnp.zeros((BLK, LANES), jnp.float32)
            for r in range(blocks):
                logs = jnp.where(lane == r, found[r][1], logs)
            for m in range(tiles):
                o_out[j, m] = jnp.where(low, found[2 * m][0], found[2 * m + 1][0]).astype(jnp.bfloat16)
            lines = jnp.transpose(jnp.concatenate([logs, jnp.zeros_like(logs)], axis=0))
            for m in range(tiles):
                first, second = lines[2 * m : 2 * m + 1], lines[2 * m + 1 : 2 * m + 2]
                l_out[j, m : m + 1] = jnp.where(low_line, first, swap_halves(second))

    batch = 2
    visits = jnp.where(visited, (groups - 1 - group) * heads, 0)
    opening = jnp.where(visits == 0, heads, 2)

    def served(t):
        visiting = (t >= opening) & (t < opening + visits)
        visitor = jnp.where(visiting, t - opening, 0)
        own = jnp.where(t < opening, t, jnp.where(visiting, 0, heads + 1 - (t - visits)))
        target = group + jnp.where(visiting, 1 + lax.div(visitor, heads), 0)
        step = jnp.where(visiting, lax.rem(visitor, heads), own)
        return target * heads + partner(idx, step, heads)

    def serve(u, carry):
        js = [served(batch * u + k) for k in range(batch)]
        for j in js:

            @pl.when(j != me)
            def _(j=j):
                arrival(q_in.at[j], q_recv.at[j]).wait_recv()

        short = functools.reduce(jnp.maximum, js) < 8 // blocks
        pl.when(short)(lambda: attend(js, 8))
        pl.when(jnp.logical_not(short))(lambda: attend(js, entries))
        for j in js:

            @pl.when(j != me)
            def _(j=j):
                o_copy(j).start()
                l_copy(j).start()

            @pl.when(j == me)
            def _(j=j):
                for m in range(tiles):
                    o_in[group, idx, m] = o_out[j, m]
                l_in[group, idx] = l_out[j]

        return carry

    lax.fori_loop(0, lax.div(heads + visits, batch), serve, 0)

    def absent(a, carry):
        o_in[a] = jnp.zeros(o_in.shape[1:], o_in.dtype)
        l_in[a] = jnp.full(l_in.shape[1:], masked_score, jnp.float32)
        return carry

    lax.fori_loop(group + 1, groups, absent, 0)

    def partly_absent(a, carry):
        o_in[a, :high] = jnp.zeros((high,) + o_in.shape[2:], o_in.dtype)
        l_in[a, :high] = jnp.full((high,) + l_in.shape[2:], masked_score, jnp.float32)
        return carry

    lax.fori_loop(0, group, partly_absent, 0)

    def spread(body, start):
        if groups <= 2:
            for a in range(groups):
                start = body(a, start)
            return start
        return lax.fori_loop(0, groups, body, start)

    for i in range(pairs):
        ch = pair_of(i)

        def take_results(a, carry, i=i, ch=ch):
            def take(count):
                o_place = o_in.at[a, pl.ds(2 * ch, count)]
                arrival(o_place, o_recv.at[a, ch]).wait_recv()
                l_place = l_in.at[a, pl.ds(2 * ch, count)]
                arrival(l_place, l_recv.at[a, ch]).wait_recv()

            pl.when(a == group)(lambda: take(2 if i > 0 else 1))
            pl.when((a < group) & (2 * ch + 1 >= high))(lambda: take(min(2, high)))
            return carry

        lax.fori_loop(0, group + 1, take_results, 0)

        def lines(a, ch=ch):
            return l_in[a, pl.ds(2 * ch, 2)]

        start = jnp.full((2, tiles, LANES), masked_score, jnp.float32)
        highest = spread(lambda a, top: jnp.maximum(top, lines(a)), start)
        sums = spread(lambda a, acc: acc + jnp.exp(lines(a) - highest), jnp.zeros_like(start))
        logs = highest + jnp.log(sums)
        total_log[pl.ds(2 * ch, 2)] = logs

        def add_share(a, parts, ch=ch, logs=logs):
            share = jnp.exp(lines(a) - logs)
            share = [share[e, m : m + 1] for e in range(2) for m in range(tiles)]
            share.append(jnp.zeros((LANES - 2 * tiles, LANES), jnp.float32))
            columns = jnp.transpose(jnp.concatenate(share, axis=0))
            made = []
            for m in range(tiles):
                t0 = o_in[a, 2 * ch, m].astype(jnp.float32)
                t1 = o_in[a, 2 * ch + 1, m].astype(jnp.float32)
                both = (jnp.where(low, t0, swap_halves(t1)), jnp.where(low, swap_halves(t0), t1))
                for e in range(2):
                    r = 2 * m + e
                    here = columns[e * BLK : (e + 1) * BLK]
                    scale = jnp.where(low, here[:, m : m + 1], here[:, tiles + m : tiles + m + 1])
                    made.append(parts[r] + both[e] * scale)
            return tuple(made)

        made = spread(add_share, tuple(jnp.zeros((BLK, LANES), jnp.float32) for _ in range(blocks)))
        for r in range(blocks):
            columns = pl.ds(pl.multiple_of(ch * LANES, LANES), LANES)
            attended[r * BLK : (r + 1) * BLK, columns] = made[r].astype(jnp.bfloat16)

    for m in range(tiles):
        log_ref[:, m * LANES : (m + 1) * LANES] = total_log[:, m, :]

    load_o.wait()
    out_rows = rows // splits
    tile_width = min(512, wo.shape[1])
    chunks = wo.shape[1] // tile_width
    peers = [lax.rem(tp + d, splits) for d in range(splits)]

    def own_rows(d):
        return pl.ds(pl.multiple_of(peers[d] * out_rows, out_rows), out_rows)

    def hop(d, c):
        return pltpu.make_async_remote_copy(
            src_ref=stage.at[c, own_rows(d)],
            dst_ref=landed_ref.at[d - 1, :, pl.ds(c * tile_width, tile_width)],
            send_sem=tp_send.at[d - 1],
            recv_sem=tp_recv.at[d - 1],
            device_id={"tp": peers[d]},
            device_id_type=MESH,
        )

    def product(place, c):
        columns = slice(c * tile_width, (c + 1) * tile_width)
        made = jnp.dot(attended[place], wo[:, columns], preferred_element_type=jnp.float32)
        stage[c, place] = made.astype(jnp.bfloat16)

    for d in range(1, splits):
        for c in range(chunks):
            product(own_rows(d), c)
            hop(d, c).start()
    for c in range(chunks):
        columns = slice(c * tile_width, (c + 1) * tile_width)
        made = jnp.dot(attended[own_rows(0)], wo[:, columns], preferred_element_type=jnp.float32)
        mine_ref[:, columns] = made.astype(jnp.bfloat16)

    def sent(ref, semaphore):
        arrival(ref, semaphore).wait_send()

    sent(kv_out.at[pl.ds(0, heads - 1)], kv_send.at[group])
    sent(q_out.at[pl.ds(0, heads - 1)], q_send.at[group])

    def sent_down(a, carry):
        sent(q_out.at[pl.ds(0, heads - high)], q_send.at[a])
        return carry

    lax.fori_loop(0, group, sent_down, 0)
    sent(o_out.at[pl.ds(0, heads - 1)], o_send.at[group])
    sent(l_out.at[pl.ds(0, heads - 1)], l_send.at[group])

    def sent_up(a, carry):
        sent(kv_out.at[pl.ds(0, high)], kv_send.at[a])

        @pl.when(visited)
        def _():
            sent(o_out.at[pl.ds(0, heads)], o_send.at[a])
            sent(l_out.at[pl.ds(0, heads)], l_send.at[a])

        return carry

    lax.fori_loop(group + 1, groups, sent_up, 0)
    for d in range(1, splits):
        sent(stage.at[:, own_rows(d)], tp_send.at[d - 1])
        arrival(landed_ref.at[d - 1], tp_recv.at[d - 1]).wait_recv()


def local(devices, splits, tokens, w_query, w_key, w_value, w_out, chosen):
    rows, depth = tokens.shape
    width = w_query.shape[1]
    out_width = w_out.shape[1]
    heads = width // HEAD_DIM
    pairs = heads // 2
    groups = devices // heads
    blocks = rows // BLK
    tiles = blocks // 2
    wide = pairs
    both = 2 if pairs % 2 == 0 else 1

    out_rows = rows // splits
    tile_width = min(512, out_width)
    chunks = out_width // tile_width
    dma = pltpu.SemaphoreType.DMA
    bf16, f32 = jnp.bfloat16, jnp.float32
    mine, landed, logs = pl.pallas_call(
        functools.partial(layer_kernel, devices, splits),
        in_specs=[in_hbm()] * 6,
        out_specs=[in_vmem()] * 3,
        out_shape=[
            jax.ShapeDtypeStruct((out_rows, out_width), bf16),
            jax.ShapeDtypeStruct((splits - 1, out_rows, out_width), bf16),
            jax.ShapeDtypeStruct((heads, rows), f32),
        ],
        scratch_shapes=[
            pltpu.VMEM((rows, depth), bf16),
            pltpu.VMEM((pairs // wide, depth, wide * LANES), bf16),
            pltpu.VMEM((pairs // both, depth, both * 2 * LANES), bf16),
            pltpu.VMEM((width, out_width), bf16),
            pltpu.VMEM((heads, blocks, BLK, LANES), bf16),
            pltpu.VMEM((heads, tiles, BLK, LANES), bf16),
            pltpu.VMEM((devices * blocks, BLK, LANES), bf16),
            pltpu.VMEM((devices * blocks, BLK, LANES), bf16),
            pltpu.VMEM(chosen.shape[::-1], jnp.int32),
            pltpu.VMEM(chosen.shape[::-1], jnp.int32),
            pltpu.SMEM(chosen.shape[::-1], jnp.int32),
            pltpu.VMEM((chosen.shape[0], chosen.shape[1] * BLK), f32),
            pltpu.VMEM((devices, tiles, BLK, LANES), bf16),
            pltpu.VMEM((devices, tiles, BLK, LANES), bf16),
            pltpu.VMEM((devices, tiles, LANES), f32),
            pltpu.VMEM((groups, heads, tiles, BLK, LANES), bf16),
            pltpu.VMEM((groups, heads, tiles, LANES), f32),
            pltpu.VMEM((heads, tiles, LANES), f32),
            pltpu.VMEM((rows, width), bf16),
            pltpu.VMEM((chunks, rows, tile_width), bf16),
            dma((4,)),
            dma((pairs // both,)),
            dma((pairs // wide,)),
            dma((groups,)),
            dma((groups,)),
            dma((groups,)),
            dma((devices,)),
            dma((groups,)),
            dma((groups, pairs)),
            dma((groups,)),
            dma((groups, pairs)),
            dma((splits - 1,)),
            dma((splits - 1,)),
        ],
        compiler_params=pltpu.CompilerParams(
            collective_id=0, has_side_effects=True, vmem_limit_bytes=VMEM_LIMIT
        ),
        name="layer",
    )(pltpu.with_memory_space_constraint(jnp.transpose(chosen), pltpu.HBM), tokens, w_query, w_key, w_value, w_out)
    total = mine.astype(f32) + jnp.sum(landed.astype(f32), axis=0)
    return total.astype(bf16), logs


def solution(mesh):
    placed = (P("kv", None), P(None, "tp"), P(None, "tp"), P(None, "tp"), P("tp", None), P())
    return jax.shard_map(
        functools.partial(local, mesh.shape["kv"], mesh.shape["tp"]),
        mesh=mesh,
        in_specs=placed,
        out_specs=(P(("kv", "tp"), None), P("tp", "kv")),
        check_vma=False,
    )
```
